256 devices in a mesh: kv: 32 (over z, y), tp: 8 (over x, core).
Axes of the slice: x: 4, y: 4, z: 8, core: 2. Of those that a mesh axis runs over, the one named last changes fastest.
Arguments:
- residual: bfloat16 [1024, 2048], P('kv', 'tp'), may hold values from -12 to 12
- first_gain: bfloat16 [2048], P('tp'), may hold values from 0.099609375 to 1.8984375
- first_gate: bfloat16 [2048, 5632], P('tp', 'kv'), may hold values from -0.125 to 0.125
- first_lift: bfloat16 [2048, 5632], P('tp', 'kv'), may hold values from -0.125 to 0.125
- first_down: bfloat16 [5632, 2048], P('kv', 'tp'), may hold values from -0.078125 to 0.078125
- mixer_gain: bfloat16 [2048], replicated, may hold values from 0.099609375 to 1.8984375
- proj_gate: bfloat16 [2048, 2048], P(None, 'tp'), may hold values from -0.125 to 0.125
- proj_input: bfloat16 [2048, 2048], P(None, 'tp'), may hold values from -0.125 to 0.125
- proj_write: bfloat16 [2048, 1024], P(None, 'tp'), may hold values from -0.125 to 0.125
- proj_read: bfloat16 [2048, 1024], P(None, 'tp'), may hold values from -0.125 to 0.125
- proj_step: bfloat16 [2048, 32], P(None, 'tp'), may hold values from -0.125 to 0.125
- step_bias: float32 [32], P('tp'), may hold values from -5 to -2
- rate_log: float32 [32], P('tp'), may hold values from -0.7 to 2.1
- skip_gain: float32 [32], P('tp'), may hold values from 0.5 to 2
- taps_input: bfloat16 [4, 2048], P(None, 'tp'), may hold values from -3 to 3
- taps_write: bfloat16 [4, 1024], P(None, 'tp'), may hold values from -3 to 3
- taps_read: bfloat16 [4, 1024], P(None, 'tp'), may hold values from -3 to 3
- buffer_input: bfloat16 [1024, 3, 2048], P('kv', None, 'tp'), may hold values from -6 to 6
- buffer_write: bfloat16 [1024, 3, 1024], P('kv', None, 'tp'), may hold values from -6 to 6
- buffer_read: bfloat16 [1024, 3, 1024], P('kv', None, 'tp'), may hold values from -6 to 6
- scan_state: float32 [1024, 32, 64, 128], P('kv', 'tp'), may hold values from -1.5 to 1.5
- group_gain: bfloat16 [2048], P('tp'), may hold values from 0.099609375 to 1.8984375
- proj_output: bfloat16 [2048, 2048], P('tp'), may hold values from -0.125 to 0.125
- second_gain: bfloat16 [2048], P('tp'), may hold values from 0.099609375 to 1.8984375
- second_gate: bfloat16 [2048, 5632], P('tp', 'kv'), may hold values from -0.125 to 0.125
- second_lift: bfloat16 [2048, 5632], P('tp', 'kv'), may hold values from -0.125 to 0.125
- second_down: bfloat16 [5632, 2048], P('kv', 'tp'), may hold values from -0.078125 to 0.078125
Outputs:
- residual_out: bfloat16 [1024, 2048], P('kv', 'tp')
- state_out: float32 [1024, 32, 64, 128], P('kv', 'tp')
The draws below stay inside these ranges and needn't reach their ends.
All inputs are finite; a program needn't handle non-finite values.
Results may differ from the reference program's by a relative error of at most 0.023.
Values may be sent and summed in bfloat16 or wider, within the bound.
No kernel may reach another device: no remote copies, remote signals or barrier semaphores. Data moves between devices by JAX's collectives and lax.ppermute only.
A program may use at most 64 MiB of HBM per device.

```python
import jax
import jax.numpy as jnp
from jax import lax

D = 2048
FF = 5632
HEADS = 32
HEAD_DIM = 64
STATE = 128
NGROUPS = 8
CONV = 4
D_SSD = 2048
BATCH = 1024
N_TP = 8


def draw_residual(key, part):
    first_key = jax.random.fold_in(key, 0)
    columns = jnp.arange(D, dtype=jnp.float32)
    column_ramp = 0.5 * jnp.power(4.0, columns / (D - 1))
    entries = jax.random.normal(first_key, (BATCH, D), jnp.float32)
    return jnp.clip(entries * column_ramp[None, :], -12.0, 12.0).astype(jnp.bfloat16)


def steps_of(own_key, extent, cuts, least, largest):
    level, own = 1.0, jax.random.fold_in(own_key, 6)
    for position, shards_of in cuts:
        heights = jnp.exp(jax.random.uniform(jax.random.fold_in(own, position), (shards_of,), jnp.float32, least / len(cuts), largest / len(cuts)))
        level = level * jnp.repeat(heights, extent[position] // shards_of).reshape([-1 if axis == position else 1 for axis in range(len(extent))])
    return level


def gaussian(key, dims, width, most, shards=(), held_as=jnp.bfloat16):
    level = steps_of(key, dims, shards, -0.22, 0.18) if shards else 1.0
    values = jax.random.normal(key, dims, jnp.float32) * width * level
    return jnp.minimum(jnp.maximum(values, -most), most).astype(held_as)


def setup_inputs(seed: int = 0) -> dict:
    seeds = jax.random.split(jax.random.key(seed), 28)
    return {
        "residual": draw_residual(jax.random.fold_in(seeds[27], 71), 0),
        "first_gain": jnp.clip(1.0 + 0.18 * jax.random.normal(seeds[1], (D,), jnp.float32), 0.099609375, 1.8984375).astype(jnp.bfloat16),
        "first_gate": gaussian(seeds[2], (D, FF), D ** -0.5, 0.125, ((0, 8), (1, 32))),
        "first_lift": gaussian(seeds[3], (D, FF), D ** -0.5, 0.125, ((0, 8), (1, 32))),
        "first_down": gaussian(seeds[4], (FF, D), FF ** -0.5, 0.078125, ((0, 32), (1, 8))),
        "mixer_gain": jnp.clip(1.0 + 0.18 * jax.random.normal(seeds[5], (D,), jnp.float32), 0.099609375, 1.8984375).astype(jnp.bfloat16),
        "proj_gate": gaussian(seeds[6], (D, D_SSD), D ** -0.5, 0.125, ((1, 8),)),
        "proj_input": gaussian(seeds[7], (D, D_SSD), D ** -0.5, 0.125, ((1, 8),)),
        "proj_write": gaussian(seeds[8], (D, NGROUPS * STATE), D ** -0.5, 0.125, ((1, 8),)),
        "proj_read": gaussian(seeds[9], (D, NGROUPS * STATE), D ** -0.5, 0.125, ((1, 8),)),
        "proj_step": gaussian(seeds[10], (D, HEADS), D ** -0.5, 0.125, ((1, 8),)),
        "step_bias": jnp.clip(-5.0 + 3.0 * jax.random.uniform(seeds[11], (HEADS,), jnp.float32) ** steps_of(seeds[11], (HEADS,), ((0, 8),), -0.2, 0.2), -5.0, -2.0),
        "rate_log": jnp.clip(-0.7 + 2.8 * jax.random.uniform(seeds[12], (HEADS,), jnp.float32) ** steps_of(seeds[12], (HEADS,), ((0, 8),), -0.2, 0.2), -0.7, 2.1),
        "skip_gain": jnp.clip(0.5 + 1.5 * jax.random.uniform(seeds[13], (HEADS,), jnp.float32) ** steps_of(seeds[13], (HEADS,), ((0, 8),), -0.2, 0.2), 0.5, 2.0),
        "taps_input": gaussian(seeds[14], (CONV, D_SSD), CONV ** -0.5, 3.0, ((1, 8),)),
        "taps_write": gaussian(seeds[15], (CONV, NGROUPS * STATE), CONV ** -0.5, 3.0, ((1, 8),)),
        "taps_read": gaussian(seeds[16], (CONV, NGROUPS * STATE), CONV ** -0.5, 3.0, ((1, 8),)),
        "buffer_input": gaussian(seeds[17], (BATCH, CONV - 1, D_SSD), 1.0, 6.0, ((0, 32), (2, 8))),
        "buffer_write": gaussian(seeds[18], (BATCH, CONV - 1, NGROUPS * STATE), 1.0, 6.0, ((0, 32), (2, 8))),
        "buffer_read": gaussian(seeds[19], (BATCH, CONV - 1, NGROUPS * STATE), 1.0, 6.0, ((0, 32), (2, 8))),
        "scan_state": gaussian(seeds[20], (BATCH, HEADS, HEAD_DIM, STATE), 0.1, 1.5, ((0, 32), (1, 8)), jnp.float32),
        "group_gain": jnp.clip(1.0 + 0.18 * jax.random.normal(seeds[21], (D_SSD,), jnp.float32), 0.099609375, 1.8984375).astype(jnp.bfloat16),
        "proj_output": gaussian(seeds[22], (D_SSD, D), D_SSD ** -0.5, 0.125, ((0, 8),)),
        "second_gain": jnp.clip(1.0 + 0.18 * jax.random.normal(seeds[23], (D,), jnp.float32), 0.099609375, 1.8984375).astype(jnp.bfloat16),
        "second_gate": gaussian(seeds[24], (D, FF), D ** -0.5, 0.125, ((0, 8), (1, 32))),
        "second_lift": gaussian(seeds[25], (D, FF), D ** -0.5, 0.125, ((0, 8), (1, 32))),
        "second_down": gaussian(seeds[26], (FF, D), FF ** -0.5, 0.078125, ((0, 32), (1, 8))),
    }


norm_eps = 1e-06

def inverse_rms(values):
    return lax.rsqrt(lax.optimization_barrier(jnp.mean(values * values, axis=-1, keepdims=True)) + norm_eps)

def block_sum(activ, weight, pieces):
    seq_rows = activ.shape[0]
    inner = activ.shape[1] // pieces
    widened = lax.optimization_barrier(activ).astype(jnp.float32).reshape(seq_rows, pieces, inner)
    weight_f = weight.astype(jnp.float32).reshape(pieces, inner, weight.shape[1])
    partial_value = jnp.einsum('btk,tkf->tbf', widened, weight_f)
    rounded = lax.optimization_barrier(partial_value.astype(jnp.bfloat16)).astype(jnp.float32)
    return lax.optimization_barrier(jnp.sum(rounded, axis=0))

def half_step(residual, gain, gate_weight, lift_weight, down_weight):
    widened = residual.astype(jnp.float32)
    normed = (widened * inverse_rms(widened) * gain.astype(jnp.float32)).astype(jnp.bfloat16)
    gate_sum = block_sum(normed, gate_weight, N_TP)
    up_sum = block_sum(normed, lift_weight, N_TP)
    hidden = (jax.nn.silu(gate_sum) * up_sum).astype(jnp.bfloat16)
    branch = jnp.dot(hidden, down_weight, preferred_element_type=jnp.float32)
    return (widened + 0.5 * branch).astype(jnp.bfloat16)

def short_conv(tap_weights, buffer, newest):
    taps_f = tap_weights.astype(jnp.float32)
    summed = lax.optimization_barrier(jnp.sum(buffer.astype(jnp.float32) * taps_f[None, :-1, :], axis=1))
    summed = summed + newest.astype(jnp.float32) * taps_f[-1][None, :]
    return jax.nn.silu(summed)

def state_mixer(residual, mixer_gain, proj_gate, proj_input, proj_write, proj_read, proj_step, step_bias, rate_log, skip_gain, taps_input, taps_write, taps_read, buffer_input, buffer_write, buffer_read, scan_state, group_gain, proj_output):
    seq_rows = residual.shape[0]
    widened = residual.astype(jnp.float32)
    normed = (widened * inverse_rms(widened) * mixer_gain.astype(jnp.float32)).astype(jnp.bfloat16)

    def project(weight):
        return jnp.dot(normed, weight, preferred_element_type=jnp.float32).astype(jnp.bfloat16)
    gate_z = project(proj_gate)
    input_new = project(proj_input)
    write_new = project(proj_write)
    read_new = project(proj_read)
    step_raw = project(proj_step)
    input_conv = short_conv(taps_input, buffer_input, input_new)
    write_conv = short_conv(taps_write, buffer_write, write_new)
    read_conv = short_conv(taps_read, buffer_read, read_new)
    head_count = proj_step.shape[1]
    group_count = proj_write.shape[1] // STATE
    per_group = head_count // group_count
    step = jax.nn.softplus(step_raw.astype(jnp.float32) + step_bias[None, :])
    retain = jnp.exp(-step * jnp.exp(rate_log)[None, :])
    input_heads = input_conv.reshape(seq_rows, group_count, per_group, HEAD_DIM)
    write_groups = write_conv.reshape(seq_rows, group_count, STATE)
    read_groups = read_conv.reshape(seq_rows, group_count, STATE)
    old_state = scan_state.reshape(seq_rows, group_count, per_group, HEAD_DIM, STATE)
    retain_g = retain.reshape(seq_rows, group_count, per_group)
    step_g = step.reshape(seq_rows, group_count, per_group)
    updated = retain_g[..., None, None] * old_state + (step_g[..., None] * input_heads)[..., None] * write_groups[:, :, None, None, :]
    head_out = jnp.einsum('bgrpn,bgn->bgrp', updated, read_groups, precision=lax.Precision.HIGHEST)
    head_out = head_out + skip_gain.reshape(group_count, per_group)[None, :, :, None] * input_heads
    head_short = lax.optimization_barrier(head_out.astype(jnp.bfloat16))
    gated = head_short.astype(jnp.float32).reshape(seq_rows, group_count, per_group * HEAD_DIM)
    gated = gated * jax.nn.silu(gate_z.astype(jnp.float32).reshape(seq_rows, group_count, per_group * HEAD_DIM))
    gated = gated * inverse_rms(gated) * group_gain.astype(jnp.float32).reshape(group_count, per_group * HEAD_DIM)[None]
    gated = gated.reshape(seq_rows, head_count * HEAD_DIM).astype(jnp.bfloat16)
    mixed = block_sum(gated, proj_output, N_TP)
    return ((widened + mixed).astype(jnp.bfloat16), updated.reshape(seq_rows, head_count, HEAD_DIM, STATE))

def reference(residual, first_gain, first_gate, first_lift, first_down, mixer_gain, proj_gate, proj_input, proj_write, proj_read, proj_step, step_bias, rate_log, skip_gain, taps_input, taps_write, taps_read, buffer_input, buffer_write, buffer_read, scan_state, group_gain, proj_output, second_gain, second_gate, second_lift, second_down):
    first = half_step(residual, first_gain, first_gate, first_lift, first_down)
    mixed, state_out = state_mixer(first, mixer_gain, proj_gate, proj_input, proj_write, proj_read, proj_step, step_bias, rate_log, skip_gain, taps_input, taps_write, taps_read, buffer_input, buffer_write, buffer_read, scan_state, group_gain, proj_output)
    residual_out = half_step(mixed, second_gain, second_gate, second_lift, second_down)
    return (residual_out, state_out)
```

```python
import jax
import jax.numpy as jnp
from jax import lax
from jax.experimental import pallas as pl
from jax.experimental.pallas import tpu as pltpu
from jax.sharding import PartitionSpec as P

D = 2048
HEAD_DIM = 64
STATE = 128
FEATS = 256
HIDDEN = 176
ROWS = 4

norm_eps = 1e-06


def sent_to_all(array, axis):
    length = lax.axis_size(axis)
    return lax.all_to_all(
        jnp.broadcast_to(array[None], (length, *array.shape)), axis, 0, 0, tiled=True
    )


def inverse_rms(values):
    return lax.rsqrt(jnp.mean(values * values, axis=-1, keepdims=True) + norm_eps)


def shift_perm(shift):
    return [(i, (i + shift) % 8) for i in range(8)]


def gathered_weights(gain, gate_weight, lift_weight, down_weight):
    gain_f = gain.astype(jnp.float32)[None, :]
    gate_t = (gate_weight.T.astype(jnp.float32) * gain_f).astype(jnp.bfloat16)
    lift_t = (lift_weight.T.astype(jnp.float32) * gain_f).astype(jnp.bfloat16)
    own = jnp.concatenate([gate_t, lift_t, down_weight], axis=0)
    pieces = [own] + [lax.ppermute(own, "tp", shift_perm(s)) for s in (2, 4, 6)]
    swap = [(i, i ^ 1) for i in range(8)]
    return pieces + [lax.ppermute(piece, "tp", swap) for piece in pieces]


def ffn_kernel(tp_ref, rows_ref, *refs):
    weights, out_ref, normed_ref = refs[:8], refs[8], refs[9]
    tp = tp_ref[0]
    values = rows_ref[...].astype(jnp.float32)
    factor = lax.rsqrt(jnp.sum(values * values, axis=-1, keepdims=True) * (1.0 / D) + norm_eps)
    for u in range(8):
        normed_ref[u] = (values[:, u * FEATS : (u + 1) * FEATS] * factor).astype(jnp.bfloat16)
    chip, core = tp // 2, tp % 2
    owners = [((chip + 4 - j) % 4) * 2 + core for j in range(4)]
    owners = owners + [((chip + 4 - j) % 4) * 2 + 1 - core for j in range(4)]
    contract = (((1,), (1,)), ((), ()))
    gate = jnp.zeros((values.shape[0], HIDDEN), jnp.float32)
    lift = jnp.zeros((values.shape[0], HIDDEN), jnp.float32)
    for j in range(8):
        block = normed_ref[owners[j]]
        gate += lax.dot_general(
            block, weights[j][:HIDDEN], contract, preferred_element_type=jnp.float32
        )
        lift += lax.dot_general(
            block, weights[j][HIDDEN : 2 * HIDDEN], contract, preferred_element_type=jnp.float32
        )
    hidden = (gate * jax.nn.sigmoid(gate) * lift).astype(jnp.bfloat16)
    for j in range(8):
        down = jnp.dot(hidden, weights[j][2 * HIDDEN :], preferred_element_type=jnp.float32)
        out_ref[owners[j]] = down.astype(jnp.bfloat16)


def ffn_partial(rows, weights):
    tp = lax.axis_index("tp").astype(jnp.int32).reshape(1)
    count = rows.shape[0]
    return pl.pallas_call(
        ffn_kernel,
        out_shape=jax.ShapeDtypeStruct((8, count, FEATS), jnp.bfloat16),
        in_specs=[pl.BlockSpec(memory_space=pltpu.SMEM)]
        + [pl.BlockSpec(memory_space=pltpu.VMEM)] * 9,
        out_specs=pl.BlockSpec(memory_space=pltpu.VMEM),
        scratch_shapes=[pltpu.VMEM((8, count, FEATS), jnp.bfloat16)],
        name="ffn",
    )(tp, rows, *weights)


def short_conv(tap_weights, buffer, newest):
    taps_f = tap_weights.astype(jnp.float32)
    summed = jnp.sum(buffer.astype(jnp.float32) * taps_f[None, :-1, :], axis=1)
    summed = summed + newest.astype(jnp.float32) * taps_f[-1][None, :]
    return jax.nn.silu(summed)


def state_mixer(
    residual,
    mixer_gain,
    proj_gate,
    proj_input,
    proj_write,
    proj_read,
    proj_step,
    step_bias,
    rate_log,
    skip_gain,
    taps_input,
    taps_write,
    taps_read,
    buffer_input,
    buffer_write,
    buffer_read,
    scan_state,
    group_gain,
    proj_output,
):
    full_rows = sent_to_all(residual, "tp").reshape(8 * ROWS, D)
    seq_rows = full_rows.shape[0]
    widened = full_rows.astype(jnp.float32)
    normed = (widened * inverse_rms(widened) * mixer_gain.astype(jnp.float32)[None, :]).astype(
        jnp.bfloat16
    )

    def state_project(weight):
        return jnp.dot(normed, weight, preferred_element_type=jnp.float32).astype(jnp.bfloat16)

    gate_z = state_project(proj_gate)
    input_new = state_project(proj_input)
    write_new = state_project(proj_write)
    read_new = state_project(proj_read)
    step_raw = state_project(proj_step)
    input_conv = short_conv(taps_input, buffer_input, input_new)
    write_conv = short_conv(taps_write, buffer_write, write_new)
    read_conv = short_conv(taps_read, buffer_read, read_new)
    head_count = proj_step.shape[1]
    group_count = proj_write.shape[1] // STATE
    per_group = head_count // group_count
    step = jax.nn.softplus(step_raw.astype(jnp.float32) + step_bias[None, :])
    retain = jnp.exp(-step * jnp.exp(rate_log)[None, :])
    input_heads = input_conv.reshape(seq_rows, group_count, per_group, HEAD_DIM)
    write_groups = write_conv.reshape(seq_rows, group_count, STATE)
    read_groups = read_conv.reshape(seq_rows, group_count, STATE)
    old_state = scan_state.reshape(seq_rows, group_count, per_group, HEAD_DIM, STATE)
    retain_g = retain.reshape(seq_rows, group_count, per_group)
    step_g = step.reshape(seq_rows, group_count, per_group)
    updated = (
        retain_g[..., None, None] * old_state
        + (step_g[..., None] * input_heads)[..., None] * write_groups[:, :, None, None, :]
    )
    head_out = jnp.einsum("bgrpn,bgn->bgrp", updated, read_groups)
    head_out = head_out + skip_gain.reshape(group_count, per_group)[None, :, :, None] * input_heads
    head_short = lax.optimization_barrier(head_out.astype(jnp.bfloat16))
    gated = head_short.astype(jnp.float32).reshape(seq_rows, group_count, per_group * HEAD_DIM)
    gated = gated * jax.nn.silu(
        gate_z.astype(jnp.float32).reshape(seq_rows, group_count, per_group * HEAD_DIM)
    )
    gated = (
        gated
        * inverse_rms(gated)
        * group_gain.astype(jnp.float32).reshape(group_count, per_group * HEAD_DIM)[None]
    )
    gated = gated.reshape(seq_rows, head_count * HEAD_DIM).astype(jnp.bfloat16)
    partial_out = jnp.dot(gated, proj_output, preferred_element_type=jnp.float32).astype(
        jnp.bfloat16
    )
    tiles = lax.all_to_all(partial_out.reshape(8, ROWS, D), "tp", 0, 0, tiled=True)
    mixed = jnp.sum(tiles.astype(jnp.float32), axis=0)
    mixed_rows = (residual.astype(jnp.float32) + mixed).astype(jnp.bfloat16)
    return (mixed_rows, updated.reshape(seq_rows, head_count, HEAD_DIM, STATE))


def per_device(
    residual,
    first_gain,
    first_gate,
    first_lift,
    first_down,
    mixer_gain,
    proj_gate,
    proj_input,
    proj_write,
    proj_read,
    proj_step,
    step_bias,
    rate_log,
    skip_gain,
    taps_input,
    taps_write,
    taps_read,
    buffer_input,
    buffer_write,
    buffer_read,
    scan_state,
    group_gain,
    proj_output,
    second_gain,
    second_gate,
    second_lift,
    second_down,
):
    weights_one = gathered_weights(first_gain, first_gate, first_lift, first_down)
    weights_two = gathered_weights(second_gain, second_gate, second_lift, second_down)
    kv = lax.axis_index("kv")
    kv_size = lax.axis_size("kv")
    both = ("kv", "tp")

    split = residual.reshape(8, ROWS, FEATS)
    tiles = lax.all_to_all(
        jnp.broadcast_to(split[None], (kv_size, 8, ROWS, FEATS)).reshape(-1, ROWS, FEATS),
        both,
        0,
        0,
        tiled=True,
    ).reshape(kv_size, 8, ROWS, FEATS)
    rows = tiles.transpose(0, 2, 1, 3).reshape(kv_size * ROWS, D)
    own_rows = lax.dynamic_slice_in_dim(rows, kv * ROWS, ROWS, 0)
    share = ffn_partial(rows, weights_one)
    share = share.reshape(8, kv_size, ROWS, FEATS).transpose(1, 2, 0, 3)
    share = lax.all_to_all(share.reshape(kv_size, ROWS, D), "kv", 0, 0, tiled=True)
    branch = jnp.sum(share.astype(jnp.float32), axis=0)
    first = (own_rows.astype(jnp.float32) + 0.5 * branch).astype(jnp.bfloat16)

    mixed, state_out = state_mixer(
        first,
        mixer_gain,
        proj_gate,
        proj_input,
        proj_write,
        proj_read,
        proj_step,
        step_bias,
        rate_log,
        skip_gain,
        taps_input,
        taps_write,
        taps_read,
        buffer_input,
        buffer_write,
        buffer_read,
        scan_state,
        group_gain,
        proj_output,
    )

    rows = sent_to_all(mixed, "kv").reshape(kv_size * ROWS, D)
    share = ffn_partial(rows, weights_two)
    share = share.reshape(8, kv_size, ROWS, FEATS).transpose(1, 0, 2, 3)
    mine = (jnp.arange(kv_size) == kv)[:, None, None, None]
    own = 2.0 * mixed.astype(jnp.float32).reshape(ROWS, 8, FEATS).transpose(1, 0, 2)
    share = jnp.where(mine, share.astype(jnp.float32) + own[None], share.astype(jnp.float32))
    share = share.astype(jnp.bfloat16).reshape(-1, ROWS, FEATS)
    share = lax.all_to_all(share, both, 0, 0, tiled=True).reshape(kv_size, 8 * ROWS, FEATS)
    residual_out = (0.5 * jnp.sum(share.astype(jnp.float32), axis=0)).astype(jnp.bfloat16)
    return (residual_out, state_out)


def solution(mesh):
    placed = (
        P("kv", "tp"),
        P("tp"),
        P("tp", "kv"),
        P("tp", "kv"),
        P("kv", "tp"),
        P(),
        P(None, "tp"),
        P(None, "tp"),
        P(None, "tp"),
        P(None, "tp"),
        P(None, "tp"),
        P("tp"),
        P("tp"),
        P("tp"),
        P(None, "tp"),
        P(None, "tp"),
        P(None, "tp"),
        P("kv", None, "tp"),
        P("kv", None, "tp"),
        P("kv", None, "tp"),
        P("kv", "tp", None, None),
        P("tp"),
        P("tp", None),
        P("tp"),
        P("tp", "kv"),
        P("tp", "kv"),
        P("kv", "tp"),
    )
    return jax.shard_map(
        per_device,
        mesh=mesh,
        in_specs=placed,
        out_specs=(P("kv", "tp"), P("kv", "tp", None, None)),
        check_vma=False,
    )
```

```python
import jax
import jax.numpy as jnp
from jax import lax
from jax.experimental import pallas as pl
from jax.experimental.pallas import tpu as pltpu
from jax.sharding import Mesh
from jax.sharding import PartitionSpec as P

D = 2048
HEAD_DIM = 64
STATE = 128
FEATS = 256
HIDDEN = 176
ROWS = 4
Z, Y, TP = 8, 4, 8

KV_AXES = ("z", "y")
TP_AXES = ("x", "core")

norm_eps = 1e-06

by_rows = (((1,), (1,)), ((), ()))


def sent_to_all(array, axis):
    length = lax.axis_size(axis)
    return lax.all_to_all(
        jnp.broadcast_to(array[None], (length, *array.shape)), axis, 0, 0, tiled=True
    )


def inverse_rms(values):
    return lax.rsqrt(jnp.mean(values * values, axis=-1, keepdims=True) + norm_eps)


def weight_share(gain, gate_weight, lift_weight, down_weight):
    gain_f = gain.astype(jnp.float32)[None, :]
    gate_t = (gate_weight.T.astype(jnp.float32) * gain_f).astype(jnp.bfloat16)
    lift_t = (lift_weight.T.astype(jnp.float32) * gain_f).astype(jnp.bfloat16)
    return jnp.concatenate([gate_t, lift_t, down_weight], axis=0)


def hidden_units(normed_ref, weights, rows):
    gate = jnp.zeros((rows, HIDDEN), jnp.float32)
    lift = jnp.zeros((rows, HIDDEN), jnp.float32)
    for u in range(TP):
        block = normed_ref[u]
        gate += lax.dot_general(
            block, weights[u, :HIDDEN], by_rows, preferred_element_type=jnp.float32
        )
        lift += lax.dot_general(
            block, weights[u, HIDDEN : 2 * HIDDEN], by_rows, preferred_element_type=jnp.float32
        )
    return (gate * jax.nn.sigmoid(gate) * lift).astype(jnp.bfloat16)


def first_kernel(rows_ref, weights_ref, out_ref, normed_ref):
    blocks = Z * Y
    total = jnp.zeros((blocks, ROWS, 1), jnp.float32)
    for u in range(TP):
        values = rows_ref[:, u].astype(jnp.float32)
        total += jnp.sum(values * values, axis=-1, keepdims=True)
    factor = lax.rsqrt(total * (1.0 / D) + norm_eps)
    for u in range(TP):
        values = rows_ref[:, u].astype(jnp.float32) * factor
        normed_ref[u] = values.reshape(blocks * ROWS, FEATS).astype(jnp.bfloat16)
    hidden = hidden_units(normed_ref, weights_ref, blocks * ROWS)
    for u in range(TP):
        down = jnp.dot(hidden, weights_ref[u, 2 * HIDDEN :], preferred_element_type=jnp.float32)
        out_ref[:, u] = down.reshape(blocks, ROWS, FEATS).astype(jnp.bfloat16)


def first_partial(rows, weights):
    return pl.pallas_call(
        first_kernel,
        out_shape=jax.ShapeDtypeStruct(rows.shape, jnp.bfloat16),
        scratch_shapes=[pltpu.VMEM((TP, Z * Y * ROWS, FEATS), jnp.bfloat16)],
        name="first_ffn",
    )(rows, weights)


def second_kernel(place_ref, rows_ref, weights_ref, out_ref, normed_ref, sum_ref):
    step = pl.program_id(0)
    rows = Z * ROWS

    @pl.when(step == 0)
    def _():
        values = rows_ref[...].astype(jnp.float32)
        factor = lax.rsqrt(jnp.sum(values * values, axis=-1, keepdims=True) * (1.0 / D) + norm_eps)
        row = lax.broadcasted_iota(jnp.int32, (rows, 1), 0)
        own = jnp.where(row // ROWS == place_ref[0], 2.0, 0.0)
        for u in range(TP):
            block = values[:, u * FEATS : (u + 1) * FEATS]
            normed_ref[u] = (block * factor).astype(jnp.bfloat16)
            sum_ref[u] = block * own

    hidden = hidden_units(normed_ref, weights_ref.at[0], rows)
    for u in range(TP):
        down = jnp.dot(hidden, weights_ref[0, u, 2 * HIDDEN :], preferred_element_type=jnp.float32)
        sum_ref[u] = sum_ref[u] + down

    @pl.when(step == pl.num_programs(0) - 1)
    def _():
        out_ref[...] = sum_ref[...].reshape(TP, Z, ROWS, FEATS).astype(jnp.bfloat16)


def second_partial(rows, weights):
    place = lax.axis_index("z").astype(jnp.int32).reshape(1)
    return pl.pallas_call(
        second_kernel,
        grid=(Y,),
        out_shape=jax.ShapeDtypeStruct((TP, Z, ROWS, FEATS), jnp.bfloat16),
        in_specs=[
            pl.BlockSpec(memory_space=pltpu.SMEM),
            pl.BlockSpec(rows.shape, lambda i: (0, 0)),
            pl.BlockSpec((1, TP, 3 * HIDDEN, FEATS), lambda i: (i, 0, 0, 0)),
        ],
        out_specs=pl.BlockSpec((TP, Z, ROWS, FEATS), lambda i: (0, 0, 0, 0)),
        scratch_shapes=[
            pltpu.VMEM((TP, Z * ROWS, FEATS), jnp.bfloat16),
            pltpu.VMEM((TP, Z * ROWS, FEATS), jnp.float32),
        ],
        name="second_ffn",
    )(place, rows, weights)


def short_conv(tap_weights, buffer, newest):
    taps_f = tap_weights.astype(jnp.float32)
    summed = jnp.sum(buffer.astype(jnp.float32) * taps_f[None, :-1, :], axis=1)
    summed = summed + newest.astype(jnp.float32) * taps_f[-1][None, :]
    return jax.nn.silu(summed)


def state_mixer(
    residual,
    mixer_gain,
    proj_gate,
    proj_input,
    proj_write,
    proj_read,
    proj_step,
    step_bias,
    rate_log,
    skip_gain,
    taps_input,
    taps_write,
    taps_read,
    buffer_input,
    buffer_write,
    buffer_read,
    scan_state,
    group_gain,
    proj_output,
):
    full_rows = sent_to_all(residual, TP_AXES).transpose(0, 2, 1, 3).reshape(TP * ROWS, D)
    seq_rows = full_rows.shape[0]
    widened = full_rows.astype(jnp.float32)
    normed = (widened * inverse_rms(widened) * mixer_gain.astype(jnp.float32)[None, :]).astype(
        jnp.bfloat16
    )

    def state_project(weight):
        return jnp.dot(normed, weight, preferred_element_type=jnp.float32).astype(jnp.bfloat16)

    gate_z = state_project(proj_gate)
    input_new = state_project(proj_input)
    write_new = state_project(proj_write)
    read_new = state_project(proj_read)
    step_raw = state_project(proj_step)
    input_conv = short_conv(taps_input, buffer_input, input_new)
    write_conv = short_conv(taps_write, buffer_write, write_new)
    read_conv = short_conv(taps_read, buffer_read, read_new)
    head_count = proj_step.shape[1]
    group_count = proj_write.shape[1] // STATE
    per_group = head_count // group_count
    step = jax.nn.softplus(step_raw.astype(jnp.float32) + step_bias[None, :])
    retain = jnp.exp(-step * jnp.exp(rate_log)[None, :])
    input_heads = input_conv.reshape(seq_rows, group_count, per_group, HEAD_DIM)
    write_groups = write_conv.reshape(seq_rows, group_count, STATE)
    read_groups = read_conv.reshape(seq_rows, group_count, STATE)
    old_state = scan_state.reshape(seq_rows, group_count, per_group, HEAD_DIM, STATE)
    retain_g = retain.reshape(seq_rows, group_count, per_group)
    step_g = step.reshape(seq_rows, group_count, per_group)
    updated = (
        retain_g[..., None, None] * old_state
        + (step_g[..., None] * input_heads)[..., None] * write_groups[:, :, None, None, :]
    )
    head_out = jnp.einsum("bgrpn,bgn->bgrp", updated, read_groups)
    head_out = head_out + skip_gain.reshape(group_count, per_group)[None, :, :, None] * input_heads
    head_short = lax.optimization_barrier(head_out.astype(jnp.bfloat16))
    gated = head_short.astype(jnp.float32).reshape(seq_rows, group_count, per_group * HEAD_DIM)
    gated = gated * jax.nn.silu(
        gate_z.astype(jnp.float32).reshape(seq_rows, group_count, per_group * HEAD_DIM)
    )
    gated = (
        gated
        * inverse_rms(gated)
        * group_gain.astype(jnp.float32).reshape(group_count, per_group * HEAD_DIM)[None]
    )
    gated = gated.reshape(seq_rows, head_count * HEAD_DIM).astype(jnp.bfloat16)
    partial_out = jnp.dot(gated, proj_output, preferred_element_type=jnp.float32).astype(
        jnp.bfloat16
    )
    tiles = lax.all_to_all(partial_out.reshape(TP, ROWS, D), TP_AXES, 0, 0, tiled=True)
    mixed = jnp.sum(tiles.astype(jnp.float32), axis=0)
    own = residual.astype(jnp.float32).transpose(1, 0, 2).reshape(ROWS, D)
    mixed_rows = (own + mixed).astype(jnp.bfloat16)
    return (mixed_rows, updated.reshape(seq_rows, head_count, HEAD_DIM, STATE))


def per_device(
    residual,
    first_gain,
    first_gate,
    first_lift,
    first_down,
    mixer_gain,
    proj_gate,
    proj_input,
    proj_write,
    proj_read,
    proj_step,
    step_bias,
    rate_log,
    skip_gain,
    taps_input,
    taps_write,
    taps_read,
    buffer_input,
    buffer_write,
    buffer_read,
    scan_state,
    group_gain,
    proj_output,
    second_gain,
    second_gate,
    second_lift,
    second_down,
):
    weights_one = lax.all_gather(
        weight_share(first_gain, first_gate, first_lift, first_down), TP_AXES
    )
    weights_two = lax.all_gather(
        weight_share(second_gain, second_gate, second_lift, second_down), ("y", *TP_AXES)
    ).reshape(Y, TP, 3 * HIDDEN, FEATS)
    everyone = (*KV_AXES, *TP_AXES)

    split = residual.reshape(TP, ROWS, FEATS)
    tiles = lax.all_to_all(
        jnp.broadcast_to(split[None], (Z * Y, TP, ROWS, FEATS)).reshape(-1, ROWS, FEATS),
        everyone,
        0,
        0,
        tiled=True,
    ).reshape(Z * Y, TP, ROWS, FEATS)
    own_rows = lax.dynamic_index_in_dim(tiles, lax.axis_index(KV_AXES), 0, keepdims=False)
    share = first_partial(tiles, weights_one)
    share = lax.all_to_all(share, KV_AXES, 0, 0, tiled=True)
    branch = jnp.sum(share.astype(jnp.float32), axis=0)
    first = (own_rows.astype(jnp.float32) + 0.5 * branch).astype(jnp.bfloat16)

    mixed, state_out = state_mixer(
        first,
        mixer_gain,
        proj_gate,
        proj_input,
        proj_write,
        proj_read,
        proj_step,
        step_bias,
        rate_log,
        skip_gain,
        taps_input,
        taps_write,
        taps_read,
        buffer_input,
        buffer_write,
        buffer_read,
        scan_state,
        group_gain,
        proj_output,
    )

    rows = sent_to_all(mixed, "z").reshape(Z * ROWS, D)
    share = second_partial(rows, weights_two).transpose(1, 0, 2, 3)
    share = lax.all_to_all(
        share.reshape(-1, ROWS, FEATS), ("z", *TP_AXES), 0, 0, tiled=True
    ).reshape(Z, TP * ROWS, FEATS)
    residual_out = (0.5 * jnp.sum(share.astype(jnp.float32), axis=0)).astype(jnp.bfloat16)
    return (residual_out, state_out)


def solution(mesh):
    mesh = Mesh(mesh.devices.reshape(Z, Y, TP // 2, 2), (*KV_AXES, *TP_AXES))
    placed = (
        P(KV_AXES, TP_AXES),
        P(TP_AXES),
        P(TP_AXES, KV_AXES),
        P(TP_AXES, KV_AXES),
        P(KV_AXES, TP_AXES),
        P(),
        P(None, TP_AXES),
        P(None, TP_AXES),
        P(None, TP_AXES),
        P(None, TP_AXES),
        P(None, TP_AXES),
        P(TP_AXES),
        P(TP_AXES),
        P(TP_AXES),
        P(None, TP_AXES),
        P(None, TP_AXES),
        P(None, TP_AXES),
        P(KV_AXES, None, TP_AXES),
        P(KV_AXES, None, TP_AXES),
        P(KV_AXES, None, TP_AXES),
        P(KV_AXES, TP_AXES, None, None),
        P(TP_AXES),
        P(TP_AXES, None),
        P(TP_AXES),
        P(TP_AXES, KV_AXES),
        P(TP_AXES, KV_AXES),
        P(KV_AXES, TP_AXES),
    )
    return jax.shard_map(
        per_device,
        mesh=mesh,
        in_specs=placed,
        out_specs=(P(KV_AXES, TP_AXES), P(KV_AXES, TP_AXES, None, None)),
        check_vma=False,
    )
```

```python
import jax
import jax.numpy as jnp
from jax import lax
from jax.experimental import pallas as pl
from jax.experimental.pallas import tpu as pltpu
from jax.sharding import Mesh
from jax.sharding import PartitionSpec as P

D = 2048
HEAD_DIM = 64
STATE = 128
FEATS = 256
HIDDEN = 176
ROWS = 4
Z, Y, TP = 8, 4, 8

KV_AXES = ("z", "y")
TP_AXES = ("x", "core")

norm_eps = 1e-06

by_rows = (((1,), (1,)), ((), ()))


def sent_to_all(array, axis):
    length = lax.axis_size(axis)
    return lax.all_to_all(
        jnp.broadcast_to(array[None], (length, *array.shape)), axis, 0, 0, tiled=True
    )


def inverse_rms(values):
    return lax.rsqrt(jnp.mean(values * values, axis=-1, keepdims=True) + norm_eps)


def share_kernel(*refs):
    for gain, gate, lift, down, out in (refs[0:4] + refs[8:9], refs[4:8] + refs[9:10]):
        gain_f = gain[...].astype(jnp.float32)
        out[:HIDDEN] = (gate[...].astype(jnp.float32) * gain_f).astype(jnp.bfloat16)
        out[HIDDEN : 2 * HIDDEN] = (lift[...].astype(jnp.float32) * gain_f).astype(jnp.bfloat16)
        out[2 * HIDDEN :] = down[...]


def weight_shares(*sets):
    operands = []
    for gain, gate_weight, lift_weight, down_weight in sets:
        operands += [gain.reshape(1, FEATS), gate_weight.T, lift_weight.T, down_weight]
    return pl.pallas_call(
        share_kernel,
        out_shape=[jax.ShapeDtypeStruct((3 * HIDDEN, FEATS), jnp.bfloat16)] * 2,
        name="shares",
    )(*operands)


def hidden_units(normed_ref, weights, rows):
    gate = jnp.zeros((rows, HIDDEN), jnp.float32)
    lift = jnp.zeros((rows, HIDDEN), jnp.float32)
    for u in range(TP):
        block = normed_ref[u]
        gate += lax.dot_general(
            block, weights[u, :HIDDEN], by_rows, preferred_element_type=jnp.float32
        )
        lift += lax.dot_general(
            block, weights[u, HIDDEN : 2 * HIDDEN], by_rows, preferred_element_type=jnp.float32
        )
    return (gate * jax.nn.sigmoid(gate) * lift).astype(jnp.bfloat16)


def first_kernel(rows_ref, weights_ref, out_ref, normed_ref):
    blocks = Z * Y
    total = jnp.zeros((blocks, ROWS, 1), jnp.float32)
    for u in range(TP):
        values = rows_ref[:, u].astype(jnp.float32)
        total += jnp.sum(values * values, axis=-1, keepdims=True)
    factor = lax.rsqrt(total * (1.0 / D) + norm_eps)
    for u in range(TP):
        values = rows_ref[:, u].astype(jnp.float32) * factor
        normed_ref[u] = values.reshape(blocks * ROWS, FEATS).astype(jnp.bfloat16)
    hidden = hidden_units(normed_ref, weights_ref, blocks * ROWS)
    for u in range(TP):
        down = jnp.dot(hidden, weights_ref[u, 2 * HIDDEN :], preferred_element_type=jnp.float32)
        out_ref[:, u] = down.reshape(blocks, ROWS, FEATS).astype(jnp.bfloat16)


def first_partial(rows, weights):
    return pl.pallas_call(
        first_kernel,
        out_shape=jax.ShapeDtypeStruct(rows.shape, jnp.bfloat16),
        scratch_shapes=[pltpu.VMEM((TP, Z * Y * ROWS, FEATS), jnp.bfloat16)],
        name="first_ffn",
    )(rows, weights)


def second_kernel(place_ref, rows_ref, weights_ref, out_ref, normed_ref, sum_ref):
    step = pl.program_id(0)
    rows = Z * ROWS

    @pl.when(step == 0)
    def _():
        values = rows_ref[...].astype(jnp.float32).reshape(rows, D)
        factor = lax.rsqrt(jnp.sum(values * values, axis=-1, keepdims=True) * (1.0 / D) + norm_eps)
        row = lax.broadcasted_iota(jnp.int32, (rows, 1), 0)
        own = jnp.where(row // ROWS == place_ref[0], 2.0, 0.0)
        for u in range(TP):
            block = values[:, u * FEATS : (u + 1) * FEATS]
            normed_ref[u] = (block * factor).astype(jnp.bfloat16)
            sum_ref[u] = block * own

    hidden = hidden_units(normed_ref, weights_ref.at[0], rows)
    for u in range(TP):
        down = jnp.dot(hidden, weights_ref[0, u, 2 * HIDDEN :], preferred_element_type=jnp.float32)
        sum_ref[u] = sum_ref[u] + down

    @pl.when(step == pl.num_programs(0) - 1)
    def _():
        for u in range(TP):
            out_ref[:, u] = sum_ref[u].reshape(Z, ROWS, FEATS).astype(jnp.bfloat16)


def second_partial(rows, weights):
    place = lax.axis_index("z").astype(jnp.int32).reshape(1)
    return pl.pallas_call(
        second_kernel,
        grid=(Y,),
        out_shape=jax.ShapeDtypeStruct((Z, TP, ROWS, FEATS), jnp.bfloat16),
        in_specs=[
            pl.BlockSpec(memory_space=pltpu.SMEM),
            pl.BlockSpec(rows.shape, lambda i: (0, 0, 0)),
            pl.BlockSpec((1, TP, 3 * HIDDEN, FEATS), lambda i: (i, 0, 0, 0)),
        ],
        out_specs=pl.BlockSpec((Z, TP, ROWS, FEATS), lambda i: (0, 0, 0, 0)),
        scratch_shapes=[
            pltpu.VMEM((TP, Z * ROWS, FEATS), jnp.bfloat16),
            pltpu.VMEM((TP, Z * ROWS, FEATS), jnp.float32),
        ],
        name="second_ffn",
    )(place, rows, weights)


def conv_silu(newest, buffer_ref, taps_ref):
    taps = taps_ref[...].astype(jnp.float32)
    summed = newest.astype(jnp.float32) * taps[3:4]
    for k in range(3):
        summed += buffer_ref[k].astype(jnp.float32) * taps[k : k + 1]
    return summed * jax.nn.sigmoid(summed)


SEQS = TP * ROWS
BLOCK = 8
CHANNELS = 256
PER_DEVICE = 4


def mixer_kernel(
    rows_ref,
    gain_ref,
    gate_ref,
    input_ref,
    write_ref,
    read_ref,
    step_ref,
    bias_ref,
    rate_ref,
    skip_ref,
    taps_input_ref,
    taps_write_ref,
    taps_read_ref,
    buffer_input_ref,
    buffer_write_ref,
    buffer_read_ref,
    state_ref,
    group_ref,
    output_ref,
    mixed_ref,
    new_state_ref,
    normed_ref,
    gate_z_ref,
    xc_ref,
    added_ref,
    retain_ref,
    bc_ref,
    rc_ref,
    out_cols_ref,
):
    i = pl.program_id(0)

    @pl.when(i == 0)
    def _():
        total = jnp.zeros((TP, ROWS, 1), jnp.float32)
        for u in range(TP):
            values = rows_ref[:, u].astype(jnp.float32)
            total += jnp.sum(values * values, axis=-1, keepdims=True)
        factor = lax.rsqrt(total * (1.0 / D) + norm_eps)
        for u in range(TP):
            values = (rows_ref[:, u].astype(jnp.float32) * factor).reshape(SEQS, FEATS)
            cols = slice(u * FEATS, (u + 1) * FEATS)
            gain = gain_ref[:, cols].astype(jnp.float32)
            normed_ref[:, cols] = (values * gain).astype(jnp.bfloat16)
        normed = normed_ref[...]

        def project(weight_ref):
            return jnp.dot(normed, weight_ref[...], preferred_element_type=jnp.float32).astype(
                jnp.bfloat16
            )

        gate_z_ref[...] = project(gate_ref)
        step_raw = lax.dot_general(
            normed, step_ref[...], by_rows, preferred_element_type=jnp.float32
        ).astype(jnp.bfloat16)
        xc = conv_silu(project(input_ref), buffer_input_ref, taps_input_ref)
        bc_ref[...] = conv_silu(project(write_ref), buffer_write_ref, taps_write_ref)
        rc_ref[...] = conv_silu(project(read_ref), buffer_read_ref, taps_read_ref)
        xc_ref[...] = xc
        step = jax.nn.softplus(step_raw.astype(jnp.float32) + bias_ref[...])
        retain = jnp.exp(-step * jnp.exp(rate_ref[...]))
        head = lax.broadcasted_iota(jnp.int32, (SEQS, CHANNELS), 1) // HEAD_DIM
        step_wide = jnp.zeros((SEQS, CHANNELS), jnp.float32)
        retain_wide = jnp.zeros((SEQS, CHANNELS), jnp.float32)
        for h in range(PER_DEVICE):
            step_wide = jnp.where(head == h, step[:, h : h + 1], step_wide)
            retain_wide = jnp.where(head == h, retain[:, h : h + 1], retain_wide)
        added = (step_wide * xc).T
        retain_cols = retain_wide.T
        for s in range(SEQS // BLOCK):
            added_ref[s] = added[:, s * BLOCK : (s + 1) * BLOCK]
            retain_ref[s] = retain_cols[:, s * BLOCK : (s + 1) * BLOCK]

    added = added_ref[i]
    retain = retain_ref[i]
    writes = bc_ref[pl.ds(pl.multiple_of(i * BLOCK, BLOCK), BLOCK)]
    reads = rc_ref[pl.ds(pl.multiple_of(i * BLOCK, BLOCK), BLOCK)]
    column = lax.broadcasted_iota(jnp.int32, (CHANNELS, BLOCK), 1)
    cols = jnp.zeros((CHANNELS, BLOCK), jnp.float32)
    for b in range(BLOCK):
        old = state_ref[b].reshape(CHANNELS, STATE)
        new = retain[:, b : b + 1] * old + added[:, b : b + 1] * writes[b : b + 1]
        new_state_ref[b] = new.reshape(PER_DEVICE, HEAD_DIM, STATE)
        read = jnp.sum(new * reads[b : b + 1], axis=-1, keepdims=True)
        cols = jnp.where(column == b, read, cols)
    out_cols_ref[i] = cols

    @pl.when(i == pl.num_programs(0) - 1)
    def _():
        cols = jnp.concatenate([out_cols_ref[s] for s in range(SEQS // BLOCK)], axis=1)
        head = lax.broadcasted_iota(jnp.int32, (1, CHANNELS), 1) // HEAD_DIM
        skip = jnp.zeros((1, CHANNELS), jnp.float32)
        for h in range(PER_DEVICE):
            skip = jnp.where(head == h, skip_ref[:, h : h + 1], skip)
        head_out = (cols.T + skip * xc_ref[...]).astype(jnp.bfloat16).astype(jnp.float32)
        gate_z = gate_z_ref[...].astype(jnp.float32)
        gated = head_out * (gate_z * jax.nn.sigmoid(gate_z))
        gated = gated * inverse_rms(gated) * group_ref[...].astype(jnp.float32)
        part = jnp.dot(
            gated.astype(jnp.bfloat16), output_ref[...], preferred_element_type=jnp.float32
        )
        mixed_ref[...] = part.reshape(TP, ROWS, D).astype(jnp.bfloat16)


def state_mixer(first, small, buffers, scan_state, group_gain, proj_output):
    rows = sent_to_all(first, TP_AXES)
    operands = [rows, *small, *[b.transpose(1, 0, 2) for b in buffers]]
    operands += [scan_state, group_gain.reshape(1, CHANNELS), proj_output]
    specs = [pl.BlockSpec(o.shape, lambda i, n=o.ndim: (0,) * n) for o in operands]
    state_spec = pl.BlockSpec((BLOCK, PER_DEVICE, HEAD_DIM, STATE), lambda i: (i, 0, 0, 0))
    specs[-3] = state_spec
    blocks = SEQS // BLOCK
    partial_out, state_out = pl.pallas_call(
        mixer_kernel,
        grid=(blocks,),
        out_shape=[
            jax.ShapeDtypeStruct((TP, ROWS, D), jnp.bfloat16),
            jax.ShapeDtypeStruct(scan_state.shape, jnp.float32),
        ],
        in_specs=specs,
        out_specs=[pl.BlockSpec((TP, ROWS, D), lambda i: (0, 0, 0)), state_spec],
        scratch_shapes=[
            pltpu.VMEM((SEQS, D), jnp.bfloat16),
            pltpu.VMEM((SEQS, CHANNELS), jnp.bfloat16),
            pltpu.VMEM((SEQS, CHANNELS), jnp.float32),
            pltpu.VMEM((blocks, CHANNELS, BLOCK), jnp.float32),
            pltpu.VMEM((blocks, CHANNELS, BLOCK), jnp.float32),
            pltpu.VMEM((SEQS, STATE), jnp.float32),
            pltpu.VMEM((SEQS, STATE), jnp.float32),
            pltpu.VMEM((blocks, CHANNELS, BLOCK), jnp.float32),
        ],
        name="mixer",
    )(*operands)
    tiles = lax.all_to_all(partial_out, TP_AXES, 0, 0, tiled=True)
    mixed = jnp.sum(tiles.astype(jnp.float32), axis=0)
    own = first.astype(jnp.float32).transpose(1, 0, 2).reshape(ROWS, D)
    return ((own + mixed).astype(jnp.bfloat16), state_out)


def per_device(
    residual,
    first_gain,
    first_gate,
    first_lift,
    first_down,
    mixer_gain,
    proj_gate,
    proj_input,
    proj_write,
    proj_read,
    proj_step,
    step_bias,
    rate_log,
    skip_gain,
    taps_input,
    taps_write,
    taps_read,
    buffer_input,
    buffer_write,
    buffer_read,
    scan_state,
    group_gain,
    proj_output,
    second_gain,
    second_gate,
    second_lift,
    second_down,
):
    share_one, share_two = weight_shares(
        (first_gain, first_gate, first_lift, first_down),
        (second_gain, second_gate, second_lift, second_down),
    )
    weights_one = lax.all_gather(share_one, TP_AXES)
    weights_two = lax.all_gather(share_two, ("y", *TP_AXES)).reshape(
        Y, TP, 3 * HIDDEN, FEATS
    )

    split = residual.reshape(TP, ROWS, FEATS)
    tiles = lax.all_to_all(
        jnp.broadcast_to(split[None], (Z, TP, ROWS, FEATS)).reshape(-1, ROWS, FEATS),
        ("z", *TP_AXES),
        0,
        0,
        tiled=True,
    )
    tiles = sent_to_all(tiles, "y").reshape(Y * Z, TP, ROWS, FEATS)
    own_rows = lax.dynamic_index_in_dim(tiles, lax.axis_index(("y", "z")), 0, keepdims=False)
    share = first_partial(tiles, weights_one)
    share = lax.all_to_all(share, ("y", "z"), 0, 0, tiled=True)
    branch = jnp.sum(share.astype(jnp.float32), axis=0)
    first = (own_rows.astype(jnp.float32) + 0.5 * branch).astype(jnp.bfloat16)

    mixed, state_out = state_mixer(
        first,
        (
            mixer_gain.reshape(1, D),
            proj_gate,
            proj_input,
            proj_write,
            proj_read,
            proj_step.T,
            step_bias.reshape(1, -1),
            rate_log.reshape(1, -1),
            skip_gain.reshape(1, -1),
            taps_input,
            taps_write,
            taps_read,
        ),
        (buffer_input, buffer_write, buffer_read),
        scan_state,
        group_gain,
        proj_output,
    )

    share = second_partial(sent_to_all(mixed, "z"), weights_two)
    share = lax.all_to_all(
        share.reshape(-1, ROWS, FEATS), ("z", *TP_AXES), 0, 0, tiled=True
    ).reshape(Z, TP * ROWS, FEATS)
    residual_out = (0.5 * jnp.sum(share.astype(jnp.float32), axis=0)).astype(jnp.bfloat16)
    return (residual_out, state_out)


def solution(mesh):
    mesh = Mesh(mesh.devices.reshape(Z, Y, TP // 2, 2), (*KV_AXES, *TP_AXES))
    placed = (
        P(KV_AXES, TP_AXES),
        P(TP_AXES),
        P(TP_AXES, KV_AXES),
        P(TP_AXES, KV_AXES),
        P(KV_AXES, TP_AXES),
        P(),
        P(None, TP_AXES),
        P(None, TP_AXES),
        P(None, TP_AXES),
        P(None, TP_AXES),
        P(None, TP_AXES),
        P(TP_AXES),
        P(TP_AXES),
        P(TP_AXES),
        P(None, TP_AXES),
        P(None, TP_AXES),
        P(None, TP_AXES),
        P(KV_AXES, None, TP_AXES),
        P(KV_AXES, None, TP_AXES),
        P(KV_AXES, None, TP_AXES),
        P(KV_AXES, TP_AXES, None, None),
        P(TP_AXES),
        P(TP_AXES, None),
        P(TP_AXES),
        P(TP_AXES, KV_AXES),
        P(TP_AXES, KV_AXES),
        P(KV_AXES, TP_AXES),
    )
    return jax.shard_map(
        per_device,
        mesh=mesh,
        in_specs=placed,
        out_specs=(P(KV_AXES, TP_AXES), P(KV_AXES, TP_AXES, None, None)),
        check_vma=False,
    )
```

```python
import jax
import jax.numpy as jnp
from jax import lax
from jax.experimental import pallas as pl
from jax.experimental.pallas import tpu as pltpu
from jax.sharding import Mesh
from jax.sharding import PartitionSpec as P

D = 2048
HEAD_DIM = 64
STATE = 128
FEATS = 256
HIDDEN = 176
ROWS = 4
Z, Y, TP = 8, 4, 8

KV_AXES = ("z", "y")
TP_AXES = ("x", "core")

norm_eps = 1e-06

by_rows = (((1,), (1,)), ((), ()))


def sent_to_all(array, axis):
    length = lax.axis_size(axis)
    return lax.all_to_all(
        jnp.broadcast_to(array[None], (length, *array.shape)), axis, 0, 0, tiled=True
    )


def inverse_rms(values):
    return lax.rsqrt(jnp.mean(values * values, axis=-1, keepdims=True) + norm_eps)


def share_kernel(*refs):
    for gain, gate, lift, down, out in (refs[0:4] + refs[8:9], refs[4:8] + refs[9:10]):
        gain_f = gain[...].astype(jnp.float32).reshape(1, FEATS)
        out[:HIDDEN] = (gate[...].astype(jnp.float32) * gain_f).astype(jnp.bfloat16)
        out[HIDDEN : 2 * HIDDEN] = (lift[...].astype(jnp.float32) * gain_f).astype(jnp.bfloat16)
        out[2 * HIDDEN :] = down[...]


def weight_shares(*sets):
    operands = []
    for gain, gate_weight, lift_weight, down_weight in sets:
        operands += [gain, gate_weight.T, lift_weight.T, down_weight]
    return pl.pallas_call(
        share_kernel,
        out_shape=[jax.ShapeDtypeStruct((3 * HIDDEN, FEATS), jnp.bfloat16)] * 2,
        compiler_params=pltpu.CompilerParams(vmem_limit_bytes=24 << 20),
        name="shares",
    )(*operands)


def hidden_units(normed_ref, weights, rows):
    gate = jnp.zeros((rows, HIDDEN), jnp.float32)
    lift = jnp.zeros((rows, HIDDEN), jnp.float32)
    for u in range(TP):
        block = normed_ref[u]
        gate += lax.dot_general(
            block, weights[u, :HIDDEN], by_rows, preferred_element_type=jnp.float32
        )
        lift += lax.dot_general(
            block, weights[u, HIDDEN : 2 * HIDDEN], by_rows, preferred_element_type=jnp.float32
        )
    return (gate * jax.nn.sigmoid(gate) * lift).astype(jnp.bfloat16)


def first_kernel(rows_ref, weights_ref, out_ref, normed_ref):
    blocks = Z * Y
    total = jnp.zeros((blocks, ROWS, 1), jnp.float32)
    for u in range(TP):
        values = rows_ref[:, u].astype(jnp.float32)
        total += jnp.sum(values * values, axis=-1, keepdims=True)
    factor = lax.rsqrt(total * (1.0 / D) + norm_eps)
    for u in range(TP):
        values = rows_ref[:, u].astype(jnp.float32) * factor
        normed_ref[u] = values.reshape(blocks * ROWS, FEATS).astype(jnp.bfloat16)
    hidden = hidden_units(normed_ref, weights_ref, blocks * ROWS)
    for u in range(TP):
        down = jnp.dot(hidden, weights_ref[u, 2 * HIDDEN :], preferred_element_type=jnp.float32)
        out_ref[:, u] = down.reshape(blocks, ROWS, FEATS).astype(jnp.bfloat16)


def first_partial(rows, weights):
    return pl.pallas_call(
        first_kernel,
        out_shape=jax.ShapeDtypeStruct(rows.shape, jnp.bfloat16),
        scratch_shapes=[pltpu.VMEM((TP, Z * Y * ROWS, FEATS), jnp.bfloat16)],
        compiler_params=pltpu.CompilerParams(vmem_limit_bytes=24 << 20),
        name="first_ffn",
    )(rows, weights)


def second_kernel(place_ref, rows_ref, weights_ref, out_ref, normed_ref, sum_ref):
    step = pl.program_id(0)
    rows = Z * ROWS

    @pl.when(step == 0)
    def _():
        values = rows_ref[...].astype(jnp.float32).reshape(rows, D)
        factor = lax.rsqrt(jnp.sum(values * values, axis=-1, keepdims=True) * (1.0 / D) + norm_eps)
        row = lax.broadcasted_iota(jnp.int32, (rows, 1), 0)
        own = jnp.where(row // ROWS == place_ref[0], 2.0, 0.0)
        for u in range(TP):
            block = values[:, u * FEATS : (u + 1) * FEATS]
            normed_ref[u] = (block * factor).astype(jnp.bfloat16)
            sum_ref[u] = block * own

    hidden = hidden_units(normed_ref, weights_ref.at[0], rows)
    for u in range(TP):
        down = jnp.dot(hidden, weights_ref[0, u, 2 * HIDDEN :], preferred_element_type=jnp.float32)
        sum_ref[u] = sum_ref[u] + down

    @pl.when(step == pl.num_programs(0) - 1)
    def _():
        for u in range(TP):
            out_ref[:, u] = sum_ref[u].reshape(Z, ROWS, FEATS).astype(jnp.bfloat16)


def second_partial(rows, weights):
    place = lax.axis_index("z").astype(jnp.int32).reshape(1)
    return pl.pallas_call(
        second_kernel,
        grid=(Y,),
        out_shape=jax.ShapeDtypeStruct((Z, TP, ROWS, FEATS), jnp.bfloat16),
        in_specs=[
            pl.BlockSpec(memory_space=pltpu.SMEM),
            pl.BlockSpec(rows.shape, lambda i: (0, 0, 0)),
            pl.BlockSpec((1, TP, 3 * HIDDEN, FEATS), lambda i: (i, 0, 0, 0)),
        ],
        out_specs=pl.BlockSpec((Z, TP, ROWS, FEATS), lambda i: (0, 0, 0, 0)),
        scratch_shapes=[
            pltpu.VMEM((TP, Z * ROWS, FEATS), jnp.bfloat16),
            pltpu.VMEM((TP, Z * ROWS, FEATS), jnp.float32),
        ],
        name="second_ffn",
    )(place, rows, weights)


def conv_silu(newest, buffer_ref, taps_ref):
    taps = taps_ref[...].astype(jnp.float32)
    summed = newest.astype(jnp.float32) * taps[3:4]
    for k in range(3):
        summed += buffer_ref[k].astype(jnp.float32) * taps[k : k + 1]
    return summed * jax.nn.sigmoid(summed)


SEQS = TP * ROWS
BLOCK = 8
CHANNELS = 256
PER_DEVICE = 4


def mixer_kernel(
    rows_ref,
    gain_ref,
    gate_ref,
    input_ref,
    write_ref,
    read_ref,
    step_ref,
    bias_ref,
    rate_ref,
    skip_ref,
    taps_input_ref,
    taps_write_ref,
    taps_read_ref,
    buffer_input_ref,
    buffer_write_ref,
    buffer_read_ref,
    state_ref,
    group_ref,
    output_ref,
    mixed_ref,
    new_state_ref,
    normed_ref,
    gate_z_ref,
    xc_ref,
    added_ref,
    retain_ref,
    bc_ref,
    rc_ref,
    out_cols_ref,
):
    i = pl.program_id(0)

    @pl.when(i == 0)
    def _():
        total = jnp.zeros((TP, ROWS, 1), jnp.float32)
        for u in range(TP):
            values = rows_ref[:, u].astype(jnp.float32)
            total += jnp.sum(values * values, axis=-1, keepdims=True)
        factor = lax.rsqrt(total * (1.0 / D) + norm_eps)
        for u in range(TP):
            values = (rows_ref[:, u].astype(jnp.float32) * factor).reshape(SEQS, FEATS)
            cols = slice(u * FEATS, (u + 1) * FEATS)
            gain = gain_ref[cols].astype(jnp.float32).reshape(1, FEATS)
            normed_ref[:, cols] = (values * gain).astype(jnp.bfloat16)
        normed = normed_ref[...]

        def project(weight_ref):
            return jnp.dot(normed, weight_ref[...], preferred_element_type=jnp.float32).astype(
                jnp.bfloat16
            )

        gate_z_ref[...] = project(gate_ref)
        step_raw = lax.dot_general(
            normed, step_ref[...], by_rows, preferred_element_type=jnp.float32
        ).astype(jnp.bfloat16)
        xc = conv_silu(project(input_ref), buffer_input_ref, taps_input_ref)
        bc_ref[...] = conv_silu(project(write_ref), buffer_write_ref, taps_write_ref)
        rc_ref[...] = conv_silu(project(read_ref), buffer_read_ref, taps_read_ref)
        xc_ref[...] = xc
        step = jax.nn.softplus(step_raw.astype(jnp.float32) + bias_ref[...].reshape(1, PER_DEVICE))
        retain = jnp.exp(-step * jnp.exp(rate_ref[...].reshape(1, PER_DEVICE)))
        head = lax.broadcasted_iota(jnp.int32, (SEQS, CHANNELS), 1) // HEAD_DIM
        step_wide = jnp.zeros((SEQS, CHANNELS), jnp.float32)
        retain_wide = jnp.zeros((SEQS, CHANNELS), jnp.float32)
        for h in range(PER_DEVICE):
            step_wide = jnp.where(head == h, step[:, h : h + 1], step_wide)
            retain_wide = jnp.where(head == h, retain[:, h : h + 1], retain_wide)
        added = (step_wide * xc).T
        retain_cols = retain_wide.T
        for s in range(SEQS // BLOCK):
            added_ref[s] = added[:, s * BLOCK : (s + 1) * BLOCK]
            retain_ref[s] = retain_cols[:, s * BLOCK : (s + 1) * BLOCK]

    added = added_ref[i]
    retain = retain_ref[i]
    writes = bc_ref[pl.ds(pl.multiple_of(i * BLOCK, BLOCK), BLOCK)]
    reads = rc_ref[pl.ds(pl.multiple_of(i * BLOCK, BLOCK), BLOCK)].astype(jnp.bfloat16)
    column = lax.broadcasted_iota(jnp.int32, (CHANNELS, BLOCK), 1)
    cols = jnp.zeros((CHANNELS, BLOCK), jnp.float32)
    for b in range(BLOCK):
        new = []
        for h in range(PER_DEVICE):
            top = h * HEAD_DIM
            kept = jnp.broadcast_to(retain[top : top + 8, b : b + 1], (8, STATE))
            old = state_ref[b, h].reshape(HEAD_DIM // 8, 8, STATE) * kept[None]
            new.append(
                old.reshape(HEAD_DIM, STATE)
                + added[top : top + HEAD_DIM, b : b + 1] * writes[b : b + 1]
            )
            new_state_ref[b, h] = new[h]
        new = jnp.concatenate(new, axis=0).astype(jnp.bfloat16)
        read = lax.dot_general(new, reads, by_rows, preferred_element_type=jnp.float32)
        cols = jnp.where(column == b, read, cols)
    out_cols_ref[i] = cols

    @pl.when(i == pl.num_programs(0) - 1)
    def _():
        cols = jnp.concatenate([out_cols_ref[s] for s in range(SEQS // BLOCK)], axis=1)
        head = lax.broadcasted_iota(jnp.int32, (1, CHANNELS), 1) // HEAD_DIM
        skip_own = skip_ref[...].reshape(1, PER_DEVICE)
        skip = jnp.zeros((1, CHANNELS), jnp.float32)
        for h in range(PER_DEVICE):
            skip = jnp.where(head == h, skip_own[:, h : h + 1], skip)
        head_out = (cols.T + skip * xc_ref[...]).astype(jnp.bfloat16).astype(jnp.float32)
        gate_z = gate_z_ref[...].astype(jnp.float32)
        gated = head_out * (gate_z * jax.nn.sigmoid(gate_z))
        gated = gated * inverse_rms(gated) * group_ref[...].astype(jnp.float32).reshape(1, CHANNELS)
        part = jnp.dot(
            gated.astype(jnp.bfloat16), output_ref[...], preferred_element_type=jnp.float32
        )
        mixed_ref[...] = part.reshape(TP, ROWS, D).astype(jnp.bfloat16)


def state_mixer(first, small, buffers, scan_state, group_gain, proj_output):
    rows = sent_to_all(first, TP_AXES)
    operands = [rows, *small, *[b.transpose(1, 0, 2) for b in buffers]]
    operands += [scan_state, group_gain, proj_output]
    state_place = len(operands) - 3
    operands = [
        o if n == state_place else pltpu.with_memory_space_constraint(o, pltpu.VMEM)
        for n, o in enumerate(operands)
    ]
    specs = [pl.BlockSpec(memory_space=pltpu.VMEM) for _ in operands]
    state_spec = pl.BlockSpec((BLOCK, PER_DEVICE, HEAD_DIM, STATE), lambda i: (i, 0, 0, 0))
    specs[state_place] = state_spec
    blocks = SEQS // BLOCK
    partial_out, state_out = pl.pallas_call(
        mixer_kernel,
        grid=(blocks,),
        out_shape=[
            jax.ShapeDtypeStruct((TP, ROWS, D), jnp.bfloat16),
            jax.ShapeDtypeStruct(scan_state.shape, jnp.float32),
        ],
        in_specs=specs,
        out_specs=[pl.BlockSpec((TP, ROWS, D), lambda i: (0, 0, 0)), state_spec],
        scratch_shapes=[
            pltpu.VMEM((SEQS, D), jnp.bfloat16),
            pltpu.VMEM((SEQS, CHANNELS), jnp.bfloat16),
            pltpu.VMEM((SEQS, CHANNELS), jnp.float32),
            pltpu.VMEM((blocks, CHANNELS, BLOCK), jnp.float32),
            pltpu.VMEM((blocks, CHANNELS, BLOCK), jnp.float32),
            pltpu.VMEM((SEQS, STATE), jnp.float32),
            pltpu.VMEM((SEQS, STATE), jnp.float32),
            pltpu.VMEM((blocks, CHANNELS, BLOCK), jnp.float32),
        ],
        compiler_params=pltpu.CompilerParams(vmem_limit_bytes=24 << 20),
        name="mixer",
    )(*operands)
    tiles = lax.all_to_all(partial_out, TP_AXES, 0, 0, tiled=True)
    mixed = jnp.sum(tiles.astype(jnp.float32), axis=0)
    own = first.astype(jnp.float32).transpose(1, 0, 2).reshape(ROWS, D)
    return ((own + mixed).astype(jnp.bfloat16), state_out)


def per_device(
    residual,
    first_gain,
    first_gate,
    first_lift,
    first_down,
    mixer_gain,
    proj_gate,
    proj_input,
    proj_write,
    proj_read,
    proj_step,
    step_bias,
    rate_log,
    skip_gain,
    taps_input,
    taps_write,
    taps_read,
    buffer_input,
    buffer_write,
    buffer_read,
    scan_state,
    group_gain,
    proj_output,
    second_gain,
    second_gate,
    second_lift,
    second_down,
):
    share_one, share_two = weight_shares(
        (first_gain, first_gate, first_lift, first_down),
        (second_gain, second_gate, second_lift, second_down),
    )
    weights_one = lax.all_gather(share_one, TP_AXES)
    weights_two = lax.all_gather(share_two, ("y", *TP_AXES)).reshape(
        Y, TP, 3 * HIDDEN, FEATS
    )

    split = residual.reshape(TP, ROWS, FEATS)
    tiles = lax.all_to_all(
        jnp.broadcast_to(split[None], (Z * Y, TP, ROWS, FEATS)).reshape(-1, ROWS, FEATS),
        (*KV_AXES, *TP_AXES),
        0,
        0,
        tiled=True,
    ).reshape(Z * Y, TP, ROWS, FEATS)
    own_rows = lax.dynamic_index_in_dim(tiles, lax.axis_index(KV_AXES), 0, keepdims=False)
    share = first_partial(tiles, weights_one)
    share = lax.all_to_all(share, KV_AXES, 0, 0, tiled=True)
    branch = jnp.sum(share.astype(jnp.float32), axis=0)
    first = (own_rows.astype(jnp.float32) + 0.5 * branch).astype(jnp.bfloat16)

    mixed, state_out = state_mixer(
        first,
        (
            mixer_gain,
            proj_gate,
            proj_input,
            proj_write,
            proj_read,
            proj_step.T,
            step_bias,
            rate_log,
            skip_gain,
            taps_input,
            taps_write,
            taps_read,
        ),
        (buffer_input, buffer_write, buffer_read),
        scan_state,
        group_gain,
        proj_output,
    )

    share = second_partial(sent_to_all(mixed, "z"), weights_two)
    share = lax.all_to_all(
        share.reshape(-1, ROWS, FEATS), ("z", *TP_AXES), 0, 0, tiled=True
    ).reshape(Z, TP * ROWS, FEATS)
    residual_out = (0.5 * jnp.sum(share.astype(jnp.float32), axis=0)).astype(jnp.bfloat16)
    return (residual_out, state_out)


def solution(mesh):
    mesh = Mesh(mesh.devices.reshape(Z, Y, TP // 2, 2), (*KV_AXES, *TP_AXES))
    placed = (
        P(KV_AXES, TP_AXES),
        P(TP_AXES),
        P(TP_AXES, KV_AXES),
        P(TP_AXES, KV_AXES),
        P(KV_AXES, TP_AXES),
        P(),
        P(None, TP_AXES),
        P(None, TP_AXES),
        P(None, TP_AXES),
        P(None, TP_AXES),
        P(None, TP_AXES),
        P(TP_AXES),
        P(TP_AXES),
        P(TP_AXES),
        P(None, TP_AXES),
        P(None, TP_AXES),
        P(None, TP_AXES),
        P(KV_AXES, None, TP_AXES),
        P(KV_AXES, None, TP_AXES),
        P(KV_AXES, None, TP_AXES),
        P(KV_AXES, TP_AXES, None, None),
        P(TP_AXES),
        P(TP_AXES, None),
        P(TP_AXES),
        P(TP_AXES, KV_AXES),
        P(TP_AXES, KV_AXES),
        P(KV_AXES, TP_AXES),
    )
    return jax.shard_map(
        per_device,
        mesh=mesh,
        in_specs=placed,
        out_specs=(P(KV_AXES, TP_AXES), P(KV_AXES, TP_AXES, None, None)),
        check_vma=False,
    )
```

```python
import jax
import jax.numpy as jnp
from jax import lax
from jax.experimental import pallas as pl
from jax.experimental.pallas import tpu as pltpu
from jax.sharding import Mesh
from jax.sharding import PartitionSpec as P

D = 2048
HEAD_DIM = 64
STATE = 128
FEATS = 256
HIDDEN = 176
ROWS = 4
Z, Y, TP = 8, 4, 8

KV_AXES = ("z", "y")
TP_AXES = ("x", "core")

norm_eps = 1e-06

by_rows = (((1,), (1,)), ((), ()))


def sent_to_all(array, axis):
    length = lax.axis_size(axis)
    return lax.all_to_all(
        jnp.broadcast_to(array[None], (length, *array.shape)), axis, 0, 0, tiled=True
    )


def inverse_rms(values):
    return lax.rsqrt(jnp.mean(values * values, axis=-1, keepdims=True) + norm_eps)


def in_hbm(array):
    return pltpu.with_memory_space_constraint(array, pltpu.HBM)


def in_vmem(array):
    return pltpu.with_memory_space_constraint(array, pltpu.VMEM)


def share_kernel(gain, gate, lift, down, out):
    gain_f = gain[...].astype(jnp.float32).reshape(1, FEATS)
    out[:HIDDEN] = (gate[...].astype(jnp.float32) * gain_f).astype(jnp.bfloat16)
    out[HIDDEN : 2 * HIDDEN] = (lift[...].astype(jnp.float32) * gain_f).astype(jnp.bfloat16)
    out[2 * HIDDEN :] = down[...]


def weight_share(gain, gate_weight, lift_weight, down_weight):
    operands = [gain, gate_weight.T, lift_weight.T, down_weight]
    return pl.pallas_call(
        share_kernel,
        out_shape=jax.ShapeDtypeStruct((3 * HIDDEN, FEATS), jnp.bfloat16),
        name="share",
    )(*[in_hbm(operand) for operand in operands])


def first_kernel(rows_ref, weights_hbm, out_ref, normed_ref, weights_ref, arrived):
    blocks = Z * Y
    count = blocks * ROWS
    copies = [
        pltpu.make_async_copy(weights_hbm.at[u], weights_ref.at[u], arrived.at[u])
        for u in range(TP)
    ]
    for copy in copies:
        copy.start()
    total = jnp.zeros((blocks, ROWS, 1), jnp.float32)
    for u in range(TP):
        values = rows_ref[:, u].astype(jnp.float32)
        total += jnp.sum(values * values, axis=-1, keepdims=True)
    factor = lax.rsqrt(total * (1.0 / D) + norm_eps)
    for u in range(TP):
        values = rows_ref[:, u].astype(jnp.float32) * factor
        normed_ref[u] = values.reshape(count, FEATS).astype(jnp.bfloat16)
    gate = jnp.zeros((count, HIDDEN), jnp.float32)
    lift = jnp.zeros((count, HIDDEN), jnp.float32)
    for u in range(TP):
        copies[u].wait()
        block = normed_ref[u]
        gate += lax.dot_general(
            block, weights_ref[u, :HIDDEN], by_rows, preferred_element_type=jnp.float32
        )
        lift += lax.dot_general(
            block, weights_ref[u, HIDDEN : 2 * HIDDEN], by_rows, preferred_element_type=jnp.float32
        )
    hidden = (gate * jax.nn.sigmoid(gate) * lift).astype(jnp.bfloat16)
    for u in range(TP):
        down = jnp.dot(hidden, weights_ref[u, 2 * HIDDEN :], preferred_element_type=jnp.float32)
        out_ref[:, u] = down.reshape(blocks, ROWS, FEATS).astype(jnp.bfloat16)


def first_partial(rows, weights):
    return pl.pallas_call(
        first_kernel,
        out_shape=jax.ShapeDtypeStruct(rows.shape, jnp.bfloat16),
        in_specs=[
            pl.BlockSpec(memory_space=pltpu.VMEM),
            pl.BlockSpec(memory_space=pltpu.HBM),
        ],
        scratch_shapes=[
            pltpu.VMEM((TP, Z * Y * ROWS, FEATS), jnp.bfloat16),
            pltpu.VMEM(weights.shape, jnp.bfloat16),
            pltpu.SemaphoreType.DMA((TP,)),
        ],
        compiler_params=pltpu.CompilerParams(vmem_limit_bytes=24 << 20),
        name="first_ffn",
    )(in_vmem(rows), in_hbm(weights))


def second_kernel(place_ref, rows_ref, weights_ref, out_ref, normed_ref, sum_ref):
    step = pl.program_id(0)
    rows = Z * ROWS

    @pl.when(step == 0)
    def _():
        values = rows_ref[...].astype(jnp.float32).reshape(rows, D)
        factor = lax.rsqrt(jnp.sum(values * values, axis=-1, keepdims=True) * (1.0 / D) + norm_eps)
        row = lax.broadcasted_iota(jnp.int32, (rows, 1), 0)
        own = jnp.where(row // ROWS == place_ref[0], 2.0, 0.0)
        for u in range(TP):
            block = values[:, u * FEATS : (u + 1) * FEATS]
            normed_ref[u] = (block * factor).astype(jnp.bfloat16)
            sum_ref[u] = block * own

    both = jnp.zeros((2 * HIDDEN, rows), jnp.float32)
    for u in range(TP):
        both += lax.dot_general(
            weights_ref[0, u, : 2 * HIDDEN],
            normed_ref[u],
            by_rows,
            preferred_element_type=jnp.float32,
        )
    gate, lift = both[:HIDDEN], both[HIDDEN:]
    hidden = (gate * jax.nn.sigmoid(gate) * lift).T.astype(jnp.bfloat16)
    for u in range(TP):
        down = jnp.dot(hidden, weights_ref[0, u, 2 * HIDDEN :], preferred_element_type=jnp.float32)
        sum_ref[u] = sum_ref[u] + down

    @pl.when(step == pl.num_programs(0) - 1)
    def _():
        for u in range(TP):
            out_ref[:, u] = sum_ref[u].reshape(Z, ROWS, FEATS).astype(jnp.bfloat16)


def second_partial(rows, weights):
    place = lax.axis_index("z").astype(jnp.int32).reshape(1)
    return pl.pallas_call(
        second_kernel,
        grid=(Y,),
        out_shape=jax.ShapeDtypeStruct((Z, TP, ROWS, FEATS), jnp.bfloat16),
        in_specs=[
            pl.BlockSpec(memory_space=pltpu.SMEM),
            pl.BlockSpec(memory_space=pltpu.VMEM),
            pl.BlockSpec((1, TP, 3 * HIDDEN, FEATS), lambda i: (i, 0, 0, 0)),
        ],
        out_specs=pl.BlockSpec((Z, TP, ROWS, FEATS), lambda i: (0, 0, 0, 0)),
        scratch_shapes=[
            pltpu.VMEM((TP, Z * ROWS, FEATS), jnp.bfloat16),
            pltpu.VMEM((TP, Z * ROWS, FEATS), jnp.float32),
        ],
        compiler_params=pltpu.CompilerParams(vmem_limit_bytes=24 << 20),
        name="second_ffn",
    )(place, in_vmem(rows), in_hbm(weights))


def conv_silu(newest, buffer_ref, taps_ref):
    taps = taps_ref[...].astype(jnp.float32)
    summed = newest.astype(jnp.float32) * taps[3:4]
    for k in range(3):
        summed += buffer_ref[k].astype(jnp.float32) * taps[k : k + 1]
    return summed * jax.nn.sigmoid(summed)


SEQS = TP * ROWS
BLOCK = 8
CHANNELS = 256
PER_DEVICE = 4


def mixer_kernel(
    rows_ref,
    gain_ref,
    gate_ref,
    input_ref,
    write_ref,
    read_hbm,
    step_ref,
    bias_ref,
    rate_ref,
    skip_ref,
    taps_input_ref,
    taps_write_ref,
    taps_read_ref,
    buffer_input_ref,
    buffer_write_ref,
    buffer_read_ref,
    state_ref,
    group_ref,
    output_hbm,
    mixed_ref,
    new_state_ref,
    normed_ref,
    gate_z_ref,
    xc_ref,
    added_ref,
    retain_ref,
    bc_ref,
    rc_ref,
    out_cols_ref,
    read_ref,
    output_ref,
    arrived,
):
    i = pl.program_id(0)
    read_copy = pltpu.make_async_copy(read_hbm, read_ref, arrived.at[0])
    output_copy = pltpu.make_async_copy(output_hbm, output_ref, arrived.at[1])

    @pl.when(i == 0)
    def _():
        read_copy.start()
        output_copy.start()
        total = jnp.zeros((TP, ROWS, 1), jnp.float32)
        for u in range(TP):
            values = rows_ref[:, u].astype(jnp.float32)
            total += jnp.sum(values * values, axis=-1, keepdims=True)
        factor = lax.rsqrt(total * (1.0 / D) + norm_eps)
        for u in range(TP):
            values = (rows_ref[:, u].astype(jnp.float32) * factor).reshape(SEQS, FEATS)
            cols = slice(u * FEATS, (u + 1) * FEATS)
            gain = gain_ref[cols].astype(jnp.float32).reshape(1, FEATS)
            normed_ref[:, cols] = (values * gain).astype(jnp.bfloat16)
        normed = normed_ref[...]

        def project(weight_ref):
            return jnp.dot(normed, weight_ref[...], preferred_element_type=jnp.float32).astype(
                jnp.bfloat16
            )

        gate_z_ref[...] = project(gate_ref)
        step_raw = lax.dot_general(
            normed, step_ref[...], by_rows, preferred_element_type=jnp.float32
        ).astype(jnp.bfloat16)
        xc = conv_silu(project(input_ref), buffer_input_ref, taps_input_ref)
        bc_ref[...] = conv_silu(project(write_ref), buffer_write_ref, taps_write_ref)
        read_copy.wait()
        rc_ref[...] = conv_silu(project(read_ref), buffer_read_ref, taps_read_ref)
        xc_ref[...] = xc
        step = jax.nn.softplus(step_raw.astype(jnp.float32) + bias_ref[...].reshape(1, PER_DEVICE))
        retain = jnp.exp(-step * jnp.exp(rate_ref[...].reshape(1, PER_DEVICE)))
        head = lax.broadcasted_iota(jnp.int32, (SEQS, CHANNELS), 1) // HEAD_DIM
        step_wide = jnp.zeros((SEQS, CHANNELS), jnp.float32)
        retain_wide = jnp.zeros((SEQS, CHANNELS), jnp.float32)
        for h in range(PER_DEVICE):
            step_wide = jnp.where(head == h, step[:, h : h + 1], step_wide)
            retain_wide = jnp.where(head == h, retain[:, h : h + 1], retain_wide)
        added = (step_wide * xc).T
        retain_cols = retain_wide.T
        for s in range(SEQS // BLOCK):
            added_ref[s] = added[:, s * BLOCK : (s + 1) * BLOCK]
            retain_ref[s] = retain_cols[:, s * BLOCK : (s + 1) * BLOCK]

    added = added_ref[i]
    retain = retain_ref[i]
    writes = bc_ref[pl.ds(pl.multiple_of(i * BLOCK, BLOCK), BLOCK)]
    reads = rc_ref[pl.ds(pl.multiple_of(i * BLOCK, BLOCK), BLOCK)].astype(jnp.bfloat16)
    column = lax.broadcasted_iota(jnp.int32, (CHANNELS, BLOCK), 1)
    cols = jnp.zeros((CHANNELS, BLOCK), jnp.float32)
    for b in range(BLOCK):
        new = []
        for h in range(PER_DEVICE):
            top = h * HEAD_DIM
            kept = jnp.broadcast_to(retain[top : top + 8, b : b + 1], (8, STATE))
            old = state_ref[b, h].reshape(HEAD_DIM // 8, 8, STATE) * kept[None]
            new.append(
                old.reshape(HEAD_DIM, STATE)
                + added[top : top + HEAD_DIM, b : b + 1] * writes[b : b + 1]
            )
            new_state_ref[b, h] = new[h]
        new = jnp.concatenate(new, axis=0).astype(jnp.bfloat16)
        read = lax.dot_general(new, reads, by_rows, preferred_element_type=jnp.float32)
        cols = jnp.where(column == b, read, cols)
    out_cols_ref[i] = cols

    @pl.when(i == pl.num_programs(0) - 1)
    def _():
        cols = jnp.concatenate([out_cols_ref[s] for s in range(SEQS // BLOCK)], axis=1)
        head = lax.broadcasted_iota(jnp.int32, (1, CHANNELS), 1) // HEAD_DIM
        skip_own = skip_ref[...].reshape(1, PER_DEVICE)
        skip = jnp.zeros((1, CHANNELS), jnp.float32)
        for h in range(PER_DEVICE):
            skip = jnp.where(head == h, skip_own[:, h : h + 1], skip)
        head_out = (cols.T + skip * xc_ref[...]).astype(jnp.bfloat16).astype(jnp.float32)
        gate_z = gate_z_ref[...].astype(jnp.float32)
        gated = head_out * (gate_z * jax.nn.sigmoid(gate_z))
        gated = gated * inverse_rms(gated) * group_ref[...].astype(jnp.float32).reshape(1, CHANNELS)
        output_copy.wait()
        part = jnp.dot(
            gated.astype(jnp.bfloat16), output_ref[...], preferred_element_type=jnp.float32
        )
        mixed_ref[...] = part.reshape(TP, ROWS, D).astype(jnp.bfloat16)


def state_mixer(first, small, buffers, scan_state, group_gain, proj_output):
    rows = sent_to_all(first, TP_AXES)
    operands = [rows, *small, *[b.transpose(1, 0, 2) for b in buffers]]
    operands += [scan_state, group_gain, proj_output]
    state_place = len(operands) - 3
    from_hbm = (5, state_place, len(operands) - 1)
    operands = [in_hbm(o) if n in from_hbm else in_vmem(o) for n, o in enumerate(operands)]
    specs = [pl.BlockSpec(memory_space=pltpu.VMEM) for _ in operands]
    for n in from_hbm:
        specs[n] = pl.BlockSpec(memory_space=pltpu.HBM)
    state_spec = pl.BlockSpec((BLOCK, PER_DEVICE, HEAD_DIM, STATE), lambda i: (i, 0, 0, 0))
    specs[state_place] = state_spec
    blocks = SEQS // BLOCK
    partial_out, state_out = pl.pallas_call(
        mixer_kernel,
        grid=(blocks,),
        out_shape=[
            jax.ShapeDtypeStruct((TP, ROWS, D), jnp.bfloat16),
            jax.ShapeDtypeStruct(scan_state.shape, jnp.float32),
        ],
        in_specs=specs,
        out_specs=[pl.BlockSpec((TP, ROWS, D), lambda i: (0, 0, 0)), state_spec],
        scratch_shapes=[
            pltpu.VMEM((SEQS, D), jnp.bfloat16),
            pltpu.VMEM((SEQS, CHANNELS), jnp.bfloat16),
            pltpu.VMEM((SEQS, CHANNELS), jnp.float32),
            pltpu.VMEM((blocks, CHANNELS, BLOCK), jnp.float32),
            pltpu.VMEM((blocks, CHANNELS, BLOCK), jnp.float32),
            pltpu.VMEM((SEQS, STATE), jnp.float32),
            pltpu.VMEM((SEQS, STATE), jnp.float32),
            pltpu.VMEM((blocks, CHANNELS, BLOCK), jnp.float32),
            pltpu.VMEM((D, STATE), jnp.bfloat16),
            pltpu.VMEM((CHANNELS, D), jnp.bfloat16),
            pltpu.SemaphoreType.DMA((2,)),
        ],
        compiler_params=pltpu.CompilerParams(vmem_limit_bytes=24 << 20),
        name="mixer",
    )(*operands)
    tiles = lax.all_to_all(partial_out, TP_AXES, 0, 0, tiled=True)
    mixed = jnp.sum(tiles.astype(jnp.float32), axis=0)
    own = first.astype(jnp.float32).transpose(1, 0, 2).reshape(ROWS, D)
    return ((own + mixed).astype(jnp.bfloat16), state_out)


def per_device(
    residual,
    first_gain,
    first_gate,
    first_lift,
    first_down,
    mixer_gain,
    proj_gate,
    proj_input,
    proj_write,
    proj_read,
    proj_step,
    step_bias,
    rate_log,
    skip_gain,
    taps_input,
    taps_write,
    taps_read,
    buffer_input,
    buffer_write,
    buffer_read,
    scan_state,
    group_gain,
    proj_output,
    second_gain,
    second_gate,
    second_lift,
    second_down,
):
    weights_one = lax.all_gather(
        weight_share(first_gain, first_gate, first_lift, first_down), TP_AXES
    )
    weights_two = lax.all_gather(
        weight_share(second_gain, second_gate, second_lift, second_down), ("y", *TP_AXES)
    ).reshape(Y, TP, 3 * HIDDEN, FEATS)

    split = residual.reshape(TP, ROWS, FEATS)
    tiles = lax.all_to_all(
        jnp.broadcast_to(split[None], (Z * Y, TP, ROWS, FEATS)).reshape(-1, ROWS, FEATS),
        (*KV_AXES, *TP_AXES),
        0,
        0,
        tiled=True,
    ).reshape(Z * Y, TP, ROWS, FEATS)
    own_rows = lax.dynamic_index_in_dim(tiles, lax.axis_index(KV_AXES), 0, keepdims=False)
    share = first_partial(tiles, weights_one)
    share = lax.all_to_all(share, KV_AXES, 0, 0, tiled=True)
    branch = jnp.sum(share.astype(jnp.float32), axis=0)
    first = (own_rows.astype(jnp.float32) + 0.5 * branch).astype(jnp.bfloat16)

    mixed, state_out = state_mixer(
        first,
        (
            mixer_gain,
            proj_gate,
            proj_input,
            proj_write,
            proj_read,
            proj_step.T,
            step_bias,
            rate_log,
            skip_gain,
            taps_input,
            taps_write,
            taps_read,
        ),
        (buffer_input, buffer_write, buffer_read),
        scan_state,
        group_gain,
        proj_output,
    )

    share = second_partial(sent_to_all(mixed, "z"), weights_two)
    share = lax.all_to_all(
        share.reshape(-1, ROWS, FEATS), ("z", *TP_AXES), 0, 0, tiled=True
    ).reshape(Z, TP * ROWS, FEATS)
    residual_out = (0.5 * jnp.sum(share.astype(jnp.float32), axis=0)).astype(jnp.bfloat16)
    return (residual_out, state_out)


def solution(mesh):
    mesh = Mesh(mesh.devices.reshape(Z, Y, TP // 2, 2), (*KV_AXES, *TP_AXES))
    placed = (
        P(KV_AXES, TP_AXES),
        P(TP_AXES),
        P(TP_AXES, KV_AXES),
        P(TP_AXES, KV_AXES),
        P(KV_AXES, TP_AXES),
        P(),
        P(None, TP_AXES),
        P(None, TP_AXES),
        P(None, TP_AXES),
        P(None, TP_AXES),
        P(None, TP_AXES),
        P(TP_AXES),
        P(TP_AXES),
        P(TP_AXES),
        P(None, TP_AXES),
        P(None, TP_AXES),
        P(None, TP_AXES),
        P(KV_AXES, None, TP_AXES),
        P(KV_AXES, None, TP_AXES),
        P(KV_AXES, None, TP_AXES),
        P(KV_AXES, TP_AXES, None, None),
        P(TP_AXES),
        P(TP_AXES, None),
        P(TP_AXES),
        P(TP_AXES, KV_AXES),
        P(TP_AXES, KV_AXES),
        P(KV_AXES, TP_AXES),
    )
    return jax.shard_map(
        per_device,
        mesh=mesh,
        in_specs=placed,
        out_specs=(P(KV_AXES, TP_AXES), P(KV_AXES, TP_AXES, None, None)),
        check_vma=False,
    )
```

```python
import jax
import jax.numpy as jnp
from jax import lax
from jax.experimental import pallas as pl
from jax.experimental.pallas import tpu as pltpu
from jax.sharding import Mesh
from jax.sharding import PartitionSpec as P

D = 2048
HEAD_DIM = 64
STATE = 128
FEATS = 256
HIDDEN = 176
ROWS = 4
Z, Y, TP = 8, 4, 8

KV_AXES = ("z", "y")
TP_AXES = ("x", "core")

norm_eps = 1e-06

by_rows = (((1,), (1,)), ((), ()))


def sent_to_all(array, axis):
    length = lax.axis_size(axis)
    return lax.all_to_all(
        jnp.broadcast_to(array[None], (length, *array.shape)), axis, 0, 0, tiled=True
    )


def inverse_rms(values):
    return lax.rsqrt(jnp.mean(values * values, axis=-1, keepdims=True) + norm_eps)


def in_hbm(array):
    return pltpu.with_memory_space_constraint(array, pltpu.HBM)


def in_vmem(array):
    return pltpu.with_memory_space_constraint(array, pltpu.VMEM)


def share_kernel(*refs):
    gain, gate, lift, down, out = refs[-5:]
    gain_f = gain[...].astype(jnp.float32).reshape(1, FEATS)
    out[:HIDDEN] = (gate[...].astype(jnp.float32) * gain_f).astype(jnp.bfloat16)
    out[HIDDEN : 2 * HIDDEN] = (lift[...].astype(jnp.float32) * gain_f).astype(jnp.bfloat16)
    out[2 * HIDDEN :] = down[...]


def weight_share(gain, gate_weight, lift_weight, down_weight, *early):
    operands = [gain, gate_weight.T, lift_weight.T, down_weight]
    return pl.pallas_call(
        share_kernel,
        out_shape=jax.ShapeDtypeStruct((3 * HIDDEN, FEATS), jnp.bfloat16),
        compiler_params=pltpu.CompilerParams(vmem_limit_bytes=4 << 20),
        in_specs=[pl.BlockSpec(memory_space=pltpu.SMEM) for _ in early]
        + [pl.BlockSpec(memory_space=pltpu.VMEM) for _ in operands],
        name="share",
    )(*early, *[in_hbm(operand) for operand in operands])


def first_kernel(
    place_ref, rows_ref, weights_hbm, out_ref, own_ref, normed_ref, weights_ref, arrived
):
    blocks = Z * Y
    count = blocks * ROWS
    copies = [
        pltpu.make_async_copy(weights_hbm.at[u], weights_ref.at[u], arrived.at[u])
        for u in range(TP)
    ]
    for copy in copies:
        copy.start()
    total = jnp.zeros((blocks, ROWS, 1), jnp.float32)
    for u in range(TP):
        values = rows_ref[:, u].astype(jnp.float32)
        total += jnp.sum(values * values, axis=-1, keepdims=True)
    factor = lax.rsqrt(total * (1.0 / D) + norm_eps)
    for u in range(TP):
        values = rows_ref[:, u].astype(jnp.float32) * factor
        normed_ref[u] = values.reshape(count, FEATS).astype(jnp.bfloat16)
    own_ref[...] = rows_ref[place_ref[0]]
    gate = jnp.zeros((count, HIDDEN), jnp.float32)
    lift = jnp.zeros((count, HIDDEN), jnp.float32)
    for u in range(TP):
        copies[u].wait()
        block = normed_ref[u]
        gate += lax.dot_general(
            block, weights_ref[u, :HIDDEN], by_rows, preferred_element_type=jnp.float32
        )
        lift += lax.dot_general(
            block, weights_ref[u, HIDDEN : 2 * HIDDEN], by_rows, preferred_element_type=jnp.float32
        )
    hidden = (gate * jax.nn.sigmoid(gate) * lift).astype(jnp.bfloat16)
    for u in range(TP):
        down = jnp.dot(hidden, weights_ref[u, 2 * HIDDEN :], preferred_element_type=jnp.float32)
        out_ref[:, u] = down.reshape(blocks, ROWS, FEATS).astype(jnp.bfloat16)


def first_partial(place, rows, weights):
    vmem = pl.BlockSpec(memory_space=pltpu.VMEM)
    return pl.pallas_call(
        first_kernel,
        out_shape=[
            pltpu.VMEM(rows.shape, jnp.bfloat16),
            pltpu.VMEM(rows.shape[1:], jnp.bfloat16),
        ],
        in_specs=[
            pl.BlockSpec(memory_space=pltpu.SMEM),
            vmem,
            pl.BlockSpec(memory_space=pltpu.HBM),
        ],
        out_specs=[vmem, vmem],
        scratch_shapes=[
            pltpu.VMEM((TP, Z * Y * ROWS, FEATS), jnp.bfloat16),
            pltpu.VMEM(weights.shape, jnp.bfloat16),
            pltpu.SemaphoreType.DMA((TP,)),
        ],
        compiler_params=pltpu.CompilerParams(vmem_limit_bytes=24 << 20),
        name="first_ffn",
    )(place, in_vmem(rows), in_hbm(weights))


def settle_kernel(rows_ref, share_ref, first_ref, copies_ref):
    for u in range(TP):
        branch = jnp.sum(share_ref[:, u].astype(jnp.float32), axis=0)
        own = rows_ref[u].astype(jnp.float32)
        first = (own + 0.5 * branch).astype(jnp.bfloat16)
        first_ref[u] = first
        for t in range(TP):
            copies_ref[t, u] = first


def settled(rows, share):
    shape = (TP, ROWS, FEATS)
    vmem = pl.BlockSpec(memory_space=pltpu.VMEM)
    return pl.pallas_call(
        settle_kernel,
        out_shape=[pltpu.VMEM(shape, jnp.bfloat16), pltpu.VMEM((TP, *shape), jnp.bfloat16)],
        in_specs=[vmem, vmem],
        out_specs=[vmem, vmem],
        compiler_params=pltpu.CompilerParams(vmem_limit_bytes=24 << 20),
        name="settle",
    )(in_vmem(rows), in_vmem(share))


def mix_kernel(first_ref, tiles_ref, copies_ref):
    mixed = jnp.sum(tiles_ref[...].astype(jnp.float32), axis=0)
    for u in range(TP):
        cols = slice(u * FEATS, (u + 1) * FEATS)
        rows = (first_ref[u].astype(jnp.float32) + mixed[:, cols]).astype(jnp.bfloat16)
        for z in range(Z):
            copies_ref[z, :, cols] = rows


def mixed_copies(first, tiles):
    vmem = pl.BlockSpec(memory_space=pltpu.VMEM)
    return pl.pallas_call(
        mix_kernel,
        out_shape=pltpu.VMEM((Z, ROWS, D), jnp.bfloat16),
        in_specs=[vmem, vmem],
        out_specs=vmem,
        compiler_params=pltpu.CompilerParams(vmem_limit_bytes=8 << 20),
        name="mix",
    )(in_vmem(first), in_vmem(tiles))


def second_kernel(place_ref, rows_ref, weights_hbm, out_ref, normed_ref, weights_ref, arrived):
    rows = Z * ROWS
    copies = [
        pltpu.make_async_copy(weights_hbm.at[n], weights_ref.at[n], arrived.at[n])
        for n in range(Y * TP)
    ]
    for copy in copies:
        copy.start()
    values = rows_ref[...].astype(jnp.float32).reshape(rows, D)
    factor = lax.rsqrt(jnp.sum(values * values, axis=-1, keepdims=True) * (1.0 / D) + norm_eps)
    row = lax.broadcasted_iota(jnp.int32, (rows, 1), 0)
    own = jnp.where(row // ROWS == place_ref[1], 2.0, 0.0)
    for u in range(TP):
        normed_ref[u] = (values[:, u * FEATS : (u + 1) * FEATS] * factor).astype(jnp.bfloat16)
    hidden = []
    for y in range(Y):
        both = jnp.zeros((2 * HIDDEN, rows), jnp.float32)
        for u in range(TP):
            copies[y * TP + u].wait()
            both += lax.dot_general(
                weights_ref[y * TP + u, : 2 * HIDDEN],
                normed_ref[u],
                by_rows,
                preferred_element_type=jnp.float32,
            )
        gate, lift = both[:HIDDEN], both[HIDDEN:]
        hidden.append((gate * jax.nn.sigmoid(gate) * lift).T.astype(jnp.bfloat16))
    for u in range(TP):
        down = values[:, u * FEATS : (u + 1) * FEATS] * own
        for y in range(Y):
            down += jnp.dot(
                hidden[y],
                weights_ref[y * TP + u, 2 * HIDDEN :],
                preferred_element_type=jnp.float32,
            )
        out_ref[:, u] = down.reshape(Z, ROWS, FEATS).astype(jnp.bfloat16)


def second_partial(place, rows, weights):
    vmem = pl.BlockSpec(memory_space=pltpu.VMEM)
    return pl.pallas_call(
        second_kernel,
        out_shape=pltpu.VMEM((Z, TP, ROWS, FEATS), jnp.bfloat16),
        in_specs=[
            pl.BlockSpec(memory_space=pltpu.SMEM),
            vmem,
            pl.BlockSpec(memory_space=pltpu.HBM),
        ],
        out_specs=vmem,
        scratch_shapes=[
            pltpu.VMEM((TP, Z * ROWS, FEATS), jnp.bfloat16),
            pltpu.VMEM(weights.shape, jnp.bfloat16),
            pltpu.SemaphoreType.DMA((Y * TP,)),
        ],
        compiler_params=pltpu.CompilerParams(vmem_limit_bytes=24 << 20),
        name="second_ffn",
    )(place, in_vmem(rows), in_hbm(weights))


def conv_silu(newest, buffer_ref, taps_ref):
    taps = taps_ref[...].astype(jnp.float32)
    summed = newest.astype(jnp.float32) * taps[3:4]
    for k in range(3):
        summed += buffer_ref[k].astype(jnp.float32) * taps[k : k + 1]
    return summed * jax.nn.sigmoid(summed)


SEQS = TP * ROWS
BLOCK = 8
CHANNELS = 256
PER_DEVICE = 4


def mixer_kernel(
    rows_ref,
    gain_ref,
    gate_ref,
    input_ref,
    write_ref,
    read_hbm,
    step_ref,
    bias_ref,
    rate_ref,
    skip_ref,
    taps_input_ref,
    taps_write_ref,
    taps_read_ref,
    buffer_input_ref,
    buffer_write_ref,
    buffer_read_ref,
    state_ref,
    group_ref,
    output_hbm,
    mixed_ref,
    new_state_ref,
    normed_ref,
    gate_z_ref,
    xc_ref,
    added_ref,
    retain_ref,
    bc_ref,
    rc_ref,
    out_cols_ref,
    read_ref,
    output_ref,
    arrived,
):
    i = pl.program_id(0)
    read_copy = pltpu.make_async_copy(read_hbm, read_ref, arrived.at[0])
    output_copy = pltpu.make_async_copy(output_hbm, output_ref, arrived.at[1])

    @pl.when(i == 0)
    def _():
        read_copy.start()
        output_copy.start()
        total = jnp.zeros((TP, ROWS, 1), jnp.float32)
        for u in range(TP):
            values = rows_ref[:, u].astype(jnp.float32)
            total += jnp.sum(values * values, axis=-1, keepdims=True)
        factor = lax.rsqrt(total * (1.0 / D) + norm_eps)
        for u in range(TP):
            values = (rows_ref[:, u].astype(jnp.float32) * factor).reshape(SEQS, FEATS)
            cols = slice(u * FEATS, (u + 1) * FEATS)
            gain = gain_ref[cols].astype(jnp.float32).reshape(1, FEATS)
            normed_ref[:, cols] = (values * gain).astype(jnp.bfloat16)
        normed = normed_ref[...]

        def project(weight_ref):
            return jnp.dot(normed, weight_ref[...], preferred_element_type=jnp.float32).astype(
                jnp.bfloat16
            )

        gate_z_ref[...] = project(gate_ref)
        step_raw = lax.dot_general(
            normed, step_ref[...], by_rows, preferred_element_type=jnp.float32
        ).astype(jnp.bfloat16)
        xc = conv_silu(project(input_ref), buffer_input_ref, taps_input_ref)
        bc_ref[...] = conv_silu(project(write_ref), buffer_write_ref, taps_write_ref)
        read_copy.wait()
        rc_ref[...] = conv_silu(project(read_ref), buffer_read_ref, taps_read_ref)
        xc_ref[...] = xc
        step = jax.nn.softplus(step_raw.astype(jnp.float32) + bias_ref[...].reshape(1, PER_DEVICE))
        retain = jnp.exp(-step * jnp.exp(rate_ref[...].reshape(1, PER_DEVICE)))
        head = lax.broadcasted_iota(jnp.int32, (SEQS, CHANNELS), 1) // HEAD_DIM
        step_wide = jnp.zeros((SEQS, CHANNELS), jnp.float32)
        retain_wide = jnp.zeros((SEQS, CHANNELS), jnp.float32)
        for h in range(PER_DEVICE):
            step_wide = jnp.where(head == h, step[:, h : h + 1], step_wide)
            retain_wide = jnp.where(head == h, retain[:, h : h + 1], retain_wide)
        added = (step_wide * xc).T
        retain_cols = retain_wide.T
        for s in range(SEQS // BLOCK):
            added_ref[s] = added[:, s * BLOCK : (s + 1) * BLOCK]
            retain_ref[s] = retain_cols[:, s * BLOCK : (s + 1) * BLOCK]

    added = added_ref[i]
    retain = retain_ref[i]
    writes = bc_ref[pl.ds(pl.multiple_of(i * BLOCK, BLOCK), BLOCK)]
    reads = rc_ref[pl.ds(pl.multiple_of(i * BLOCK, BLOCK), BLOCK)].astype(jnp.bfloat16)
    column = lax.broadcasted_iota(jnp.int32, (CHANNELS, BLOCK), 1)
    cols = jnp.zeros((CHANNELS, BLOCK), jnp.float32)
    for b in range(BLOCK):
        new = []
        for h in range(PER_DEVICE):
            top = h * HEAD_DIM
            kept = jnp.broadcast_to(retain[top : top + 8, b : b + 1], (8, STATE))
            old = state_ref[i * BLOCK + b, h].reshape(HEAD_DIM // 8, 8, STATE) * kept[None]
            new.append(
                old.reshape(HEAD_DIM, STATE)
                + added[top : top + HEAD_DIM, b : b + 1] * writes[b : b + 1]
            )
            new_state_ref[b, h] = new[h]
        new = jnp.concatenate(new, axis=0).astype(jnp.bfloat16)
        read = lax.dot_general(new, reads, by_rows, preferred_element_type=jnp.float32)
        cols = jnp.where(column == b, read, cols)
    out_cols_ref[i] = cols

    @pl.when(i == pl.num_programs(0) - 1)
    def _():
        cols = jnp.concatenate([out_cols_ref[s] for s in range(SEQS // BLOCK)], axis=1)
        head = lax.broadcasted_iota(jnp.int32, (1, CHANNELS), 1) // HEAD_DIM
        skip_own = skip_ref[...].reshape(1, PER_DEVICE)
        skip = jnp.zeros((1, CHANNELS), jnp.float32)
        for h in range(PER_DEVICE):
            skip = jnp.where(head == h, skip_own[:, h : h + 1], skip)
        head_out = (cols.T + skip * xc_ref[...]).astype(jnp.bfloat16).astype(jnp.float32)
        gate_z = gate_z_ref[...].astype(jnp.float32)
        gated = head_out * (gate_z * jax.nn.sigmoid(gate_z))
        gated = gated * inverse_rms(gated) * group_ref[...].astype(jnp.float32).reshape(1, CHANNELS)
        output_copy.wait()
        part = jnp.dot(
            gated.astype(jnp.bfloat16), output_ref[...], preferred_element_type=jnp.float32
        )
        mixed_ref[...] = part.reshape(TP, ROWS, D).astype(jnp.bfloat16)


def state_mixer(first, rows, small, buffers, scan_state, group_gain, proj_output):
    operands = [rows, *small, *[b.transpose(1, 0, 2) for b in buffers]]
    operands += [scan_state, group_gain, proj_output]
    from_hbm = (5, len(operands) - 1)
    operands = [in_hbm(o) if n in from_hbm else in_vmem(o) for n, o in enumerate(operands)]
    specs = [pl.BlockSpec(memory_space=pltpu.VMEM) for _ in operands]
    for n in from_hbm:
        specs[n] = pl.BlockSpec(memory_space=pltpu.HBM)
    state_spec = pl.BlockSpec((BLOCK, PER_DEVICE, HEAD_DIM, STATE), lambda i: (i, 0, 0, 0))
    blocks = SEQS // BLOCK
    partial_out, state_out = pl.pallas_call(
        mixer_kernel,
        grid=(blocks,),
        out_shape=[
            pltpu.VMEM((TP, ROWS, D), jnp.bfloat16),
            jax.ShapeDtypeStruct(scan_state.shape, jnp.float32),
        ],
        in_specs=specs,
        out_specs=[pl.BlockSpec(memory_space=pltpu.VMEM), state_spec],
        scratch_shapes=[
            pltpu.VMEM((SEQS, D), jnp.bfloat16),
            pltpu.VMEM((SEQS, CHANNELS), jnp.bfloat16),
            pltpu.VMEM((SEQS, CHANNELS), jnp.float32),
            pltpu.VMEM((blocks, CHANNELS, BLOCK), jnp.float32),
            pltpu.VMEM((blocks, CHANNELS, BLOCK), jnp.float32),
            pltpu.VMEM((SEQS, STATE), jnp.float32),
            pltpu.VMEM((SEQS, STATE), jnp.float32),
            pltpu.VMEM((blocks, CHANNELS, BLOCK), jnp.float32),
            pltpu.VMEM((D, STATE), jnp.bfloat16),
            pltpu.VMEM((CHANNELS, D), jnp.bfloat16),
            pltpu.SemaphoreType.DMA((2,)),
        ],
        compiler_params=pltpu.CompilerParams(vmem_limit_bytes=24 << 20),
        name="mixer",
    )(*operands)
    tiles = lax.all_to_all(partial_out, TP_AXES, 0, 0, tiled=True)
    return (mixed_copies(first, tiles), state_out)


def per_device(
    residual,
    first_gain,
    first_gate,
    first_lift,
    first_down,
    mixer_gain,
    proj_gate,
    proj_input,
    proj_write,
    proj_read,
    proj_step,
    step_bias,
    rate_log,
    skip_gain,
    taps_input,
    taps_write,
    taps_read,
    buffer_input,
    buffer_write,
    buffer_read,
    scan_state,
    group_gain,
    proj_output,
    second_gain,
    second_gate,
    second_lift,
    second_down,
):
    place = jnp.stack([lax.axis_index(KV_AXES), lax.axis_index("z")]).astype(jnp.int32)
    weights_one = lax.all_gather(
        weight_share(first_gain, first_gate, first_lift, first_down), TP_AXES
    )
    weights_two = lax.all_gather(
        weight_share(second_gain, second_gate, second_lift, second_down, place), ("y", *TP_AXES)
    )

    split = residual.reshape(TP, ROWS, FEATS)
    tiles = lax.all_to_all(
        jnp.broadcast_to(split[None], (Z * Y, TP, ROWS, FEATS)).reshape(-1, ROWS, FEATS),
        (*KV_AXES, *TP_AXES),
        0,
        0,
        tiled=True,
    ).reshape(Z * Y, TP, ROWS, FEATS)
    share, own = first_partial(place, tiles, weights_one)
    share = lax.all_to_all(share, KV_AXES, 0, 0, tiled=True)
    first, copies = settled(own, share)

    mixed, state_out = state_mixer(
        first,
        lax.all_to_all(copies, TP_AXES, 0, 0, tiled=True),
        (
            mixer_gain,
            proj_gate,
            proj_input,
            proj_write,
            proj_read,
            proj_step.T,
            step_bias,
            rate_log,
            skip_gain,
            taps_input,
            taps_write,
            taps_read,
        ),
        (buffer_input, buffer_write, buffer_read),
        scan_state,
        group_gain,
        proj_output,
    )

    rows = lax.all_to_all(mixed, "z", 0, 0, tiled=True)
    share = second_partial(place, rows, weights_two)
    share = lax.all_to_all(
        share.reshape(-1, ROWS, FEATS), ("z", *TP_AXES), 0, 0, tiled=True
    ).reshape(Z, TP * ROWS, FEATS)
    residual_out = (0.5 * jnp.sum(share.astype(jnp.float32), axis=0)).astype(jnp.bfloat16)
    return (residual_out, state_out)


def solution(mesh):
    mesh = Mesh(mesh.devices.reshape(Z, Y, TP // 2, 2), (*KV_AXES, *TP_AXES))
    placed = (
        P(KV_AXES, TP_AXES),
        P(TP_AXES),
        P(TP_AXES, KV_AXES),
        P(TP_AXES, KV_AXES),
        P(KV_AXES, TP_AXES),
        P(),
        P(None, TP_AXES),
        P(None, TP_AXES),
        P(None, TP_AXES),
        P(None, TP_AXES),
        P(None, TP_AXES),
        P(TP_AXES),
        P(TP_AXES),
        P(TP_AXES),
        P(None, TP_AXES),
        P(None, TP_AXES),
        P(None, TP_AXES),
        P(KV_AXES, None, TP_AXES),
        P(KV_AXES, None, TP_AXES),
        P(KV_AXES, None, TP_AXES),
        P(KV_AXES, TP_AXES, None, None),
        P(TP_AXES),
        P(TP_AXES, None),
        P(TP_AXES),
        P(TP_AXES, KV_AXES),
        P(TP_AXES, KV_AXES),
        P(KV_AXES, TP_AXES),
    )
    return jax.shard_map(
        per_device,
        mesh=mesh,
        in_specs=placed,
        out_specs=(P(KV_AXES, TP_AXES), P(KV_AXES, TP_AXES, None, None)),
        check_vma=False,
    )
```

```python
import jax
import jax.numpy as jnp
from jax import lax
from jax.experimental import pallas as pl
from jax.experimental.pallas import tpu as pltpu
from jax.sharding import Mesh
from jax.sharding import PartitionSpec as P

D = 2048
HEAD_DIM = 64
STATE = 128
FEATS = 256
HIDDEN = 176
ROWS = 4
Z, Y, TP = 8, 4, 8

KV_AXES = ("z", "y")
TP_AXES = ("x", "core")
BLOCK_AXES = ("y", "z")

norm_eps = 1e-06

by_rows = (((1,), (1,)), ((), ()))


def sent_to_all(array, axis):
    length = lax.axis_size(axis)
    return lax.all_to_all(
        jnp.broadcast_to(array[None], (length, *array.shape)), axis, 0, 0, tiled=True
    )


def inverse_rms(values):
    return lax.rsqrt(jnp.mean(values * values, axis=-1, keepdims=True) + norm_eps)


def in_hbm(array):
    return pltpu.with_memory_space_constraint(array, pltpu.HBM)


def in_vmem(array):
    return pltpu.with_memory_space_constraint(array, pltpu.VMEM)


def share_kernel(*refs):
    gain, gate, lift, down, out = refs[-5:]
    gain_f = gain[...].astype(jnp.float32).reshape(1, FEATS)
    out[:HIDDEN] = (gate[...].astype(jnp.float32) * gain_f).astype(jnp.bfloat16)
    out[HIDDEN : 2 * HIDDEN] = (lift[...].astype(jnp.float32) * gain_f).astype(jnp.bfloat16)
    out[2 * HIDDEN :] = down[...]


def weight_share(gain, gate_weight, lift_weight, down_weight, *early):
    operands = [gain, gate_weight.T, lift_weight.T, down_weight]
    return pl.pallas_call(
        share_kernel,
        out_shape=jax.ShapeDtypeStruct((3 * HIDDEN, FEATS), jnp.bfloat16),
        compiler_params=pltpu.CompilerParams(vmem_limit_bytes=4 << 20),
        in_specs=[pl.BlockSpec(memory_space=pltpu.SMEM) for _ in early]
        + [pl.BlockSpec(memory_space=pltpu.VMEM) for _ in operands],
        name="share",
    )(*early, *[in_hbm(operand) for operand in operands])


def first_kernel(
    place_ref, rows_ref, weights_hbm, out_ref, own_ref, normed_ref, weights_ref, arrived
):
    blocks = Z * Y
    count = blocks * ROWS
    copies = [
        pltpu.make_async_copy(weights_hbm.at[u], weights_ref.at[u], arrived.at[u])
        for u in range(TP)
    ]
    for copy in copies:
        copy.start()
    total = jnp.zeros((blocks, ROWS, 1), jnp.float32)
    for u in range(TP):
        values = rows_ref[:, u].astype(jnp.float32)
        total += jnp.sum(values * values, axis=-1, keepdims=True)
    factor = lax.rsqrt(total * (1.0 / D) + norm_eps)
    for u in range(TP):
        values = rows_ref[:, u].astype(jnp.float32) * factor
        normed_ref[u] = values.reshape(count, FEATS).astype(jnp.bfloat16)
    own_ref[...] = rows_ref[place_ref[0]]
    gate = jnp.zeros((count, HIDDEN), jnp.float32)
    lift = jnp.zeros((count, HIDDEN), jnp.float32)
    for u in range(TP):
        copies[u].wait()
        block = normed_ref[u]
        gate += lax.dot_general(
            block, weights_ref[u, :HIDDEN], by_rows, preferred_element_type=jnp.float32
        )
        lift += lax.dot_general(
            block, weights_ref[u, HIDDEN : 2 * HIDDEN], by_rows, preferred_element_type=jnp.float32
        )
    hidden = (gate * jax.nn.sigmoid(gate) * lift).astype(jnp.bfloat16)
    for u in range(TP):
        down = jnp.dot(hidden, weights_ref[u, 2 * HIDDEN :], preferred_element_type=jnp.float32)
        out_ref[:, u] = down.reshape(blocks, ROWS, FEATS).astype(jnp.bfloat16)


def first_partial(place, rows, weights):
    vmem = pl.BlockSpec(memory_space=pltpu.VMEM)
    return pl.pallas_call(
        first_kernel,
        out_shape=[
            pltpu.VMEM(rows.shape, jnp.bfloat16),
            pltpu.VMEM(rows.shape[1:], jnp.bfloat16),
        ],
        in_specs=[
            pl.BlockSpec(memory_space=pltpu.SMEM),
            vmem,
            pl.BlockSpec(memory_space=pltpu.HBM),
        ],
        out_specs=[vmem, vmem],
        scratch_shapes=[
            pltpu.VMEM((TP, Z * Y * ROWS, FEATS), jnp.bfloat16),
            pltpu.VMEM(weights.shape, jnp.bfloat16),
            pltpu.SemaphoreType.DMA((TP,)),
        ],
        compiler_params=pltpu.CompilerParams(vmem_limit_bytes=24 << 20),
        name="first_ffn",
    )(place, in_vmem(rows), in_hbm(weights))


def settle_kernel(rows_ref, share_ref, first_ref, copies_ref):
    for u in range(TP):
        branch = jnp.sum(share_ref[:, u].astype(jnp.float32), axis=0)
        own = rows_ref[u].astype(jnp.float32)
        first = (own + 0.5 * branch).astype(jnp.bfloat16)
        first_ref[u] = first
        for t in range(TP):
            copies_ref[t, u] = first


def settled(rows, share):
    shape = (TP, ROWS, FEATS)
    vmem = pl.BlockSpec(memory_space=pltpu.VMEM)
    return pl.pallas_call(
        settle_kernel,
        out_shape=[pltpu.VMEM(shape, jnp.bfloat16), pltpu.VMEM((TP, *shape), jnp.bfloat16)],
        in_specs=[vmem, vmem],
        out_specs=[vmem, vmem],
        compiler_params=pltpu.CompilerParams(vmem_limit_bytes=24 << 20),
        name="settle",
    )(in_vmem(rows), in_vmem(share))


def mix_kernel(first_ref, tiles_ref, copies_ref):
    mixed = jnp.sum(tiles_ref[...].astype(jnp.float32), axis=0)
    for u in range(TP):
        cols = slice(u * FEATS, (u + 1) * FEATS)
        rows = (first_ref[u].astype(jnp.float32) + mixed[:, cols]).astype(jnp.bfloat16)
        for z in range(Z):
            copies_ref[z, :, cols] = rows


def mixed_copies(first, tiles):
    vmem = pl.BlockSpec(memory_space=pltpu.VMEM)
    return pl.pallas_call(
        mix_kernel,
        out_shape=pltpu.VMEM((Z, ROWS, D), jnp.bfloat16),
        in_specs=[vmem, vmem],
        out_specs=vmem,
        compiler_params=pltpu.CompilerParams(vmem_limit_bytes=8 << 20),
        name="mix",
    )(in_vmem(first), in_vmem(tiles))


def second_kernel(
    place_ref, rows_ref, weights_hbm, out_ref, normed_ref, sum_ref, weights_ref, arrived
):
    rows = Z * ROWS
    copies = [
        pltpu.make_async_copy(weights_hbm.at[n], weights_ref.at[n], arrived.at[n])
        for n in range(Y * TP)
    ]
    for copy in copies:
        copy.start()
    values = rows_ref[...].astype(jnp.float32).reshape(rows, D)
    factor = lax.rsqrt(jnp.sum(values * values, axis=-1, keepdims=True) * (1.0 / D) + norm_eps)
    row = lax.broadcasted_iota(jnp.int32, (rows, 1), 0)
    own = jnp.where(row // ROWS == place_ref[1], 2.0, 0.0)
    for u in range(TP):
        normed_ref[u] = (values[:, u * FEATS : (u + 1) * FEATS] * factor).astype(jnp.bfloat16)
    for y in range(Y):
        both = jnp.zeros((2 * HIDDEN, rows), jnp.float32)
        for u in range(TP):
            copies[y * TP + u].wait()
            both += lax.dot_general(
                weights_ref[y * TP + u, : 2 * HIDDEN],
                normed_ref[u],
                by_rows,
                preferred_element_type=jnp.float32,
            )
        gate, lift = both[:HIDDEN], both[HIDDEN:]
        hidden = (gate * jax.nn.sigmoid(gate) * lift).T.astype(jnp.bfloat16)
        for u in range(TP):
            down = jnp.dot(
                hidden, weights_ref[y * TP + u, 2 * HIDDEN :], preferred_element_type=jnp.float32
            )
            if y == 0:
                down += values[:, u * FEATS : (u + 1) * FEATS] * own
            else:
                down += sum_ref[u]
            if y < Y - 1:
                sum_ref[u] = down
            else:
                out_ref[:, u] = down.reshape(Z, ROWS, FEATS).astype(jnp.bfloat16)


def second_partial(place, rows, weights):
    vmem = pl.BlockSpec(memory_space=pltpu.VMEM)
    return pl.pallas_call(
        second_kernel,
        out_shape=pltpu.VMEM((Z, TP, ROWS, FEATS), jnp.bfloat16),
        in_specs=[
            pl.BlockSpec(memory_space=pltpu.SMEM),
            vmem,
            pl.BlockSpec(memory_space=pltpu.HBM),
        ],
        out_specs=vmem,
        scratch_shapes=[
            pltpu.VMEM((TP, Z * ROWS, FEATS), jnp.bfloat16),
            pltpu.VMEM((TP, Z * ROWS, FEATS), jnp.float32),
            pltpu.VMEM(weights.shape, jnp.bfloat16),
            pltpu.SemaphoreType.DMA((Y * TP,)),
        ],
        compiler_params=pltpu.CompilerParams(vmem_limit_bytes=24 << 20),
        name="second_ffn",
    )(place, in_vmem(rows), in_hbm(weights))


def last_kernel(share_ref, out_ref):
    branch = jnp.sum(share_ref[...].astype(jnp.float32), axis=0)
    out_ref[...] = (0.5 * branch).reshape(TP * ROWS, FEATS).astype(jnp.bfloat16)


def last_sum(share):
    return pl.pallas_call(
        last_kernel,
        out_shape=jax.ShapeDtypeStruct((TP * ROWS, FEATS), jnp.bfloat16),
        in_specs=[pl.BlockSpec(memory_space=pltpu.VMEM)],
        compiler_params=pltpu.CompilerParams(vmem_limit_bytes=8 << 20),
        name="last",
    )(in_vmem(share))


def conv_silu(newest, buffer_ref, taps_ref):
    taps = taps_ref[...].astype(jnp.float32)
    summed = newest.astype(jnp.float32) * taps[3:4]
    for k in range(3):
        summed += buffer_ref[k].astype(jnp.float32) * taps[k : k + 1]
    return summed * jax.nn.sigmoid(summed)


SEQS = TP * ROWS
BLOCK = 8
CHANNELS = 256
PER_DEVICE = 4


def mixer_kernel(
    rows_ref,
    gain_ref,
    gate_ref,
    input_ref,
    write_ref,
    read_hbm,
    step_ref,
    bias_ref,
    rate_ref,
    skip_ref,
    taps_input_ref,
    taps_write_ref,
    taps_read_ref,
    buffer_input_ref,
    buffer_write_ref,
    buffer_read_ref,
    state_ref,
    group_ref,
    output_hbm,
    mixed_ref,
    new_state_ref,
    normed_ref,
    gate_z_ref,
    xc_ref,
    added_ref,
    retain_ref,
    bc_ref,
    rc_ref,
    out_cols_ref,
    read_ref,
    output_ref,
    arrived,
):
    i = pl.program_id(0)
    read_copy = pltpu.make_async_copy(read_hbm, read_ref, arrived.at[0])
    output_copy = pltpu.make_async_copy(output_hbm, output_ref, arrived.at[1])

    @pl.when(i == 0)
    def _():
        read_copy.start()
        output_copy.start()
        total = jnp.zeros((TP, ROWS, 1), jnp.float32)
        for u in range(TP):
            values = rows_ref[:, u].astype(jnp.float32)
            total += jnp.sum(values * values, axis=-1, keepdims=True)
        factor = lax.rsqrt(total * (1.0 / D) + norm_eps)
        for u in range(TP):
            values = (rows_ref[:, u].astype(jnp.float32) * factor).reshape(SEQS, FEATS)
            cols = slice(u * FEATS, (u + 1) * FEATS)
            gain = gain_ref[cols].astype(jnp.float32).reshape(1, FEATS)
            normed_ref[:, cols] = (values * gain).astype(jnp.bfloat16)
        normed = normed_ref[...]

        def project(weight_ref):
            return jnp.dot(normed, weight_ref[...], preferred_element_type=jnp.float32).astype(
                jnp.bfloat16
            )

        gate_z_ref[...] = project(gate_ref)
        step_raw = lax.dot_general(
            normed, step_ref[...], by_rows, preferred_element_type=jnp.float32
        ).astype(jnp.bfloat16)
        xc = conv_silu(project(input_ref), buffer_input_ref, taps_input_ref)
        bc_ref[...] = conv_silu(project(write_ref), buffer_write_ref, taps_write_ref)
        read_copy.wait()
        rc_ref[...] = conv_silu(project(read_ref), buffer_read_ref, taps_read_ref)
        xc_ref[...] = xc
        step = jax.nn.softplus(step_raw.astype(jnp.float32) + bias_ref[...].reshape(1, PER_DEVICE))
        retain = jnp.exp(-step * jnp.exp(rate_ref[...].reshape(1, PER_DEVICE)))
        head = lax.broadcasted_iota(jnp.int32, (SEQS, CHANNELS), 1) // HEAD_DIM
        step_wide = jnp.zeros((SEQS, CHANNELS), jnp.float32)
        retain_wide = jnp.zeros((SEQS, CHANNELS), jnp.float32)
        for h in range(PER_DEVICE):
            step_wide = jnp.where(head == h, step[:, h : h + 1], step_wide)
            retain_wide = jnp.where(head == h, retain[:, h : h + 1], retain_wide)
        added = (step_wide * xc).T
        retain_cols = retain_wide.T
        for s in range(SEQS // BLOCK):
            added_ref[s] = added[:, s * BLOCK : (s + 1) * BLOCK]
            retain_ref[s] = retain_cols[:, s * BLOCK : (s + 1) * BLOCK]

    added = added_ref[i]
    retain = retain_ref[i]
    writes = bc_ref[pl.ds(pl.multiple_of(i * BLOCK, BLOCK), BLOCK)]
    reads = rc_ref[pl.ds(pl.multiple_of(i * BLOCK, BLOCK), BLOCK)].astype(jnp.bfloat16)
    column = lax.broadcasted_iota(jnp.int32, (CHANNELS, BLOCK), 1)
    cols = jnp.zeros((CHANNELS, BLOCK), jnp.float32)
    for b in range(BLOCK):
        new = []
        for h in range(PER_DEVICE):
            top = h * HEAD_DIM
            kept = jnp.broadcast_to(retain[top : top + 8, b : b + 1], (8, STATE))
            old = state_ref[i * BLOCK + b, h].reshape(HEAD_DIM // 8, 8, STATE) * kept[None]
            new.append(
                old.reshape(HEAD_DIM, STATE)
                + added[top : top + HEAD_DIM, b : b + 1] * writes[b : b + 1]
            )
            new_state_ref[b, h] = new[h]
        new = jnp.concatenate(new, axis=0).astype(jnp.bfloat16)
        read = lax.dot_general(new, reads, by_rows, preferred_element_type=jnp.float32)
        cols = jnp.where(column == b, read, cols)
    out_cols_ref[i] = cols

    @pl.when(i == pl.num_programs(0) - 1)
    def _():
        cols = jnp.concatenate([out_cols_ref[s] for s in range(SEQS // BLOCK)], axis=1)
        head = lax.broadcasted_iota(jnp.int32, (1, CHANNELS), 1) // HEAD_DIM
        skip_own = skip_ref[...].reshape(1, PER_DEVICE)
        skip = jnp.zeros((1, CHANNELS), jnp.float32)
        for h in range(PER_DEVICE):
            skip = jnp.where(head == h, skip_own[:, h : h + 1], skip)
        head_out = (cols.T + skip * xc_ref[...]).astype(jnp.bfloat16).astype(jnp.float32)
        gate_z = gate_z_ref[...].astype(jnp.float32)
        gated = head_out * (gate_z * jax.nn.sigmoid(gate_z))
        gated = gated * inverse_rms(gated) * group_ref[...].astype(jnp.float32).reshape(1, CHANNELS)
        output_copy.wait()
        part = jnp.dot(
            gated.astype(jnp.bfloat16), output_ref[...], preferred_element_type=jnp.float32
        )
        mixed_ref[...] = part.reshape(TP, ROWS, D).astype(jnp.bfloat16)


def state_mixer(first, rows, small, buffers, scan_state, group_gain, proj_output):
    operands = [rows, *small, *[b.transpose(1, 0, 2) for b in buffers]]
    operands += [scan_state, group_gain, proj_output]
    from_hbm = (5, len(operands) - 1)
    operands = [in_hbm(o) if n in from_hbm else in_vmem(o) for n, o in enumerate(operands)]
    specs = [pl.BlockSpec(memory_space=pltpu.VMEM) for _ in operands]
    for n in from_hbm:
        specs[n] = pl.BlockSpec(memory_space=pltpu.HBM)
    state_spec = pl.BlockSpec((BLOCK, PER_DEVICE, HEAD_DIM, STATE), lambda i: (i, 0, 0, 0))
    blocks = SEQS // BLOCK
    partial_out, state_out = pl.pallas_call(
        mixer_kernel,
        grid=(blocks,),
        out_shape=[
            pltpu.VMEM((TP, ROWS, D), jnp.bfloat16),
            jax.ShapeDtypeStruct(scan_state.shape, jnp.float32),
        ],
        in_specs=specs,
        out_specs=[pl.BlockSpec(memory_space=pltpu.VMEM), state_spec],
        scratch_shapes=[
            pltpu.VMEM((SEQS, D), jnp.bfloat16),
            pltpu.VMEM((SEQS, CHANNELS), jnp.bfloat16),
            pltpu.VMEM((SEQS, CHANNELS), jnp.float32),
            pltpu.VMEM((blocks, CHANNELS, BLOCK), jnp.float32),
            pltpu.VMEM((blocks, CHANNELS, BLOCK), jnp.float32),
            pltpu.VMEM((SEQS, STATE), jnp.float32),
            pltpu.VMEM((SEQS, STATE), jnp.float32),
            pltpu.VMEM((blocks, CHANNELS, BLOCK), jnp.float32),
            pltpu.VMEM((D, STATE), jnp.bfloat16),
            pltpu.VMEM((CHANNELS, D), jnp.bfloat16),
            pltpu.SemaphoreType.DMA((2,)),
        ],
        compiler_params=pltpu.CompilerParams(vmem_limit_bytes=24 << 20),
        name="mixer",
    )(*operands)
    tiles = lax.all_to_all(partial_out, TP_AXES, 0, 0, tiled=True)
    return (mixed_copies(first, tiles), state_out)


def per_device(
    residual,
    first_gain,
    first_gate,
    first_lift,
    first_down,
    mixer_gain,
    proj_gate,
    proj_input,
    proj_write,
    proj_read,
    proj_step,
    step_bias,
    rate_log,
    skip_gain,
    taps_input,
    taps_write,
    taps_read,
    buffer_input,
    buffer_write,
    buffer_read,
    scan_state,
    group_gain,
    proj_output,
    second_gain,
    second_gate,
    second_lift,
    second_down,
):
    place = jnp.stack([lax.axis_index(BLOCK_AXES), lax.axis_index("z")]).astype(jnp.int32)
    weights_one = lax.all_gather(
        weight_share(first_gain, first_gate, first_lift, first_down), TP_AXES
    )
    weights_two = lax.all_gather(
        weight_share(second_gain, second_gate, second_lift, second_down, place), ("y", *TP_AXES)
    )

    mine = lax.all_to_all(residual.reshape(TP, ROWS, FEATS), TP_AXES, 0, 0, tiled=True)
    tiles = sent_to_all(mine, BLOCK_AXES).reshape(Z * Y, TP, ROWS, FEATS)
    share, own = first_partial(place, tiles, weights_one)
    share = lax.all_to_all(share, BLOCK_AXES, 0, 0, tiled=True)
    first, copies = settled(own, share)

    mixed, state_out = state_mixer(
        first,
        lax.all_to_all(copies, TP_AXES, 0, 0, tiled=True),
        (
            mixer_gain,
            proj_gate,
            proj_input,
            proj_write,
            proj_read,
            proj_step.T,
            step_bias,
            rate_log,
            skip_gain,
            taps_input,
            taps_write,
            taps_read,
        ),
        (buffer_input, buffer_write, buffer_read),
        scan_state,
        group_gain,
        proj_output,
    )

    rows = lax.all_to_all(mixed, "z", 0, 0, tiled=True)
    share = second_partial(place, rows, weights_two)
    share = lax.all_to_all(share.reshape(-1, ROWS, FEATS), ("z", *TP_AXES), 0, 0, tiled=True)
    residual_out = last_sum(share.reshape(Z, TP, ROWS, FEATS))
    return (residual_out, state_out)


def solution(mesh):
    mesh = Mesh(mesh.devices.reshape(Z, Y, TP // 2, 2), (*KV_AXES, *TP_AXES))
    placed = (
        P(KV_AXES, TP_AXES),
        P(TP_AXES),
        P(TP_AXES, KV_AXES),
        P(TP_AXES, KV_AXES),
        P(KV_AXES, TP_AXES),
        P(),
        P(None, TP_AXES),
        P(None, TP_AXES),
        P(None, TP_AXES),
        P(None, TP_AXES),
        P(None, TP_AXES),
        P(TP_AXES),
        P(TP_AXES),
        P(TP_AXES),
        P(None, TP_AXES),
        P(None, TP_AXES),
        P(None, TP_AXES),
        P(KV_AXES, None, TP_AXES),
        P(KV_AXES, None, TP_AXES),
        P(KV_AXES, None, TP_AXES),
        P(KV_AXES, TP_AXES, None, None),
        P(TP_AXES),
        P(TP_AXES, None),
        P(TP_AXES),
        P(TP_AXES, KV_AXES),
        P(TP_AXES, KV_AXES),
        P(KV_AXES, TP_AXES),
    )
    return jax.shard_map(
        per_device,
        mesh=mesh,
        in_specs=placed,
        out_specs=(P(KV_AXES, TP_AXES), P(KV_AXES, TP_AXES, None, None)),
        check_vma=False,
    )
```

```python
import jax
import jax.numpy as jnp
from jax import lax
from jax.experimental import pallas as pl
from jax.experimental.pallas import tpu as pltpu
from jax.sharding import Mesh
from jax.sharding import PartitionSpec as P

D = 2048
HEAD_DIM = 64
STATE = 128
FEATS = 256
HIDDEN = 176
ROWS = 4
Z, Y, TP = 8, 4, 8

KV_AXES = ("z", "y")
TP_AXES = ("x", "core")
BLOCK_AXES = ("y", "z")

norm_eps = 1e-06

by_rows = (((1,), (1,)), ((), ()))


def sent_to_all(array, axis):
    length = lax.axis_size(axis)
    return lax.all_to_all(
        jnp.broadcast_to(array[None], (length, *array.shape)), axis, 0, 0, tiled=True
    )


def inverse_rms(values):
    return lax.rsqrt(jnp.mean(values * values, axis=-1, keepdims=True) + norm_eps)


def in_hbm(array):
    return pltpu.with_memory_space_constraint(array, pltpu.HBM)


def in_vmem(array):
    return pltpu.with_memory_space_constraint(array, pltpu.VMEM)


def share_kernel(place_ref, rows_ref, *refs):
    pieces_ref = refs[-1]
    pieces_ref[...] = rows_ref[...].astype(jnp.float32).reshape(TP, ROWS, FEATS).astype(
        jnp.bfloat16
    )
    for gain, gate, lift, down, out in (refs[0:4] + refs[8:9], refs[4:8] + refs[9:10]):
        gain_f = gain[...].astype(jnp.float32).reshape(1, FEATS)
        out[:HIDDEN] = (gate[...].astype(jnp.float32) * gain_f).astype(jnp.bfloat16)
        out[HIDDEN : 2 * HIDDEN] = (lift[...].astype(jnp.float32) * gain_f).astype(jnp.bfloat16)
        out[2 * HIDDEN :] = down[...]


def weight_shares(place, residual, *sets):
    operands = [residual]
    for gain, gate_weight, lift_weight, down_weight in sets:
        operands += [gain, gate_weight.T, lift_weight.T, down_weight]
    vmem = pl.BlockSpec(memory_space=pltpu.VMEM)
    share = jax.ShapeDtypeStruct((3 * HIDDEN, FEATS), jnp.bfloat16)
    return pl.pallas_call(
        share_kernel,
        out_shape=[share, share, pltpu.VMEM((TP, ROWS, FEATS), jnp.bfloat16)],
        compiler_params=pltpu.CompilerParams(vmem_limit_bytes=4 << 20),
        in_specs=[pl.BlockSpec(memory_space=pltpu.SMEM)] + [vmem for _ in operands],
        out_specs=[vmem] * 3,
        name="shares",
    )(place, *[in_hbm(operand) for operand in operands])


def first_kernel(
    place_ref, rows_ref, weights_hbm, out_ref, own_ref, normed_ref, weights_ref, arrived
):
    blocks = Z * Y
    count = blocks * ROWS
    copies = [
        pltpu.make_async_copy(weights_hbm.at[u], weights_ref.at[u], arrived.at[u])
        for u in range(TP)
    ]
    for copy in copies:
        copy.start()
    total = jnp.zeros((blocks, ROWS, 1), jnp.float32)
    for u in range(TP):
        values = rows_ref[:, u].astype(jnp.float32)
        total += jnp.sum(values * values, axis=-1, keepdims=True)
    factor = lax.rsqrt(total * (1.0 / D) + norm_eps)
    for u in range(TP):
        values = rows_ref[:, u].astype(jnp.float32) * factor
        normed_ref[u] = values.reshape(count, FEATS).astype(jnp.bfloat16)
    own_ref[...] = rows_ref[place_ref[0]]
    gate = jnp.zeros((count, HIDDEN), jnp.float32)
    lift = jnp.zeros((count, HIDDEN), jnp.float32)
    for u in range(TP):
        copies[u].wait()
        block = normed_ref[u]
        gate += lax.dot_general(
            block, weights_ref[u, :HIDDEN], by_rows, preferred_element_type=jnp.float32
        )
        lift += lax.dot_general(
            block, weights_ref[u, HIDDEN : 2 * HIDDEN], by_rows, preferred_element_type=jnp.float32
        )
    hidden = (gate * jax.nn.sigmoid(gate) * lift).astype(jnp.bfloat16)
    for u in range(TP):
        down = jnp.dot(hidden, weights_ref[u, 2 * HIDDEN :], preferred_element_type=jnp.float32)
        out_ref[:, u] = down.reshape(blocks, ROWS, FEATS).astype(jnp.bfloat16)


def first_partial(place, rows, weights):
    vmem = pl.BlockSpec(memory_space=pltpu.VMEM)
    return pl.pallas_call(
        first_kernel,
        out_shape=[
            pltpu.VMEM(rows.shape, jnp.bfloat16),
            pltpu.VMEM(rows.shape[1:], jnp.bfloat16),
        ],
        in_specs=[
            pl.BlockSpec(memory_space=pltpu.SMEM),
            vmem,
            pl.BlockSpec(memory_space=pltpu.HBM),
        ],
        out_specs=[vmem, vmem],
        scratch_shapes=[
            pltpu.VMEM((TP, Z * Y * ROWS, FEATS), jnp.bfloat16),
            pltpu.VMEM(weights.shape, jnp.bfloat16),
            pltpu.SemaphoreType.DMA((TP,)),
        ],
        compiler_params=pltpu.CompilerParams(vmem_limit_bytes=24 << 20),
        name="first_ffn",
    )(place, in_vmem(rows), in_hbm(weights))


def settle_kernel(rows_ref, share_ref, first_ref, copies_ref):
    for u in range(TP):
        branch = jnp.sum(share_ref[:, u].astype(jnp.float32), axis=0)
        own = rows_ref[u].astype(jnp.float32)
        first = (own + 0.5 * branch).astype(jnp.bfloat16)
        first_ref[u] = first
        for t in range(TP):
            copies_ref[t, u] = first


def settled(rows, share):
    shape = (TP, ROWS, FEATS)
    vmem = pl.BlockSpec(memory_space=pltpu.VMEM)
    return pl.pallas_call(
        settle_kernel,
        out_shape=[pltpu.VMEM(shape, jnp.bfloat16), pltpu.VMEM((TP, *shape), jnp.bfloat16)],
        in_specs=[vmem, vmem],
        out_specs=[vmem, vmem],
        compiler_params=pltpu.CompilerParams(vmem_limit_bytes=24 << 20),
        name="settle",
    )(in_vmem(rows), in_vmem(share))


def mix_kernel(first_ref, tiles_ref, copies_ref):
    mixed = jnp.sum(tiles_ref[...].astype(jnp.float32), axis=0)
    for u in range(TP):
        cols = slice(u * FEATS, (u + 1) * FEATS)
        rows = (first_ref[u].astype(jnp.float32) + mixed[:, cols]).astype(jnp.bfloat16)
        for z in range(Z):
            copies_ref[z, :, cols] = rows


def mixed_copies(first, tiles):
    vmem = pl.BlockSpec(memory_space=pltpu.VMEM)
    return pl.pallas_call(
        mix_kernel,
        out_shape=pltpu.VMEM((Z, ROWS, D), jnp.bfloat16),
        in_specs=[vmem, vmem],
        out_specs=vmem,
        compiler_params=pltpu.CompilerParams(vmem_limit_bytes=8 << 20),
        name="mix",
    )(in_vmem(first), in_vmem(tiles))


def second_kernel(
    place_ref, rows_ref, weights_hbm, out_ref, normed_ref, weights_ref, arrived
):
    rows = Z * ROWS
    copies = [
        pltpu.make_async_copy(weights_hbm.at[n], weights_ref.at[n], arrived.at[n])
        for n in range(Y * TP)
    ]
    for copy in copies:
        copy.start()
    values = rows_ref[...].astype(jnp.float32).reshape(rows, D)
    factor = lax.rsqrt(jnp.sum(values * values, axis=-1, keepdims=True) * (1.0 / D) + norm_eps)
    row = lax.broadcasted_iota(jnp.int32, (rows, 1), 0)
    own = jnp.where(row // ROWS == place_ref[1], 2.0, 0.0)
    for u in range(TP):
        normed_ref[u] = (values[:, u * FEATS : (u + 1) * FEATS] * factor).astype(jnp.bfloat16)
    hidden = []
    for y in range(Y):
        both = jnp.zeros((rows, 2 * HIDDEN), jnp.float32)
        for u in range(TP):
            copies[y * TP + u].wait()
        for u in range(TP):
            both += lax.dot_general(
                normed_ref[u],
                weights_ref[y * TP + u, : 2 * HIDDEN],
                by_rows,
                preferred_element_type=jnp.float32,
            )
        gate, lift = both[:, :HIDDEN], both[:, HIDDEN:]
        hidden.append((gate * jax.nn.sigmoid(gate) * lift).astype(jnp.bfloat16))
    for u in range(TP):
        down = values[:, u * FEATS : (u + 1) * FEATS] * own
        for y in range(Y):
            down += jnp.dot(
                hidden[y],
                weights_ref[y * TP + u, 2 * HIDDEN :],
                preferred_element_type=jnp.float32,
            )
        out_ref[:, u] = down.reshape(Z, ROWS, FEATS).astype(jnp.bfloat16)


def second_partial(place, rows, weights):
    vmem = pl.BlockSpec(memory_space=pltpu.VMEM)
    return pl.pallas_call(
        second_kernel,
        out_shape=pltpu.VMEM((Z, TP, ROWS, FEATS), jnp.bfloat16),
        in_specs=[
            pl.BlockSpec(memory_space=pltpu.SMEM),
            vmem,
            pl.BlockSpec(memory_space=pltpu.HBM),
        ],
        out_specs=vmem,
        scratch_shapes=[
            pltpu.VMEM((TP, Z * ROWS, FEATS), jnp.bfloat16),
            pltpu.VMEM(weights.shape, jnp.bfloat16),
            pltpu.SemaphoreType.DMA((Y * TP,)),
        ],
        compiler_params=pltpu.CompilerParams(vmem_limit_bytes=24 << 20),
        name="second_ffn",
    )(place, in_vmem(rows), in_hbm(weights))


def last_kernel(share_ref, out_ref):
    branch = jnp.sum(share_ref[...].astype(jnp.float32), axis=0)
    out_ref[...] = (0.5 * branch).reshape(TP * ROWS, FEATS).astype(jnp.bfloat16)


def last_sum(share):
    return pl.pallas_call(
        last_kernel,
        out_shape=jax.ShapeDtypeStruct((TP * ROWS, FEATS), jnp.bfloat16),
        in_specs=[pl.BlockSpec(memory_space=pltpu.VMEM)],
        compiler_params=pltpu.CompilerParams(vmem_limit_bytes=8 << 20),
        name="last",
    )(in_vmem(share))


def conv_silu(newest, buffer_ref, taps_ref):
    taps = taps_ref[...].astype(jnp.float32)
    summed = newest.astype(jnp.float32) * taps[3:4]
    for k in range(3):
        summed += buffer_ref[k].astype(jnp.float32) * taps[k : k + 1]
    return summed * jax.nn.sigmoid(summed)


SEQS = TP * ROWS
BLOCK = 8
CHANNELS = 256
PER_DEVICE = 4


def mixer_kernel(
    rows_ref,
    gain_ref,
    gate_ref,
    input_ref,
    write_ref,
    read_hbm,
    step_ref,
    bias_ref,
    rate_ref,
    skip_ref,
    taps_input_ref,
    taps_write_ref,
    taps_read_ref,
    buffer_input_ref,
    buffer_write_ref,
    buffer_read_ref,
    state_ref,
    group_ref,
    output_hbm,
    mixed_ref,
    new_state_ref,
    normed_ref,
    gate_z_ref,
    xc_ref,
    added_ref,
    retain_ref,
    bc_ref,
    rc_ref,
    out_cols_ref,
    read_ref,
    output_ref,
    arrived,
):
    i = pl.program_id(0)
    read_copy = pltpu.make_async_copy(read_hbm, read_ref, arrived.at[0])
    output_copy = pltpu.make_async_copy(output_hbm, output_ref, arrived.at[1])

    @pl.when(i == 0)
    def _():
        read_copy.start()
        output_copy.start()
        total = jnp.zeros((TP, ROWS, 1), jnp.float32)
        for u in range(TP):
            values = rows_ref[:, u].astype(jnp.float32)
            total += jnp.sum(values * values, axis=-1, keepdims=True)
        factor = lax.rsqrt(total * (1.0 / D) + norm_eps)
        for u in range(TP):
            values = (rows_ref[:, u].astype(jnp.float32) * factor).reshape(SEQS, FEATS)
            cols = slice(u * FEATS, (u + 1) * FEATS)
            gain = gain_ref[cols].astype(jnp.float32).reshape(1, FEATS)
            normed_ref[:, cols] = (values * gain).astype(jnp.bfloat16)
        normed = normed_ref[...]

        def project(weight_ref):
            return jnp.dot(normed, weight_ref[...], preferred_element_type=jnp.float32).astype(
                jnp.bfloat16
            )

        gate_z_ref[...] = project(gate_ref)
        step_raw = lax.dot_general(
            normed, step_ref[...], by_rows, preferred_element_type=jnp.float32
        ).astype(jnp.bfloat16)
        xc = conv_silu(project(input_ref), buffer_input_ref, taps_input_ref)
        bc_ref[...] = conv_silu(project(write_ref), buffer_write_ref, taps_write_ref)
        read_copy.wait()
        rc_ref[...] = conv_silu(project(read_ref), buffer_read_ref, taps_read_ref)
        xc_ref[...] = xc
        step = jax.nn.softplus(step_raw.astype(jnp.float32) + bias_ref[...].reshape(1, PER_DEVICE))
        retain = jnp.exp(-step * jnp.exp(rate_ref[...].reshape(1, PER_DEVICE)))
        head = lax.broadcasted_iota(jnp.int32, (SEQS, CHANNELS), 1) // HEAD_DIM
        step_wide = jnp.zeros((SEQS, CHANNELS), jnp.float32)
        retain_wide = jnp.zeros((SEQS, CHANNELS), jnp.float32)
        for h in range(PER_DEVICE):
            step_wide = jnp.where(head == h, step[:, h : h + 1], step_wide)
            retain_wide = jnp.where(head == h, retain[:, h : h + 1], retain_wide)
        added = (step_wide * xc).T
        retain_cols = retain_wide.T
        for s in range(SEQS // BLOCK):
            added_ref[s] = added[:, s * BLOCK : (s + 1) * BLOCK]
            retain_ref[s] = retain_cols[:, s * BLOCK : (s + 1) * BLOCK]

    added = added_ref[i]
    retain = retain_ref[i]
    writes = bc_ref[pl.ds(pl.multiple_of(i * BLOCK, BLOCK), BLOCK)]
    reads = rc_ref[pl.ds(pl.multiple_of(i * BLOCK, BLOCK), BLOCK)].astype(jnp.bfloat16)
    column = lax.broadcasted_iota(jnp.int32, (CHANNELS, BLOCK), 1)
    cols = jnp.zeros((CHANNELS, BLOCK), jnp.float32)
    for b in range(BLOCK):
        new = []
        for h in range(PER_DEVICE):
            top = h * HEAD_DIM
            kept = jnp.broadcast_to(retain[top : top + 8, b : b + 1], (8, STATE))
            old = state_ref[i * BLOCK + b, h].reshape(HEAD_DIM // 8, 8, STATE) * kept[None]
            new.append(
                old.reshape(HEAD_DIM, STATE)
                + added[top : top + HEAD_DIM, b : b + 1] * writes[b : b + 1]
            )
            new_state_ref[b, h] = new[h]
        new = jnp.concatenate(new, axis=0).astype(jnp.bfloat16)
        read = lax.dot_general(new, reads, by_rows, preferred_element_type=jnp.float32)
        cols = jnp.where(column == b, read, cols)
    out_cols_ref[i] = cols

    @pl.when(i == pl.num_programs(0) - 1)
    def _():
        cols = jnp.concatenate([out_cols_ref[s] for s in range(SEQS // BLOCK)], axis=1)
        head = lax.broadcasted_iota(jnp.int32, (1, CHANNELS), 1) // HEAD_DIM
        skip_own = skip_ref[...].reshape(1, PER_DEVICE)
        skip = jnp.zeros((1, CHANNELS), jnp.float32)
        for h in range(PER_DEVICE):
            skip = jnp.where(head == h, skip_own[:, h : h + 1], skip)
        head_out = (cols.T + skip * xc_ref[...]).astype(jnp.bfloat16).astype(jnp.float32)
        gate_z = gate_z_ref[...].astype(jnp.float32)
        gated = head_out * (gate_z * jax.nn.sigmoid(gate_z))
        gated = gated * inverse_rms(gated) * group_ref[...].astype(jnp.float32).reshape(1, CHANNELS)
        output_copy.wait()
        part = jnp.dot(
            gated.astype(jnp.bfloat16), output_ref[...], preferred_element_type=jnp.float32
        )
        mixed_ref[...] = part.reshape(TP, ROWS, D).astype(jnp.bfloat16)


def state_mixer(first, rows, small, buffers, scan_state, group_gain, proj_output):
    operands = [rows, *small, *[b.transpose(1, 0, 2) for b in buffers]]
    operands += [scan_state, group_gain, proj_output]
    from_hbm = (5, len(operands) - 1)
    operands = [in_hbm(o) if n in from_hbm else in_vmem(o) for n, o in enumerate(operands)]
    specs = [pl.BlockSpec(memory_space=pltpu.VMEM) for _ in operands]
    for n in from_hbm:
        specs[n] = pl.BlockSpec(memory_space=pltpu.HBM)
    state_spec = pl.BlockSpec((BLOCK, PER_DEVICE, HEAD_DIM, STATE), lambda i: (i, 0, 0, 0))
    blocks = SEQS // BLOCK
    partial_out, state_out = pl.pallas_call(
        mixer_kernel,
        grid=(blocks,),
        out_shape=[
            pltpu.VMEM((TP, ROWS, D), jnp.bfloat16),
            jax.ShapeDtypeStruct(scan_state.shape, jnp.float32),
        ],
        in_specs=specs,
        out_specs=[pl.BlockSpec(memory_space=pltpu.VMEM), state_spec],
        scratch_shapes=[
            pltpu.VMEM((SEQS, D), jnp.bfloat16),
            pltpu.VMEM((SEQS, CHANNELS), jnp.bfloat16),
            pltpu.VMEM((SEQS, CHANNELS), jnp.float32),
            pltpu.VMEM((blocks, CHANNELS, BLOCK), jnp.float32),
            pltpu.VMEM((blocks, CHANNELS, BLOCK), jnp.float32),
            pltpu.VMEM((SEQS, STATE), jnp.float32),
            pltpu.VMEM((SEQS, STATE), jnp.float32),
            pltpu.VMEM((blocks, CHANNELS, BLOCK), jnp.float32),
            pltpu.VMEM((D, STATE), jnp.bfloat16),
            pltpu.VMEM((CHANNELS, D), jnp.bfloat16),
            pltpu.SemaphoreType.DMA((2,)),
        ],
        compiler_params=pltpu.CompilerParams(vmem_limit_bytes=24 << 20),
        name="mixer",
    )(*operands)
    tiles = lax.all_to_all(partial_out, TP_AXES, 0, 0, tiled=True)
    return (mixed_copies(first, tiles), state_out)


def per_device(
    residual,
    first_gain,
    first_gate,
    first_lift,
    first_down,
    mixer_gain,
    proj_gate,
    proj_input,
    proj_write,
    proj_read,
    proj_step,
    step_bias,
    rate_log,
    skip_gain,
    taps_input,
    taps_write,
    taps_read,
    buffer_input,
    buffer_write,
    buffer_read,
    scan_state,
    group_gain,
    proj_output,
    second_gain,
    second_gate,
    second_lift,
    second_down,
):
    place = jnp.stack([lax.axis_index(BLOCK_AXES), lax.axis_index("z")]).astype(jnp.int32)
    share_one, share_two, pieces = weight_shares(
        place,
        residual,
        (first_gain, first_gate, first_lift, first_down),
        (second_gain, second_gate, second_lift, second_down),
    )
    weights_one = lax.all_gather(share_one, TP_AXES)
    weights_two = lax.all_gather(share_two, ("y", *TP_AXES))

    mine = lax.all_to_all(pieces, TP_AXES, 0, 0, tiled=True)
    tiles = sent_to_all(mine, BLOCK_AXES).reshape(Z * Y, TP, ROWS, FEATS)
    share, own = first_partial(place, tiles, weights_one)
    share = lax.all_to_all(share, BLOCK_AXES, 0, 0, tiled=True)
    first, copies = settled(own, share)

    mixed, state_out = state_mixer(
        first,
        lax.all_to_all(copies, TP_AXES, 0, 0, tiled=True),
        (
            mixer_gain,
            proj_gate,
            proj_input,
            proj_write,
            proj_read,
            proj_step.T,
            step_bias,
            rate_log,
            skip_gain,
            taps_input,
            taps_write,
            taps_read,
        ),
        (buffer_input, buffer_write, buffer_read),
        scan_state,
        group_gain,
        proj_output,
    )

    rows = lax.all_to_all(mixed, "z", 0, 0, tiled=True)
    share = second_partial(place, rows, weights_two)
    share = lax.all_to_all(share.reshape(-1, ROWS, FEATS), ("z", *TP_AXES), 0, 0, tiled=True)
    residual_out = last_sum(share.reshape(Z, TP, ROWS, FEATS))
    return (residual_out, state_out)


def solution(mesh):
    mesh = Mesh(mesh.devices.reshape(Z, Y, TP // 2, 2), (*KV_AXES, *TP_AXES))
    placed = (
        P(KV_AXES, TP_AXES),
        P(TP_AXES),
        P(TP_AXES, KV_AXES),
        P(TP_AXES, KV_AXES),
        P(KV_AXES, TP_AXES),
        P(),
        P(None, TP_AXES),
        P(None, TP_AXES),
        P(None, TP_AXES),
        P(None, TP_AXES),
        P(None, TP_AXES),
        P(TP_AXES),
        P(TP_AXES),
        P(TP_AXES),
        P(None, TP_AXES),
        P(None, TP_AXES),
        P(None, TP_AXES),
        P(KV_AXES, None, TP_AXES),
        P(KV_AXES, None, TP_AXES),
        P(KV_AXES, None, TP_AXES),
        P(KV_AXES, TP_AXES, None, None),
        P(TP_AXES),
        P(TP_AXES, None),
        P(TP_AXES),
        P(TP_AXES, KV_AXES),
        P(TP_AXES, KV_AXES),
        P(KV_AXES, TP_AXES),
    )
    return jax.shard_map(
        per_device,
        mesh=mesh,
        in_specs=placed,
        out_specs=(P(KV_AXES, TP_AXES), P(KV_AXES, TP_AXES, None, None)),
        check_vma=False,
    )
```

```python
import jax
import jax.numpy as jnp
from jax import lax
from jax.experimental import pallas as pl
from jax.experimental.pallas import tpu as pltpu
from jax.sharding import Mesh
from jax.sharding import PartitionSpec as P

D = 2048
HEAD_DIM = 64
STATE = 128
FEATS = 256
HIDDEN = 176
ROWS = 4
Z, Y, TP = 8, 4, 8

KV_AXES = ("z", "y_hi", "y_lo")
TP_AXES = ("x", "core")
BLOCK_AXES = ("y_hi", "y_lo", "z")
PAIR = 2
ROW_AXES = ("z", "y_hi")
ROW_BLOCKS = Z * Y // PAIR

norm_eps = 1e-06

by_rows = (((1,), (1,)), ((), ()))


def sent_to_all(array, axis):
    length = lax.axis_size(axis)
    return lax.all_to_all(
        jnp.broadcast_to(array[None], (length, *array.shape)), axis, 0, 0, tiled=True
    )


def inverse_rms(values):
    return lax.rsqrt(jnp.mean(values * values, axis=-1, keepdims=True) + norm_eps)


def in_hbm(array):
    return pltpu.with_memory_space_constraint(array, pltpu.HBM)


def in_vmem(array):
    return pltpu.with_memory_space_constraint(array, pltpu.VMEM)


def share_kernel(place_ref, rows_ref, *refs):
    pieces_ref = refs[-1]
    pieces_ref[...] = rows_ref[...].astype(jnp.float32).reshape(TP, ROWS, FEATS).astype(
        jnp.bfloat16
    )
    for gain, gate, lift, down, out in (refs[0:4] + refs[8:9], refs[4:8] + refs[9:10]):
        gain_f = gain[...].astype(jnp.float32).reshape(1, FEATS)
        out[:HIDDEN] = (gate[...].astype(jnp.float32) * gain_f).astype(jnp.bfloat16)
        out[HIDDEN : 2 * HIDDEN] = (lift[...].astype(jnp.float32) * gain_f).astype(jnp.bfloat16)
        out[2 * HIDDEN :] = down[...]


def weight_shares(place, residual, *sets):
    operands = [residual]
    for gain, gate_weight, lift_weight, down_weight in sets:
        operands += [gain, gate_weight.T, lift_weight.T, down_weight]
    vmem = pl.BlockSpec(memory_space=pltpu.VMEM)
    share = jax.ShapeDtypeStruct((3 * HIDDEN, FEATS), jnp.bfloat16)
    return pl.pallas_call(
        share_kernel,
        out_shape=[share, share, pltpu.VMEM((TP, ROWS, FEATS), jnp.bfloat16)],
        compiler_params=pltpu.CompilerParams(vmem_limit_bytes=4 << 20),
        in_specs=[pl.BlockSpec(memory_space=pltpu.SMEM)] + [vmem for _ in operands],
        out_specs=[vmem] * 3,
        name="shares",
    )(place, *[in_hbm(operand) for operand in operands])


def first_kernel(
    place_ref, rows_ref, weights_hbm, out_ref, own_ref, normed_ref, weights_ref, arrived
):
    blocks = Z * Y
    count = blocks * ROWS
    copies = [
        pltpu.make_async_copy(weights_hbm.at[u], weights_ref.at[u], arrived.at[u])
        for u in range(TP)
    ]
    for copy in copies:
        copy.start()
    total = jnp.zeros((blocks, ROWS, 1), jnp.float32)
    for u in range(TP):
        values = rows_ref[:, u].astype(jnp.float32)
        total += jnp.sum(values * values, axis=-1, keepdims=True)
    factor = lax.rsqrt(total * (1.0 / D) + norm_eps)
    for u in range(TP):
        values = rows_ref[:, u].astype(jnp.float32) * factor
        normed_ref[u] = values.reshape(count, FEATS).astype(jnp.bfloat16)
    own_ref[...] = rows_ref[place_ref[0]]
    gate = jnp.zeros((count, HIDDEN), jnp.float32)
    lift = jnp.zeros((count, HIDDEN), jnp.float32)
    for u in range(TP):
        copies[u].wait()
        block = normed_ref[u]
        gate += lax.dot_general(
            block, weights_ref[u, :HIDDEN], by_rows, preferred_element_type=jnp.float32
        )
        lift += lax.dot_general(
            block, weights_ref[u, HIDDEN : 2 * HIDDEN], by_rows, preferred_element_type=jnp.float32
        )
    hidden = (gate * jax.nn.sigmoid(gate) * lift).astype(jnp.bfloat16)
    for u in range(TP):
        down = jnp.dot(hidden, weights_ref[u, 2 * HIDDEN :], preferred_element_type=jnp.float32)
        out_ref[:, u] = down.reshape(blocks, ROWS, FEATS).astype(jnp.bfloat16)


def first_partial(place, rows, weights):
    vmem = pl.BlockSpec(memory_space=pltpu.VMEM)
    return pl.pallas_call(
        first_kernel,
        out_shape=[
            pltpu.VMEM(rows.shape, jnp.bfloat16),
            pltpu.VMEM(rows.shape[1:], jnp.bfloat16),
        ],
        in_specs=[
            pl.BlockSpec(memory_space=pltpu.SMEM),
            vmem,
            pl.BlockSpec(memory_space=pltpu.HBM),
        ],
        out_specs=[vmem, vmem],
        scratch_shapes=[
            pltpu.VMEM((TP, Z * Y * ROWS, FEATS), jnp.bfloat16),
            pltpu.VMEM(weights.shape, jnp.bfloat16),
            pltpu.SemaphoreType.DMA((TP,)),
        ],
        compiler_params=pltpu.CompilerParams(vmem_limit_bytes=24 << 20),
        name="first_ffn",
    )(place, in_vmem(rows), in_hbm(weights))


def settle_kernel(rows_ref, share_ref, first_ref, copies_ref):
    for u in range(TP):
        branch = jnp.sum(share_ref[:, u].astype(jnp.float32), axis=0)
        own = rows_ref[u].astype(jnp.float32)
        first = (own + 0.5 * branch).astype(jnp.bfloat16)
        first_ref[u] = first
        for t in range(TP):
            copies_ref[t, u] = first


def settled(rows, share):
    shape = (TP, ROWS, FEATS)
    vmem = pl.BlockSpec(memory_space=pltpu.VMEM)
    return pl.pallas_call(
        settle_kernel,
        out_shape=[pltpu.VMEM(shape, jnp.bfloat16), pltpu.VMEM((TP, *shape), jnp.bfloat16)],
        in_specs=[vmem, vmem],
        out_specs=[vmem, vmem],
        compiler_params=pltpu.CompilerParams(vmem_limit_bytes=24 << 20),
        name="settle",
    )(in_vmem(rows), in_vmem(share))


def mix_kernel(first_ref, tiles_ref, copies_ref):
    mixed = jnp.sum(tiles_ref[...].astype(jnp.float32), axis=0)
    for u in range(TP):
        cols = slice(u * FEATS, (u + 1) * FEATS)
        rows = (first_ref[u].astype(jnp.float32) + mixed[:, cols]).astype(jnp.bfloat16)
        for n in range(ROW_BLOCKS):
            copies_ref[n, :, cols] = rows


def mixed_copies(first, tiles):
    vmem = pl.BlockSpec(memory_space=pltpu.VMEM)
    return pl.pallas_call(
        mix_kernel,
        out_shape=pltpu.VMEM((ROW_BLOCKS, ROWS, D), jnp.bfloat16),
        in_specs=[vmem, vmem],
        out_specs=vmem,
        compiler_params=pltpu.CompilerParams(vmem_limit_bytes=8 << 20),
        name="mix",
    )(in_vmem(first), in_vmem(tiles))


def second_kernel(
    place_ref, rows_ref, weights_hbm, out_ref, normed_ref, weights_ref, arrived
):
    rows = ROW_BLOCKS * ROWS
    copies = [
        pltpu.make_async_copy(weights_hbm.at[n], weights_ref.at[n], arrived.at[n])
        for n in range(PAIR * TP)
    ]
    for copy in copies:
        copy.start()
    values = rows_ref[...].astype(jnp.float32).reshape(rows, D)
    factor = lax.rsqrt(jnp.sum(values * values, axis=-1, keepdims=True) * (1.0 / D) + norm_eps)
    row = lax.broadcasted_iota(jnp.int32, (rows, 1), 0)
    own = jnp.where(row // ROWS == place_ref[1], 2.0, 0.0)
    for u in range(TP):
        normed_ref[u] = (values[:, u * FEATS : (u + 1) * FEATS] * factor).astype(jnp.bfloat16)
    hidden = []
    for y in range(PAIR):
        both = jnp.zeros((rows, 2 * HIDDEN), jnp.float32)
        for u in range(TP):
            copies[y * TP + u].wait()
        for u in range(TP):
            both += lax.dot_general(
                normed_ref[u],
                weights_ref[y * TP + u, : 2 * HIDDEN],
                by_rows,
                preferred_element_type=jnp.float32,
            )
        gate, lift = both[:, :HIDDEN], both[:, HIDDEN:]
        hidden.append((gate * jax.nn.sigmoid(gate) * lift).astype(jnp.bfloat16))
    for u in range(TP):
        down = values[:, u * FEATS : (u + 1) * FEATS] * own
        for y in range(PAIR):
            down += jnp.dot(
                hidden[y],
                weights_ref[y * TP + u, 2 * HIDDEN :],
                preferred_element_type=jnp.float32,
            )
        out_ref[:, u] = down.reshape(ROW_BLOCKS, ROWS, FEATS).astype(jnp.bfloat16)


def second_partial(place, rows, weights):
    vmem = pl.BlockSpec(memory_space=pltpu.VMEM)
    return pl.pallas_call(
        second_kernel,
        out_shape=pltpu.VMEM((ROW_BLOCKS, TP, ROWS, FEATS), jnp.bfloat16),
        in_specs=[
            pl.BlockSpec(memory_space=pltpu.SMEM),
            vmem,
            pl.BlockSpec(memory_space=pltpu.HBM),
        ],
        out_specs=vmem,
        scratch_shapes=[
            pltpu.VMEM((TP, ROW_BLOCKS * ROWS, FEATS), jnp.bfloat16),
            pltpu.VMEM(weights.shape, jnp.bfloat16),
            pltpu.SemaphoreType.DMA((PAIR * TP,)),
        ],
        compiler_params=pltpu.CompilerParams(vmem_limit_bytes=24 << 20),
        name="second_ffn",
    )(place, in_vmem(rows), in_hbm(weights))


def last_kernel(share_ref, out_ref):
    branch = jnp.sum(share_ref[...].astype(jnp.float32), axis=0)
    out_ref[...] = (0.5 * branch).reshape(TP * ROWS, FEATS).astype(jnp.bfloat16)


def last_sum(share):
    return pl.pallas_call(
        last_kernel,
        out_shape=jax.ShapeDtypeStruct((TP * ROWS, FEATS), jnp.bfloat16),
        in_specs=[pl.BlockSpec(memory_space=pltpu.VMEM)],
        compiler_params=pltpu.CompilerParams(vmem_limit_bytes=8 << 20),
        name="last",
    )(in_vmem(share))


def conv_silu(newest, buffer_ref, taps_ref):
    taps = taps_ref[...].astype(jnp.float32)
    summed = newest.astype(jnp.float32) * taps[3:4]
    for k in range(3):
        summed += buffer_ref[k].astype(jnp.float32) * taps[k : k + 1]
    return summed * jax.nn.sigmoid(summed)


SEQS = TP * ROWS
BLOCK = 8
CHANNELS = 256
PER_DEVICE = 4


def mixer_kernel(
    rows_ref,
    gain_ref,
    gate_ref,
    input_ref,
    write_ref,
    read_hbm,
    step_ref,
    bias_ref,
    rate_ref,
    skip_ref,
    taps_input_ref,
    taps_write_ref,
    taps_read_ref,
    buffer_input_ref,
    buffer_write_ref,
    buffer_read_ref,
    state_ref,
    group_ref,
    output_hbm,
    mixed_ref,
    new_state_ref,
    normed_ref,
    gate_z_ref,
    xc_ref,
    added_ref,
    retain_ref,
    bc_ref,
    rc_ref,
    out_cols_ref,
    read_ref,
    output_ref,
    arrived,
):
    i = pl.program_id(0)
    read_copy = pltpu.make_async_copy(read_hbm, read_ref, arrived.at[0])
    output_copy = pltpu.make_async_copy(output_hbm, output_ref, arrived.at[1])

    @pl.when(i == 0)
    def _():
        read_copy.start()
        output_copy.start()
        total = jnp.zeros((TP, ROWS, 1), jnp.float32)
        for u in range(TP):
            values = rows_ref[:, u].astype(jnp.float32)
            total += jnp.sum(values * values, axis=-1, keepdims=True)
        factor = lax.rsqrt(total * (1.0 / D) + norm_eps)
        for u in range(TP):
            values = (rows_ref[:, u].astype(jnp.float32) * factor).reshape(SEQS, FEATS)
            cols = slice(u * FEATS, (u + 1) * FEATS)
            gain = gain_ref[cols].astype(jnp.float32).reshape(1, FEATS)
            normed_ref[:, cols] = (values * gain).astype(jnp.bfloat16)
        normed = normed_ref[...]

        def project(weight_ref):
            return jnp.dot(normed, weight_ref[...], preferred_element_type=jnp.float32).astype(
                jnp.bfloat16
            )

        gate_z_ref[...] = project(gate_ref)
        step_raw = lax.dot_general(
            normed, step_ref[...], by_rows, preferred_element_type=jnp.float32
        ).astype(jnp.bfloat16)
        xc = conv_silu(project(input_ref), buffer_input_ref, taps_input_ref)
        bc_ref[...] = conv_silu(project(write_ref), buffer_write_ref, taps_write_ref)
        read_copy.wait()
        rc_ref[...] = conv_silu(project(read_ref), buffer_read_ref, taps_read_ref)
        xc_ref[...] = xc
        step = jax.nn.softplus(step_raw.astype(jnp.float32) + bias_ref[...].reshape(1, PER_DEVICE))
        retain = jnp.exp(-step * jnp.exp(rate_ref[...].reshape(1, PER_DEVICE)))
        head = lax.broadcasted_iota(jnp.int32, (SEQS, CHANNELS), 1) // HEAD_DIM
        step_wide = jnp.zeros((SEQS, CHANNELS), jnp.float32)
        retain_wide = jnp.zeros((SEQS, CHANNELS), jnp.float32)
        for h in range(PER_DEVICE):
            step_wide = jnp.where(head == h, step[:, h : h + 1], step_wide)
            retain_wide = jnp.where(head == h, retain[:, h : h + 1], retain_wide)
        added = (step_wide * xc).T
        retain_cols = retain_wide.T
        for s in range(SEQS // BLOCK):
            added_ref[s] = added[:, s * BLOCK : (s + 1) * BLOCK]
            retain_ref[s] = retain_cols[:, s * BLOCK : (s + 1) * BLOCK]

    added = added_ref[i]
    retain = retain_ref[i]
    writes = bc_ref[pl.ds(pl.multiple_of(i * BLOCK, BLOCK), BLOCK)]
    reads = rc_ref[pl.ds(pl.multiple_of(i * BLOCK, BLOCK), BLOCK)].astype(jnp.bfloat16)
    column = lax.broadcasted_iota(jnp.int32, (CHANNELS, BLOCK), 1)
    cols = jnp.zeros((CHANNELS, BLOCK), jnp.float32)
    for b in range(BLOCK):
        new = []
        for h in range(PER_DEVICE):
            top = h * HEAD_DIM
            kept = jnp.broadcast_to(retain[top : top + 8, b : b + 1], (8, STATE))
            old = state_ref[i * BLOCK + b, h].reshape(HEAD_DIM // 8, 8, STATE) * kept[None]
            new.append(
                old.reshape(HEAD_DIM, STATE)
                + added[top : top + HEAD_DIM, b : b + 1] * writes[b : b + 1]
            )
            new_state_ref[b, h] = new[h]
        new = jnp.concatenate(new, axis=0).astype(jnp.bfloat16)
        read = lax.dot_general(new, reads, by_rows, preferred_element_type=jnp.float32)
        cols = jnp.where(column == b, read, cols)
    out_cols_ref[i] = cols

    @pl.when(i == pl.num_programs(0) - 1)
    def _():
        cols = jnp.concatenate([out_cols_ref[s] for s in range(SEQS // BLOCK)], axis=1)
        head = lax.broadcasted_iota(jnp.int32, (1, CHANNELS), 1) // HEAD_DIM
        skip_own = skip_ref[...].reshape(1, PER_DEVICE)
        skip = jnp.zeros((1, CHANNELS), jnp.float32)
        for h in range(PER_DEVICE):
            skip = jnp.where(head == h, skip_own[:, h : h + 1], skip)
        head_out = (cols.T + skip * xc_ref[...]).astype(jnp.bfloat16).astype(jnp.float32)
        gate_z = gate_z_ref[...].astype(jnp.float32)
        gated = head_out * (gate_z * jax.nn.sigmoid(gate_z))
        gated = gated * inverse_rms(gated) * group_ref[...].astype(jnp.float32).reshape(1, CHANNELS)
        output_copy.wait()
        part = jnp.dot(
            gated.astype(jnp.bfloat16), output_ref[...], preferred_element_type=jnp.float32
        )
        mixed_ref[...] = part.reshape(TP, ROWS, D).astype(jnp.bfloat16)


def state_mixer(first, rows, small, buffers, scan_state, group_gain, proj_output):
    operands = [rows, *small, *[b.transpose(1, 0, 2) for b in buffers]]
    operands += [scan_state, group_gain, proj_output]
    from_hbm = (5, len(operands) - 1)
    operands = [in_hbm(o) if n in from_hbm else in_vmem(o) for n, o in enumerate(operands)]
    specs = [pl.BlockSpec(memory_space=pltpu.VMEM) for _ in operands]
    for n in from_hbm:
        specs[n] = pl.BlockSpec(memory_space=pltpu.HBM)
    state_spec = pl.BlockSpec((BLOCK, PER_DEVICE, HEAD_DIM, STATE), lambda i: (i, 0, 0, 0))
    blocks = SEQS // BLOCK
    partial_out, state_out = pl.pallas_call(
        mixer_kernel,
        grid=(blocks,),
        out_shape=[
            pltpu.VMEM((TP, ROWS, D), jnp.bfloat16),
            jax.ShapeDtypeStruct(scan_state.shape, jnp.float32),
        ],
        in_specs=specs,
        out_specs=[pl.BlockSpec(memory_space=pltpu.VMEM), state_spec],
        scratch_shapes=[
            pltpu.VMEM((SEQS, D), jnp.bfloat16),
            pltpu.VMEM((SEQS, CHANNELS), jnp.bfloat16),
            pltpu.VMEM((SEQS, CHANNELS), jnp.float32),
            pltpu.VMEM((blocks, CHANNELS, BLOCK), jnp.float32),
            pltpu.VMEM((blocks, CHANNELS, BLOCK), jnp.float32),
            pltpu.VMEM((SEQS, STATE), jnp.float32),
            pltpu.VMEM((SEQS, STATE), jnp.float32),
            pltpu.VMEM((blocks, CHANNELS, BLOCK), jnp.float32),
            pltpu.VMEM((D, STATE), jnp.bfloat16),
            pltpu.VMEM((CHANNELS, D), jnp.bfloat16),
            pltpu.SemaphoreType.DMA((2,)),
        ],
        compiler_params=pltpu.CompilerParams(vmem_limit_bytes=24 << 20),
        name="mixer",
    )(*operands)
    tiles = lax.all_to_all(partial_out, TP_AXES, 0, 0, tiled=True)
    return (mixed_copies(first, tiles), state_out)


def per_device(
    residual,
    first_gain,
    first_gate,
    first_lift,
    first_down,
    mixer_gain,
    proj_gate,
    proj_input,
    proj_write,
    proj_read,
    proj_step,
    step_bias,
    rate_log,
    skip_gain,
    taps_input,
    taps_write,
    taps_read,
    buffer_input,
    buffer_write,
    buffer_read,
    scan_state,
    group_gain,
    proj_output,
    second_gain,
    second_gate,
    second_lift,
    second_down,
):
    place = jnp.stack([lax.axis_index(BLOCK_AXES), lax.axis_index(ROW_AXES)]).astype(jnp.int32)
    share_one, share_two, pieces = weight_shares(
        place,
        residual,
        (first_gain, first_gate, first_lift, first_down),
        (second_gain, second_gate, second_lift, second_down),
    )
    weights_one = lax.all_gather(share_one, TP_AXES)

    mine = lax.all_to_all(pieces, TP_AXES, 0, 0, tiled=True)
    share_two, mine = lax.optimization_barrier((share_two, mine))
    weights_two = lax.all_gather(share_two, ("y_lo", *TP_AXES))
    tiles = sent_to_all(mine, BLOCK_AXES).reshape(Z * Y, TP, ROWS, FEATS)
    share, own = first_partial(place, tiles, weights_one)
    share = lax.all_to_all(share, BLOCK_AXES, 0, 0, tiled=True)
    first, copies = settled(own, share)

    mixed, state_out = state_mixer(
        first,
        lax.all_to_all(copies, TP_AXES, 0, 0, tiled=True),
        (
            mixer_gain,
            proj_gate,
            proj_input,
            proj_write,
            proj_read,
            proj_step.T,
            step_bias,
            rate_log,
            skip_gain,
            taps_input,
            taps_write,
            taps_read,
        ),
        (buffer_input, buffer_write, buffer_read),
        scan_state,
        group_gain,
        proj_output,
    )

    rows = lax.all_to_all(mixed, ROW_AXES, 0, 0, tiled=True)
    share = second_partial(place, rows, weights_two)
    share = lax.all_to_all(share.reshape(-1, ROWS, FEATS), (*ROW_AXES, *TP_AXES), 0, 0, tiled=True)
    residual_out = last_sum(share.reshape(ROW_BLOCKS, TP, ROWS, FEATS))
    return (residual_out, state_out)


def solution(mesh):
    mesh = Mesh(mesh.devices.reshape(Z, Y // PAIR, PAIR, TP // 2, 2), (*KV_AXES, *TP_AXES))
    placed = (
        P(KV_AXES, TP_AXES),
        P(TP_AXES),
        P(TP_AXES, KV_AXES),
        P(TP_AXES, KV_AXES),
        P(KV_AXES, TP_AXES),
        P(),
        P(None, TP_AXES),
        P(None, TP_AXES),
        P(None, TP_AXES),
        P(None, TP_AXES),
        P(None, TP_AXES),
        P(TP_AXES),
        P(TP_AXES),
        P(TP_AXES),
        P(None, TP_AXES),
        P(None, TP_AXES),
        P(None, TP_AXES),
        P(KV_AXES, None, TP_AXES),
        P(KV_AXES, None, TP_AXES),
        P(KV_AXES, None, TP_AXES),
        P(KV_AXES, TP_AXES, None, None),
        P(TP_AXES),
        P(TP_AXES, None),
        P(TP_AXES),
        P(TP_AXES, KV_AXES),
        P(TP_AXES, KV_AXES),
        P(KV_AXES, TP_AXES),
    )
    return jax.shard_map(
        per_device,
        mesh=mesh,
        in_specs=placed,
        out_specs=(P(KV_AXES, TP_AXES), P(KV_AXES, TP_AXES, None, None)),
        check_vma=False,
    )
```

```python
import jax
import jax.numpy as jnp
from jax import lax
from jax.experimental import pallas as pl
from jax.experimental.pallas import tpu as pltpu
from jax.sharding import Mesh
from jax.sharding import PartitionSpec as P

D = 2048
HEAD_DIM = 64
STATE = 128
FEATS = 256
HIDDEN = 176
ROWS = 4
Z, Y, TP = 8, 4, 8

KV_AXES = ("z", "y")
TP_AXES = ("x", "core")
BLOCK_AXES = ("y", "z")

norm_eps = 1e-06

by_rows = (((1,), (1,)), ((), ()))


def sent_to_all(array, axis):
    length = lax.axis_size(axis)
    return lax.all_to_all(
        jnp.broadcast_to(array[None], (length, *array.shape)), axis, 0, 0, tiled=True
    )


def inverse_rms(values):
    return lax.rsqrt(jnp.mean(values * values, axis=-1, keepdims=True) + norm_eps)


def in_hbm(array):
    return pltpu.with_memory_space_constraint(array, pltpu.HBM)


def in_vmem(array):
    return pltpu.with_memory_space_constraint(array, pltpu.VMEM)


def share_kernel(place_ref, rows_ref, *refs):
    copies_ref = refs[-1]
    pieces = rows_ref[...].astype(jnp.float32).reshape(TP, ROWS, FEATS).astype(jnp.bfloat16)
    for n in range(Z * Y):
        copies_ref[n] = pieces
    for gain, gate, lift, down, out in (refs[0:4] + refs[8:9], refs[4:8] + refs[9:10]):
        gain_f = gain[...].astype(jnp.float32).reshape(1, FEATS)
        out[:HIDDEN] = (gate[...].astype(jnp.float32) * gain_f).astype(jnp.bfloat16)
        out[HIDDEN : 2 * HIDDEN] = (lift[...].astype(jnp.float32) * gain_f).astype(jnp.bfloat16)
        out[2 * HIDDEN :] = down[...]


def weight_shares(place, residual, *sets):
    operands = [residual]
    for gain, gate_weight, lift_weight, down_weight in sets:
        operands += [gain, gate_weight.T, lift_weight.T, down_weight]
    vmem = pl.BlockSpec(memory_space=pltpu.VMEM)
    share = jax.ShapeDtypeStruct((3 * HIDDEN, FEATS), jnp.bfloat16)
    return pl.pallas_call(
        share_kernel,
        out_shape=[share, share, pltpu.VMEM((Z * Y, TP, ROWS, FEATS), jnp.bfloat16)],
        compiler_params=pltpu.CompilerParams(vmem_limit_bytes=4 << 20),
        in_specs=[pl.BlockSpec(memory_space=pltpu.SMEM)] + [vmem for _ in operands],
        out_specs=[vmem] * 3,
        name="shares",
    )(place, *[in_hbm(operand) for operand in operands])


def first_kernel(
    place_ref, rows_ref, weights_hbm, out_ref, own_ref, normed_ref, weights_ref, arrived
):
    blocks = Z * Y
    count = blocks * ROWS
    copies = [
        pltpu.make_async_copy(weights_hbm.at[u], weights_ref.at[u], arrived.at[u])
        for u in range(TP)
    ]
    for copy in copies:
        copy.start()
    total = jnp.zeros((blocks, ROWS, 1), jnp.float32)
    for u in range(TP):
        values = rows_ref[:, u].astype(jnp.float32)
        total += jnp.sum(values * values, axis=-1, keepdims=True)
    factor = lax.rsqrt(total * (1.0 / D) + norm_eps)
    for u in range(TP):
        values = rows_ref[:, u].astype(jnp.float32) * factor
        normed_ref[u] = values.reshape(count, FEATS).astype(jnp.bfloat16)
    own_ref[...] = rows_ref[place_ref[0]]
    gate = jnp.zeros((count, HIDDEN), jnp.float32)
    lift = jnp.zeros((count, HIDDEN), jnp.float32)
    for u in range(TP):
        copies[u].wait()
        block = normed_ref[u]
        gate += lax.dot_general(
            block, weights_ref[u, :HIDDEN], by_rows, preferred_element_type=jnp.float32
        )
        lift += lax.dot_general(
            block, weights_ref[u, HIDDEN : 2 * HIDDEN], by_rows, preferred_element_type=jnp.float32
        )
    hidden = (gate * jax.nn.sigmoid(gate) * lift).astype(jnp.bfloat16)
    for u in range(TP):
        down = jnp.dot(hidden, weights_ref[u, 2 * HIDDEN :], preferred_element_type=jnp.float32)
        out_ref[:, u] = down.reshape(blocks, ROWS, FEATS).astype(jnp.bfloat16)


def first_partial(place, rows, weights):
    vmem = pl.BlockSpec(memory_space=pltpu.VMEM)
    return pl.pallas_call(
        first_kernel,
        out_shape=[
            pltpu.VMEM(rows.shape, jnp.bfloat16),
            pltpu.VMEM(rows.shape[1:], jnp.bfloat16),
        ],
        in_specs=[
            pl.BlockSpec(memory_space=pltpu.SMEM),
            vmem,
            pl.BlockSpec(memory_space=pltpu.HBM),
        ],
        out_specs=[vmem, vmem],
        scratch_shapes=[
            pltpu.VMEM((TP, Z * Y * ROWS, FEATS), jnp.bfloat16),
            pltpu.VMEM(weights.shape, jnp.bfloat16),
            pltpu.SemaphoreType.DMA((TP,)),
        ],
        compiler_params=pltpu.CompilerParams(vmem_limit_bytes=24 << 20),
        name="first_ffn",
    )(place, in_vmem(rows), in_hbm(weights))


def settle_kernel(rows_ref, share_ref, first_ref, copies_ref):
    for u in range(TP):
        branch = jnp.sum(share_ref[:, u].astype(jnp.float32), axis=0)
        own = rows_ref[u].astype(jnp.float32)
        first = (own + 0.5 * branch).astype(jnp.bfloat16)
        first_ref[u] = first
        for t in range(TP):
            copies_ref[t, u] = first


def settled(rows, share):
    shape = (TP, ROWS, FEATS)
    vmem = pl.BlockSpec(memory_space=pltpu.VMEM)
    return pl.pallas_call(
        settle_kernel,
        out_shape=[pltpu.VMEM(shape, jnp.bfloat16), pltpu.VMEM((TP, *shape), jnp.bfloat16)],
        in_specs=[vmem, vmem],
        out_specs=[vmem, vmem],
        compiler_params=pltpu.CompilerParams(vmem_limit_bytes=24 << 20),
        name="settle",
    )(in_vmem(rows), in_vmem(share))


def mix_kernel(first_ref, tiles_ref, copies_ref):
    mixed = jnp.sum(tiles_ref[...].astype(jnp.float32), axis=0)
    for u in range(TP):
        cols = slice(u * FEATS, (u + 1) * FEATS)
        rows = (first_ref[u].astype(jnp.float32) + mixed[:, cols]).astype(jnp.bfloat16)
        for z in range(Z):
            copies_ref[z, :, cols] = rows


def mixed_copies(first, tiles):
    vmem = pl.BlockSpec(memory_space=pltpu.VMEM)
    return pl.pallas_call(
        mix_kernel,
        out_shape=pltpu.VMEM((Z, ROWS, D), jnp.bfloat16),
        in_specs=[vmem, vmem],
        out_specs=vmem,
        compiler_params=pltpu.CompilerParams(vmem_limit_bytes=8 << 20),
        name="mix",
    )(in_vmem(first), in_vmem(tiles))


def second_kernel(
    place_ref, rows_ref, weights_hbm, out_ref, normed_ref, weights_ref, arrived
):
    rows = Z * ROWS
    copies = [
        pltpu.make_async_copy(
            weights_hbm.at[pl.ds(n * 4, 4)], weights_ref.at[pl.ds(n * 4, 4)], arrived.at[n]
        )
        for n in range(Y * TP // 4)
    ]
    for copy in copies:
        copy.start()
    values = rows_ref[...].astype(jnp.float32).reshape(rows, D)
    factor = lax.rsqrt(jnp.sum(values * values, axis=-1, keepdims=True) * (1.0 / D) + norm_eps)
    row = lax.broadcasted_iota(jnp.int32, (rows, 1), 0)
    own = jnp.where(row // ROWS == place_ref[1], 2.0, 0.0)
    for u in range(TP):
        normed_ref[u] = (values[:, u * FEATS : (u + 1) * FEATS] * factor).astype(jnp.bfloat16)
    hidden = []
    for y in range(Y):
        both = jnp.zeros((rows, 2 * HIDDEN), jnp.float32)
        for n in range(TP // 4):
            copies[y * TP // 4 + n].wait()
        for u in range(TP):
            both += lax.dot_general(
                normed_ref[u],
                weights_ref[y * TP + u, : 2 * HIDDEN],
                by_rows,
                preferred_element_type=jnp.float32,
            )
        gate, lift = both[:, :HIDDEN], both[:, HIDDEN:]
        hidden.append((gate * jax.nn.sigmoid(gate) * lift).astype(jnp.bfloat16))
    for u in range(TP):
        down = values[:, u * FEATS : (u + 1) * FEATS] * own
        for y in range(Y):
            down += jnp.dot(
                hidden[y],
                weights_ref[y * TP + u, 2 * HIDDEN :],
                preferred_element_type=jnp.float32,
            )
        out_ref[:, u] = down.reshape(Z, ROWS, FEATS).astype(jnp.bfloat16)


def second_partial(place, rows, weights):
    vmem = pl.BlockSpec(memory_space=pltpu.VMEM)
    return pl.pallas_call(
        second_kernel,
        out_shape=pltpu.VMEM((Z, TP, ROWS, FEATS), jnp.bfloat16),
        in_specs=[
            pl.BlockSpec(memory_space=pltpu.SMEM),
            vmem,
            pl.BlockSpec(memory_space=pltpu.HBM),
        ],
        out_specs=vmem,
        scratch_shapes=[
            pltpu.VMEM((TP, Z * ROWS, FEATS), jnp.bfloat16),
            pltpu.VMEM(weights.shape, jnp.bfloat16),
            pltpu.SemaphoreType.DMA((Y * TP // 4,)),
        ],
        compiler_params=pltpu.CompilerParams(vmem_limit_bytes=24 << 20),
        name="second_ffn",
    )(place, in_vmem(rows), in_hbm(weights))


def last_kernel(share_ref, out_ref):
    branch = jnp.sum(share_ref[...].astype(jnp.float32), axis=0)
    out_ref[...] = (0.5 * branch).reshape(TP * ROWS, FEATS).astype(jnp.bfloat16)


def last_sum(share):
    return pl.pallas_call(
        last_kernel,
        out_shape=jax.ShapeDtypeStruct((TP * ROWS, FEATS), jnp.bfloat16),
        in_specs=[pl.BlockSpec(memory_space=pltpu.VMEM)],
        compiler_params=pltpu.CompilerParams(vmem_limit_bytes=8 << 20),
        name="last",
    )(in_vmem(share))


def conv_silu(newest, buffer_ref, taps_ref):
    taps = taps_ref[...].astype(jnp.float32)
    summed = newest.astype(jnp.float32) * taps[3:4]
    for k in range(3):
        summed += buffer_ref[k].astype(jnp.float32) * taps[k : k + 1]
    return summed * jax.nn.sigmoid(summed)


SEQS = TP * ROWS
BLOCK = 8
CHANNELS = 256
PER_DEVICE = 4


def mixer_kernel(
    rows_ref,
    gain_ref,
    gate_ref,
    input_ref,
    write_ref,
    read_hbm,
    step_ref,
    bias_ref,
    rate_ref,
    skip_ref,
    taps_input_ref,
    taps_write_ref,
    taps_read_ref,
    buffer_input_ref,
    buffer_write_ref,
    buffer_read_ref,
    state_ref,
    group_ref,
    output_hbm,
    mixed_ref,
    new_state_ref,
    normed_ref,
    gate_z_ref,
    xc_ref,
    added_ref,
    retain_ref,
    bc_ref,
    rc_ref,
    out_cols_ref,
    read_ref,
    output_ref,
    arrived,
):
    i = pl.program_id(0)
    read_copy = pltpu.make_async_copy(read_hbm, read_ref, arrived.at[0])
    output_copy = pltpu.make_async_copy(output_hbm, output_ref, arrived.at[1])

    @pl.when(i == 0)
    def _():
        read_copy.start()
        output_copy.start()
        total = jnp.zeros((TP, ROWS, 1), jnp.float32)
        for u in range(TP):
            values = rows_ref[:, u].astype(jnp.float32)
            total += jnp.sum(values * values, axis=-1, keepdims=True)
        factor = lax.rsqrt(total * (1.0 / D) + norm_eps)
        for u in range(TP):
            values = (rows_ref[:, u].astype(jnp.float32) * factor).reshape(SEQS, FEATS)
            cols = slice(u * FEATS, (u + 1) * FEATS)
            gain = gain_ref[cols].astype(jnp.float32).reshape(1, FEATS)
            normed_ref[:, cols] = (values * gain).astype(jnp.bfloat16)
        normed = normed_ref[...]

        def project(weight_ref):
            return jnp.dot(normed, weight_ref[...], preferred_element_type=jnp.float32).astype(
                jnp.bfloat16
            )

        gate_z_ref[...] = project(gate_ref)
        step_raw = lax.dot_general(
            normed, step_ref[...], by_rows, preferred_element_type=jnp.float32
        ).astype(jnp.bfloat16)
        xc = conv_silu(project(input_ref), buffer_input_ref, taps_input_ref)
        bc_ref[...] = conv_silu(project(write_ref), buffer_write_ref, taps_write_ref)
        read_copy.wait()
        rc_ref[...] = conv_silu(project(read_ref), buffer_read_ref, taps_read_ref)
        xc_ref[...] = xc
        step = jax.nn.softplus(step_raw.astype(jnp.float32) + bias_ref[...].reshape(1, PER_DEVICE))
        retain = jnp.exp(-step * jnp.exp(rate_ref[...].reshape(1, PER_DEVICE)))
        head = lax.broadcasted_iota(jnp.int32, (SEQS, CHANNELS), 1) // HEAD_DIM
        step_wide = jnp.zeros((SEQS, CHANNELS), jnp.float32)
        retain_wide = jnp.zeros((SEQS, CHANNELS), jnp.float32)
        for h in range(PER_DEVICE):
            step_wide = jnp.where(head == h, step[:, h : h + 1], step_wide)
            retain_wide = jnp.where(head == h, retain[:, h : h + 1], retain_wide)
        added = (step_wide * xc).T
        retain_cols = retain_wide.T
        for s in range(SEQS // BLOCK):
            added_ref[s] = added[:, s * BLOCK : (s + 1) * BLOCK]
            retain_ref[s] = retain_cols[:, s * BLOCK : (s + 1) * BLOCK]

    added = added_ref[i]
    retain = retain_ref[i]
    writes = bc_ref[pl.ds(pl.multiple_of(i * BLOCK, BLOCK), BLOCK)]
    reads = rc_ref[pl.ds(pl.multiple_of(i * BLOCK, BLOCK), BLOCK)].astype(jnp.bfloat16)
    column = lax.broadcasted_iota(jnp.int32, (CHANNELS, BLOCK), 1)
    cols = jnp.zeros((CHANNELS, BLOCK), jnp.float32)
    for b in range(BLOCK):
        new = []
        for h in range(PER_DEVICE):
            top = h * HEAD_DIM
            kept = jnp.broadcast_to(retain[top : top + 8, b : b + 1], (8, STATE))
            old = state_ref[i * BLOCK + b, h].reshape(HEAD_DIM // 8, 8, STATE) * kept[None]
            new.append(
                old.reshape(HEAD_DIM, STATE)
                + added[top : top + HEAD_DIM, b : b + 1] * writes[b : b + 1]
            )
            new_state_ref[b, h] = new[h]
        new = jnp.concatenate(new, axis=0).astype(jnp.bfloat16)
        read = lax.dot_general(new, reads, by_rows, preferred_element_type=jnp.float32)
        cols = jnp.where(column == b, read, cols)
    out_cols_ref[i] = cols

    @pl.when(i == pl.num_programs(0) - 1)
    def _():
        cols = jnp.concatenate([out_cols_ref[s] for s in range(SEQS // BLOCK)], axis=1)
        head = lax.broadcasted_iota(jnp.int32, (1, CHANNELS), 1) // HEAD_DIM
        skip_own = skip_ref[...].reshape(1, PER_DEVICE)
        skip = jnp.zeros((1, CHANNELS), jnp.float32)
        for h in range(PER_DEVICE):
            skip = jnp.where(head == h, skip_own[:, h : h + 1], skip)
        head_out = (cols.T + skip * xc_ref[...]).astype(jnp.bfloat16).astype(jnp.float32)
        gate_z = gate_z_ref[...].astype(jnp.float32)
        gated = head_out * (gate_z * jax.nn.sigmoid(gate_z))
        gated = gated * inverse_rms(gated) * group_ref[...].astype(jnp.float32).reshape(1, CHANNELS)
        output_copy.wait()
        part = jnp.dot(
            gated.astype(jnp.bfloat16), output_ref[...], preferred_element_type=jnp.float32
        )
        mixed_ref[...] = part.reshape(TP, ROWS, D).astype(jnp.bfloat16)


def state_mixer(first, rows, small, buffers, scan_state, group_gain, proj_output):
    operands = [rows, *small, *[b.transpose(1, 0, 2) for b in buffers]]
    operands += [scan_state, group_gain, proj_output]
    from_hbm = (5, len(operands) - 1)
    operands = [in_hbm(o) if n in from_hbm else in_vmem(o) for n, o in enumerate(operands)]
    specs = [pl.BlockSpec(memory_space=pltpu.VMEM) for _ in operands]
    for n in from_hbm:
        specs[n] = pl.BlockSpec(memory_space=pltpu.HBM)
    state_spec = pl.BlockSpec((BLOCK, PER_DEVICE, HEAD_DIM, STATE), lambda i: (i, 0, 0, 0))
    blocks = SEQS // BLOCK
    partial_out, state_out = pl.pallas_call(
        mixer_kernel,
        grid=(blocks,),
        out_shape=[
            pltpu.VMEM((TP, ROWS, D), jnp.bfloat16),
            jax.ShapeDtypeStruct(scan_state.shape, jnp.float32),
        ],
        in_specs=specs,
        out_specs=[pl.BlockSpec(memory_space=pltpu.VMEM), state_spec],
        scratch_shapes=[
            pltpu.VMEM((SEQS, D), jnp.bfloat16),
            pltpu.VMEM((SEQS, CHANNELS), jnp.bfloat16),
            pltpu.VMEM((SEQS, CHANNELS), jnp.float32),
            pltpu.VMEM((blocks, CHANNELS, BLOCK), jnp.float32),
            pltpu.VMEM((blocks, CHANNELS, BLOCK), jnp.float32),
            pltpu.VMEM((SEQS, STATE), jnp.float32),
            pltpu.VMEM((SEQS, STATE), jnp.float32),
            pltpu.VMEM((blocks, CHANNELS, BLOCK), jnp.float32),
            pltpu.VMEM((D, STATE), jnp.bfloat16),
            pltpu.VMEM((CHANNELS, D), jnp.bfloat16),
            pltpu.SemaphoreType.DMA((2,)),
        ],
        compiler_params=pltpu.CompilerParams(vmem_limit_bytes=24 << 20),
        name="mixer",
    )(*operands)
    tiles = lax.all_to_all(partial_out, TP_AXES, 0, 0, tiled=True)
    return (mixed_copies(first, tiles), state_out)


def per_device(
    residual,
    first_gain,
    first_gate,
    first_lift,
    first_down,
    mixer_gain,
    proj_gate,
    proj_input,
    proj_write,
    proj_read,
    proj_step,
    step_bias,
    rate_log,
    skip_gain,
    taps_input,
    taps_write,
    taps_read,
    buffer_input,
    buffer_write,
    buffer_read,
    scan_state,
    group_gain,
    proj_output,
    second_gain,
    second_gate,
    second_lift,
    second_down,
):
    place = jnp.stack([lax.axis_index(BLOCK_AXES), lax.axis_index("z")]).astype(jnp.int32)
    share_one, share_two, pieces = weight_shares(
        place,
        residual,
        (first_gain, first_gate, first_lift, first_down),
        (second_gain, second_gate, second_lift, second_down),
    )
    weights_one = lax.all_gather(share_one, TP_AXES)
    weights_two = lax.all_gather(share_two, ("y", *TP_AXES))

    tiles = lax.all_to_all(
        pieces.reshape(-1, ROWS, FEATS), (*BLOCK_AXES, *TP_AXES), 0, 0, tiled=True
    ).reshape(Z * Y, TP, ROWS, FEATS)
    share, own = first_partial(place, tiles, weights_one)
    share = lax.all_to_all(share, BLOCK_AXES, 0, 0, tiled=True)
    first, copies = settled(own, share)

    mixed, state_out = state_mixer(
        first,
        lax.all_to_all(copies, TP_AXES, 0, 0, tiled=True),
        (
            mixer_gain,
            proj_gate,
            proj_input,
            proj_write,
            proj_read,
            proj_step.T,
            step_bias,
            rate_log,
            skip_gain,
            taps_input,
            taps_write,
            taps_read,
        ),
        (buffer_input, buffer_write, buffer_read),
        scan_state,
        group_gain,
        proj_output,
    )

    rows = lax.all_to_all(mixed, "z", 0, 0, tiled=True)
    share = second_partial(place, rows, weights_two)
    share = lax.all_to_all(share.reshape(-1, ROWS, FEATS), ("z", *TP_AXES), 0, 0, tiled=True)
    residual_out = last_sum(share.reshape(Z, TP, ROWS, FEATS))
    return (residual_out, state_out)


def solution(mesh):
    mesh = Mesh(mesh.devices.reshape(Z, Y, TP // 2, 2), (*KV_AXES, *TP_AXES))
    placed = (
        P(KV_AXES, TP_AXES),
        P(TP_AXES),
        P(TP_AXES, KV_AXES),
        P(TP_AXES, KV_AXES),
        P(KV_AXES, TP_AXES),
        P(),
        P(None, TP_AXES),
        P(None, TP_AXES),
        P(None, TP_AXES),
        P(None, TP_AXES),
        P(None, TP_AXES),
        P(TP_AXES),
        P(TP_AXES),
        P(TP_AXES),
        P(None, TP_AXES),
        P(None, TP_AXES),
        P(None, TP_AXES),
        P(KV_AXES, None, TP_AXES),
        P(KV_AXES, None, TP_AXES),
        P(KV_AXES, None, TP_AXES),
        P(KV_AXES, TP_AXES, None, None),
        P(TP_AXES),
        P(TP_AXES, None),
        P(TP_AXES),
        P(TP_AXES, KV_AXES),
        P(TP_AXES, KV_AXES),
        P(KV_AXES, TP_AXES),
    )
    return jax.shard_map(
        per_device,
        mesh=mesh,
        in_specs=placed,
        out_specs=(P(KV_AXES, TP_AXES), P(KV_AXES, TP_AXES, None, None)),
        check_vma=False,
    )
```

```python
import jax
import jax.numpy as jnp
from jax import lax
from jax.experimental import pallas as pl
from jax.experimental.pallas import tpu as pltpu
from jax.sharding import Mesh
from jax.sharding import PartitionSpec as P

D = 2048
HEAD_DIM = 64
STATE = 128
FEATS = 256
HIDDEN = 176
ROWS = 4
Z, Y, TP = 8, 4, 8

KV_AXES = ("z", "y")
TP_AXES = ("x", "core")
BLOCK_AXES = ("y", "z")

norm_eps = 1e-06

by_rows = (((1,), (1,)), ((), ()))


def sent_to_all(array, axis):
    length = lax.axis_size(axis)
    return lax.all_to_all(
        jnp.broadcast_to(array[None], (length, *array.shape)), axis, 0, 0, tiled=True
    )


def inverse_rms(values):
    return lax.rsqrt(jnp.mean(values * values, axis=-1, keepdims=True) + norm_eps)


def in_hbm(array):
    return pltpu.with_memory_space_constraint(array, pltpu.HBM)


def in_vmem(array):
    return pltpu.with_memory_space_constraint(array, pltpu.VMEM)


def share_kernel(place_ref, rows_ref, *refs):
    pieces_ref = refs[-1]
    pieces_ref[...] = rows_ref[...].astype(jnp.float32).reshape(TP, ROWS, FEATS).astype(
        jnp.bfloat16
    )
    for gain, gate, lift, down, out in (refs[0:4] + refs[8:9], refs[4:8] + refs[9:10]):
        gain_f = gain[...].astype(jnp.float32).reshape(1, FEATS)
        out[:HIDDEN] = (gate[...].astype(jnp.float32) * gain_f).astype(jnp.bfloat16)
        out[HIDDEN : 2 * HIDDEN] = (lift[...].astype(jnp.float32) * gain_f).astype(jnp.bfloat16)
        out[2 * HIDDEN :] = down[...]


def weight_shares(place, residual, *sets):
    operands = [residual]
    for gain, gate_weight, lift_weight, down_weight in sets:
        operands += [gain, gate_weight.T, lift_weight.T, down_weight]
    vmem = pl.BlockSpec(memory_space=pltpu.VMEM)
    share = jax.ShapeDtypeStruct((3 * HIDDEN, FEATS), jnp.bfloat16)
    return pl.pallas_call(
        share_kernel,
        out_shape=[share, share, pltpu.VMEM((TP, ROWS, FEATS), jnp.bfloat16)],
        compiler_params=pltpu.CompilerParams(vmem_limit_bytes=4 << 20),
        in_specs=[pl.BlockSpec(memory_space=pltpu.SMEM)] + [vmem for _ in operands],
        out_specs=[vmem] * 3,
        name="shares",
    )(place, *[in_hbm(operand) for operand in operands])


def first_kernel(
    place_ref, rows_ref, weights_hbm, out_ref, own_ref, normed_ref, weights_ref, arrived
):
    blocks = Z * Y
    count = blocks * ROWS
    copies = [
        pltpu.make_async_copy(weights_hbm.at[u], weights_ref.at[u], arrived.at[u])
        for u in range(TP)
    ]
    for copy in copies:
        copy.start()
    total = jnp.zeros((blocks, ROWS, 1), jnp.float32)
    for u in range(TP):
        values = rows_ref[:, u].astype(jnp.float32)
        total += jnp.sum(values * values, axis=-1, keepdims=True)
    factor = lax.rsqrt(total * (1.0 / D) + norm_eps)
    for u in range(TP):
        values = rows_ref[:, u].astype(jnp.float32) * factor
        normed_ref[u] = values.reshape(count, FEATS).astype(jnp.bfloat16)
    own_ref[...] = rows_ref[place_ref[0]]
    gate = jnp.zeros((count, HIDDEN), jnp.float32)
    lift = jnp.zeros((count, HIDDEN), jnp.float32)
    for u in range(TP):
        copies[u].wait()
        block = normed_ref[u]
        gate += lax.dot_general(
            block, weights_ref[u, :HIDDEN], by_rows, preferred_element_type=jnp.float32
        )
        lift += lax.dot_general(
            block, weights_ref[u, HIDDEN : 2 * HIDDEN], by_rows, preferred_element_type=jnp.float32
        )
    hidden = (gate * jax.nn.sigmoid(gate) * lift).astype(jnp.bfloat16)
    for u in range(TP):
        down = jnp.dot(hidden, weights_ref[u, 2 * HIDDEN :], preferred_element_type=jnp.float32)
        out_ref[:, u] = down.reshape(blocks, ROWS, FEATS).astype(jnp.bfloat16)


def first_partial(place, rows, weights):
    vmem = pl.BlockSpec(memory_space=pltpu.VMEM)
    return pl.pallas_call(
        first_kernel,
        out_shape=[
            pltpu.VMEM(rows.shape, jnp.bfloat16),
            pltpu.VMEM(rows.shape[1:], jnp.bfloat16),
        ],
        in_specs=[
            pl.BlockSpec(memory_space=pltpu.SMEM),
            vmem,
            pl.BlockSpec(memory_space=pltpu.HBM),
        ],
        out_specs=[vmem, vmem],
        scratch_shapes=[
            pltpu.VMEM((TP, Z * Y * ROWS, FEATS), jnp.bfloat16),
            pltpu.VMEM(weights.shape, jnp.bfloat16),
            pltpu.SemaphoreType.DMA((TP,)),
        ],
        compiler_params=pltpu.CompilerParams(vmem_limit_bytes=24 << 20),
        name="first_ffn",
    )(place, in_vmem(rows), in_hbm(weights))


def settle_kernel(rows_ref, share_ref, first_ref, copies_ref):
    for u in range(TP):
        branch = jnp.sum(share_ref[:, u].astype(jnp.float32), axis=0)
        own = rows_ref[u].astype(jnp.float32)
        first = (own + 0.5 * branch).astype(jnp.bfloat16)
        first_ref[u] = first
        for t in range(TP):
            copies_ref[t, u] = first


def settled(rows, share):
    shape = (TP, ROWS, FEATS)
    vmem = pl.BlockSpec(memory_space=pltpu.VMEM)
    return pl.pallas_call(
        settle_kernel,
        out_shape=[pltpu.VMEM(shape, jnp.bfloat16), pltpu.VMEM((TP, *shape), jnp.bfloat16)],
        in_specs=[vmem, vmem],
        out_specs=[vmem, vmem],
        compiler_params=pltpu.CompilerParams(vmem_limit_bytes=24 << 20),
        name="settle",
    )(in_vmem(rows), in_vmem(share))


def mix_kernel(first_ref, tiles_ref, copies_ref):
    mixed = jnp.sum(tiles_ref[...].astype(jnp.float32), axis=0)
    for u in range(TP):
        cols = slice(u * FEATS, (u + 1) * FEATS)
        rows = (first_ref[u].astype(jnp.float32) + mixed[:, cols]).astype(jnp.bfloat16)
        for z in range(Z):
            copies_ref[z, :, cols] = rows


def mixed_copies(first, tiles):
    vmem = pl.BlockSpec(memory_space=pltpu.VMEM)
    return pl.pallas_call(
        mix_kernel,
        out_shape=pltpu.VMEM((Z, ROWS, D), jnp.bfloat16),
        in_specs=[vmem, vmem],
        out_specs=vmem,
        compiler_params=pltpu.CompilerParams(vmem_limit_bytes=8 << 20),
        name="mix",
    )(in_vmem(first), in_vmem(tiles))


def second_kernel(
    place_ref, rows_ref, weights_hbm, out_ref, normed_ref, weights_ref, arrived
):
    rows = Z * ROWS
    copies = [
        pltpu.make_async_copy(
            weights_hbm.at[pl.ds(n * 4, 4)], weights_ref.at[pl.ds(n * 4, 4)], arrived.at[n]
        )
        for n in range(Y * TP // 4)
    ]
    for copy in copies:
        copy.start()
    values = rows_ref[...].astype(jnp.float32).reshape(rows, D)
    factor = lax.rsqrt(jnp.sum(values * values, axis=-1, keepdims=True) * (1.0 / D) + norm_eps)
    row = lax.broadcasted_iota(jnp.int32, (rows, 1), 0)
    own = jnp.where(row // ROWS == place_ref[1], 2.0, 0.0)
    for u in range(TP):
        normed_ref[u] = (values[:, u * FEATS : (u + 1) * FEATS] * factor).astype(jnp.bfloat16)
    hidden = []
    for y in range(Y):
        both = jnp.zeros((rows, 2 * HIDDEN), jnp.float32)
        for n in range(TP // 4):
            copies[y * TP // 4 + n].wait()
        for u in range(TP):
            both += lax.dot_general(
                normed_ref[u],
                weights_ref[y * TP + u, : 2 * HIDDEN],
                by_rows,
                preferred_element_type=jnp.float32,
            )
        gate, lift = both[:, :HIDDEN], both[:, HIDDEN:]
        hidden.append((gate * jax.nn.sigmoid(gate) * lift).astype(jnp.bfloat16))
    for u in range(TP):
        down = values[:, u * FEATS : (u + 1) * FEATS] * own
        for y in range(Y):
            down += jnp.dot(
                hidden[y],
                weights_ref[y * TP + u, 2 * HIDDEN :],
                preferred_element_type=jnp.float32,
            )
        out_ref[:, u] = down.reshape(Z, ROWS, FEATS).astype(jnp.bfloat16)


def second_partial(place, rows, weights):
    vmem = pl.BlockSpec(memory_space=pltpu.VMEM)
    return pl.pallas_call(
        second_kernel,
        out_shape=pltpu.VMEM((Z, TP, ROWS, FEATS), jnp.bfloat16),
        in_specs=[
            pl.BlockSpec(memory_space=pltpu.SMEM),
            vmem,
            pl.BlockSpec(memory_space=pltpu.HBM),
        ],
        out_specs=vmem,
        scratch_shapes=[
            pltpu.VMEM((TP, Z * ROWS, FEATS), jnp.bfloat16),
            pltpu.VMEM(weights.shape, jnp.bfloat16),
            pltpu.SemaphoreType.DMA((Y * TP // 4,)),
        ],
        compiler_params=pltpu.CompilerParams(vmem_limit_bytes=24 << 20),
        name="second_ffn",
    )(place, in_vmem(rows), in_hbm(weights))


def last_kernel(share_ref, out_ref):
    branch = jnp.sum(share_ref[...].astype(jnp.float32), axis=0)
    out_ref[...] = (0.5 * branch).reshape(TP * ROWS, FEATS).astype(jnp.bfloat16)


def last_sum(share):
    return pl.pallas_call(
        last_kernel,
        out_shape=jax.ShapeDtypeStruct((TP * ROWS, FEATS), jnp.bfloat16),
        in_specs=[pl.BlockSpec(memory_space=pltpu.VMEM)],
        compiler_params=pltpu.CompilerParams(vmem_limit_bytes=8 << 20),
        name="last",
    )(in_vmem(share))


def conv_silu(newest, buffer_ref, taps_ref):
    taps = taps_ref[...].astype(jnp.float32)
    summed = newest.astype(jnp.float32) * taps[3:4]
    for k in range(3):
        summed += buffer_ref[k].astype(jnp.float32) * taps[k : k + 1]
    return summed * jax.nn.sigmoid(summed)


SEQS = TP * ROWS
BLOCK = 8
CHANNELS = 256
PER_DEVICE = 4


def mixer_kernel(
    rows_ref,
    gain_ref,
    gate_ref,
    input_ref,
    write_ref,
    read_hbm,
    step_ref,
    bias_ref,
    rate_ref,
    skip_ref,
    taps_input_ref,
    taps_write_ref,
    taps_read_ref,
    buffer_input_ref,
    buffer_write_ref,
    buffer_read_ref,
    state_ref,
    group_ref,
    output_hbm,
    mixed_ref,
    new_state_ref,
    normed_ref,
    gate_z_ref,
    xc_ref,
    added_ref,
    retain_ref,
    bc_ref,
    rc_ref,
    out_cols_ref,
    read_ref,
    output_ref,
    arrived,
):
    i = pl.program_id(0)
    read_copy = pltpu.make_async_copy(read_hbm, read_ref, arrived.at[0])
    output_copy = pltpu.make_async_copy(output_hbm, output_ref, arrived.at[1])

    @pl.when(i == 0)
    def _():
        read_copy.start()
        output_copy.start()
        total = jnp.zeros((TP, ROWS, 1), jnp.float32)
        for u in range(TP):
            values = rows_ref[:, u].astype(jnp.float32)
            total += jnp.sum(values * values, axis=-1, keepdims=True)
        factor = lax.rsqrt(total * (1.0 / D) + norm_eps)
        for u in range(TP):
            values = (rows_ref[:, u].astype(jnp.float32) * factor).reshape(SEQS, FEATS)
            cols = slice(u * FEATS, (u + 1) * FEATS)
            gain = gain_ref[cols].astype(jnp.float32).reshape(1, FEATS)
            normed_ref[:, cols] = (values * gain).astype(jnp.bfloat16)
        normed = normed_ref[...]

        def project(weight_ref):
            return jnp.dot(normed, weight_ref[...], preferred_element_type=jnp.float32).astype(
                jnp.bfloat16
            )

        gate_z_ref[...] = project(gate_ref)
        step_raw = lax.dot_general(
            normed, step_ref[...], by_rows, preferred_element_type=jnp.float32
        ).astype(jnp.bfloat16)
        xc = conv_silu(project(input_ref), buffer_input_ref, taps_input_ref)
        bc_ref[...] = conv_silu(project(write_ref), buffer_write_ref, taps_write_ref)
        read_copy.wait()
        rc_ref[...] = conv_silu(project(read_ref), buffer_read_ref, taps_read_ref)
        xc_ref[...] = xc
        step = jax.nn.softplus(step_raw.astype(jnp.float32) + bias_ref[...].reshape(1, PER_DEVICE))
        retain = jnp.exp(-step * jnp.exp(rate_ref[...].reshape(1, PER_DEVICE)))
        head = lax.broadcasted_iota(jnp.int32, (SEQS, CHANNELS), 1) // HEAD_DIM
        step_wide = jnp.zeros((SEQS, CHANNELS), jnp.float32)
        retain_wide = jnp.zeros((SEQS, CHANNELS), jnp.float32)
        for h in range(PER_DEVICE):
            step_wide = jnp.where(head == h, step[:, h : h + 1], step_wide)
            retain_wide = jnp.where(head == h, retain[:, h : h + 1], retain_wide)
        added = (step_wide * xc).T
        retain_cols = retain_wide.T
        for s in range(SEQS // BLOCK):
            added_ref[s] = added[:, s * BLOCK : (s + 1) * BLOCK]
            retain_ref[s] = retain_cols[:, s * BLOCK : (s + 1) * BLOCK]

    added = added_ref[i]
    retain = retain_ref[i]
    writes = bc_ref[pl.ds(pl.multiple_of(i * BLOCK, BLOCK), BLOCK)]
    reads = rc_ref[pl.ds(pl.multiple_of(i * BLOCK, BLOCK), BLOCK)].astype(jnp.bfloat16)
    column = lax.broadcasted_iota(jnp.int32, (CHANNELS, BLOCK), 1)
    cols = jnp.zeros((CHANNELS, BLOCK), jnp.float32)
    for b in range(BLOCK):
        new = []
        for h in range(PER_DEVICE):
            top = h * HEAD_DIM
            kept = jnp.broadcast_to(retain[top : top + 8, b : b + 1], (8, STATE))
            old = state_ref[i * BLOCK + b, h].reshape(HEAD_DIM // 8, 8, STATE) * kept[None]
            new.append(
                old.reshape(HEAD_DIM, STATE)
                + added[top : top + HEAD_DIM, b : b + 1] * writes[b : b + 1]
            )
            new_state_ref[b, h] = new[h]
        new = jnp.concatenate(new, axis=0).astype(jnp.bfloat16)
        read = lax.dot_general(new, reads, by_rows, preferred_element_type=jnp.float32)
        cols = jnp.where(column == b, read, cols)
    out_cols_ref[i] = cols

    @pl.when(i == pl.num_programs(0) - 1)
    def _():
        cols = jnp.concatenate([out_cols_ref[s] for s in range(SEQS // BLOCK)], axis=1)
        head = lax.broadcasted_iota(jnp.int32, (1, CHANNELS), 1) // HEAD_DIM
        skip_own = skip_ref[...].reshape(1, PER_DEVICE)
        skip = jnp.zeros((1, CHANNELS), jnp.float32)
        for h in range(PER_DEVICE):
            skip = jnp.where(head == h, skip_own[:, h : h + 1], skip)
        head_out = (cols.T + skip * xc_ref[...]).astype(jnp.bfloat16).astype(jnp.float32)
        gate_z = gate_z_ref[...].astype(jnp.float32)
        gated = head_out * (gate_z * jax.nn.sigmoid(gate_z))
        gated = gated * inverse_rms(gated) * group_ref[...].astype(jnp.float32).reshape(1, CHANNELS)
        output_copy.wait()
        part = jnp.dot(
            gated.astype(jnp.bfloat16), output_ref[...], preferred_element_type=jnp.float32
        )
        mixed_ref[...] = part.reshape(TP, ROWS, D).astype(jnp.bfloat16)


def state_mixer(first, rows, small, buffers, scan_state, group_gain, proj_output):
    operands = [rows, *small, *[b.transpose(1, 0, 2) for b in buffers]]
    operands += [scan_state, group_gain, proj_output]
    from_hbm = (5, len(operands) - 1)
    operands = [in_hbm(o) if n in from_hbm else in_vmem(o) for n, o in enumerate(operands)]
    specs = [pl.BlockSpec(memory_space=pltpu.VMEM) for _ in operands]
    for n in from_hbm:
        specs[n] = pl.BlockSpec(memory_space=pltpu.HBM)
    state_spec = pl.BlockSpec((BLOCK, PER_DEVICE, HEAD_DIM, STATE), lambda i: (i, 0, 0, 0))
    blocks = SEQS // BLOCK
    partial_out, state_out = pl.pallas_call(
        mixer_kernel,
        grid=(blocks,),
        out_shape=[
            pltpu.VMEM((TP, ROWS, D), jnp.bfloat16),
            jax.ShapeDtypeStruct(scan_state.shape, jnp.float32),
        ],
        in_specs=specs,
        out_specs=[pl.BlockSpec(memory_space=pltpu.VMEM), state_spec],
        scratch_shapes=[
            pltpu.VMEM((SEQS, D), jnp.bfloat16),
            pltpu.VMEM((SEQS, CHANNELS), jnp.bfloat16),
            pltpu.VMEM((SEQS, CHANNELS), jnp.float32),
            pltpu.VMEM((blocks, CHANNELS, BLOCK), jnp.float32),
            pltpu.VMEM((blocks, CHANNELS, BLOCK), jnp.float32),
            pltpu.VMEM((SEQS, STATE), jnp.float32),
            pltpu.VMEM((SEQS, STATE), jnp.float32),
            pltpu.VMEM((blocks, CHANNELS, BLOCK), jnp.float32),
            pltpu.VMEM((D, STATE), jnp.bfloat16),
            pltpu.VMEM((CHANNELS, D), jnp.bfloat16),
            pltpu.SemaphoreType.DMA((2,)),
        ],
        compiler_params=pltpu.CompilerParams(vmem_limit_bytes=24 << 20),
        name="mixer",
    )(*operands)
    tiles = lax.all_to_all(partial_out, TP_AXES, 0, 0, tiled=True)
    return (mixed_copies(first, tiles), state_out)


def per_device(
    residual,
    first_gain,
    first_gate,
    first_lift,
    first_down,
    mixer_gain,
    proj_gate,
    proj_input,
    proj_write,
    proj_read,
    proj_step,
    step_bias,
    rate_log,
    skip_gain,
    taps_input,
    taps_write,
    taps_read,
    buffer_input,
    buffer_write,
    buffer_read,
    scan_state,
    group_gain,
    proj_output,
    second_gain,
    second_gate,
    second_lift,
    second_down,
):
    place = jnp.stack([lax.axis_index(BLOCK_AXES), lax.axis_index("z")]).astype(jnp.int32)
    share_one, share_two, pieces = weight_shares(
        place,
        residual,
        (first_gain, first_gate, first_lift, first_down),
        (second_gain, second_gate, second_lift, second_down),
    )
    weights_one = lax.all_gather(share_one, TP_AXES)

    mine = lax.all_to_all(pieces, TP_AXES, 0, 0, tiled=True)
    share_two, mine = lax.optimization_barrier((share_two, mine))
    weights_two = lax.all_gather(share_two, ("y", *TP_AXES))
    tiles = sent_to_all(mine, BLOCK_AXES).reshape(Z * Y, TP, ROWS, FEATS)
    share, own = first_partial(place, tiles, weights_one)
    share = lax.all_to_all(share, BLOCK_AXES, 0, 0, tiled=True)
    first, copies = settled(own, share)

    mixed, state_out = state_mixer(
        first,
        lax.all_to_all(copies, TP_AXES, 0, 0, tiled=True),
        (
            mixer_gain,
            proj_gate,
            proj_input,
            proj_write,
            proj_read,
            proj_step.T,
            step_bias,
            rate_log,
            skip_gain,
            taps_input,
            taps_write,
            taps_read,
        ),
        (buffer_input, buffer_write, buffer_read),
        scan_state,
        group_gain,
        proj_output,
    )

    rows = lax.all_to_all(mixed, "z", 0, 0, tiled=True)
    share = second_partial(place, rows, weights_two)
    share = lax.all_to_all(share.reshape(-1, ROWS, FEATS), ("z", *TP_AXES), 0, 0, tiled=True)
    residual_out = last_sum(share.reshape(Z, TP, ROWS, FEATS))
    return (residual_out, state_out)


def solution(mesh):
    mesh = Mesh(mesh.devices.reshape(Z, Y, TP // 2, 2), (*KV_AXES, *TP_AXES))
    placed = (
        P(KV_AXES, TP_AXES),
        P(TP_AXES),
        P(TP_AXES, KV_AXES),
        P(TP_AXES, KV_AXES),
        P(KV_AXES, TP_AXES),
        P(),
        P(None, TP_AXES),
        P(None, TP_AXES),
        P(None, TP_AXES),
        P(None, TP_AXES),
        P(None, TP_AXES),
        P(TP_AXES),
        P(TP_AXES),
        P(TP_AXES),
        P(None, TP_AXES),
        P(None, TP_AXES),
        P(None, TP_AXES),
        P(KV_AXES, None, TP_AXES),
        P(KV_AXES, None, TP_AXES),
        P(KV_AXES, None, TP_AXES),
        P(KV_AXES, TP_AXES, None, None),
        P(TP_AXES),
        P(TP_AXES, None),
        P(TP_AXES),
        P(TP_AXES, KV_AXES),
        P(TP_AXES, KV_AXES),
        P(KV_AXES, TP_AXES),
    )
    return jax.shard_map(
        per_device,
        mesh=mesh,
        in_specs=placed,
        out_specs=(P(KV_AXES, TP_AXES), P(KV_AXES, TP_AXES, None, None)),
        check_vma=False,
    )
```

```python
import jax
import jax.numpy as jnp
from jax import lax
from jax.experimental import pallas as pl
from jax.experimental.pallas import tpu as pltpu
from jax.sharding import Mesh
from jax.sharding import PartitionSpec as P

D = 2048
HEAD_DIM = 64
STATE = 128
FEATS = 256
HIDDEN = 176
ROWS = 4
Z, Y, TP = 8, 4, 8

KV_AXES = ("z", "y")
TP_AXES = ("x", "core")
BLOCK_AXES = ("y", "z")

norm_eps = 1e-06

by_rows = (((1,), (1,)), ((), ()))


def sent_to_all(array, axis):
    length = lax.axis_size(axis)
    return lax.all_to_all(
        jnp.broadcast_to(array[None], (length, *array.shape)), axis, 0, 0, tiled=True
    )


def inverse_rms(values):
    return lax.rsqrt(jnp.mean(values * values, axis=-1, keepdims=True) + norm_eps)


def in_hbm(array):
    return pltpu.with_memory_space_constraint(array, pltpu.HBM)


def in_vmem(array):
    return pltpu.with_memory_space_constraint(array, pltpu.VMEM)


def share_kernel(place_ref, rows_ref, *refs):
    pieces_ref = refs[-1]
    pieces_ref[...] = rows_ref[...].astype(jnp.float32).reshape(TP, ROWS, FEATS).astype(
        jnp.bfloat16
    )
    for gain, gate, lift, down, out in (refs[0:4] + refs[8:9], refs[4:8] + refs[9:10]):
        gain_f = gain[...].astype(jnp.float32).reshape(1, FEATS)
        out[:HIDDEN] = (gate[...].astype(jnp.float32) * gain_f).astype(jnp.bfloat16)
        out[HIDDEN : 2 * HIDDEN] = (lift[...].astype(jnp.float32) * gain_f).astype(jnp.bfloat16)
        out[2 * HIDDEN :] = down[...]


def weight_shares(place, residual, *sets):
    operands = [residual]
    for gain, gate_weight, lift_weight, down_weight in sets:
        operands += [gain, gate_weight.T, lift_weight.T, down_weight]
    vmem = pl.BlockSpec(memory_space=pltpu.VMEM)
    share = jax.ShapeDtypeStruct((3 * HIDDEN, FEATS), jnp.bfloat16)
    return pl.pallas_call(
        share_kernel,
        out_shape=[share, share, pltpu.VMEM((TP, ROWS, FEATS), jnp.bfloat16)],
        compiler_params=pltpu.CompilerParams(vmem_limit_bytes=4 << 20),
        in_specs=[pl.BlockSpec(memory_space=pltpu.SMEM)] + [vmem for _ in operands],
        out_specs=[vmem] * 3,
        name="shares",
    )(place, *[in_hbm(operand) for operand in operands])


def first_kernel(
    place_ref, rows_ref, weights_hbm, out_ref, own_ref, normed_ref, weights_ref, arrived
):
    blocks = Z * Y
    count = blocks * ROWS
    copies = [
        pltpu.make_async_copy(weights_hbm.at[u], weights_ref.at[u], arrived.at[u])
        for u in range(TP)
    ]
    for copy in copies:
        copy.start()
    total = jnp.zeros((blocks, ROWS, 1), jnp.float32)
    for u in range(TP):
        values = rows_ref[:, u].astype(jnp.float32)
        total += jnp.sum(values * values, axis=-1, keepdims=True)
    factor = lax.rsqrt(total * (1.0 / D) + norm_eps)
    for u in range(TP):
        values = rows_ref[:, u].astype(jnp.float32) * factor
        normed_ref[u] = values.reshape(count, FEATS).astype(jnp.bfloat16)
    own_ref[...] = rows_ref[place_ref[0]]
    gate = jnp.zeros((count, HIDDEN), jnp.float32)
    lift = jnp.zeros((count, HIDDEN), jnp.float32)
    for u in range(TP):
        copies[u].wait()
        block = normed_ref[u]
        gate += lax.dot_general(
            block, weights_ref[u, :HIDDEN], by_rows, preferred_element_type=jnp.float32
        )
        lift += lax.dot_general(
            block, weights_ref[u, HIDDEN : 2 * HIDDEN], by_rows, preferred_element_type=jnp.float32
        )
    hidden = (gate * jax.nn.sigmoid(gate) * lift).astype(jnp.bfloat16)
    for u in range(TP):
        down = jnp.dot(hidden, weights_ref[u, 2 * HIDDEN :], preferred_element_type=jnp.float32)
        out_ref[:, u] = down.reshape(blocks, ROWS, FEATS).astype(jnp.bfloat16)


def first_partial(place, rows, weights):
    vmem = pl.BlockSpec(memory_space=pltpu.VMEM)
    return pl.pallas_call(
        first_kernel,
        out_shape=[
            pltpu.VMEM(rows.shape, jnp.bfloat16),
            pltpu.VMEM(rows.shape[1:], jnp.bfloat16),
        ],
        in_specs=[
            pl.BlockSpec(memory_space=pltpu.SMEM),
            vmem,
            pl.BlockSpec(memory_space=pltpu.HBM),
        ],
        out_specs=[vmem, vmem],
        scratch_shapes=[
            pltpu.VMEM((TP, Z * Y * ROWS, FEATS), jnp.bfloat16),
            pltpu.VMEM(weights.shape, jnp.bfloat16),
            pltpu.SemaphoreType.DMA((TP,)),
        ],
        compiler_params=pltpu.CompilerParams(vmem_limit_bytes=24 << 20),
        name="first_ffn",
    )(place, in_vmem(rows), in_hbm(weights))


def settle_kernel(rows_ref, share_ref, first_ref, copies_ref):
    for u in range(TP):
        branch = jnp.sum(share_ref[:, u].astype(jnp.float32), axis=0)
        own = rows_ref[u].astype(jnp.float32)
        first = (own + 0.5 * branch).astype(jnp.bfloat16)
        first_ref[u] = first
        for t in range(TP):
            copies_ref[t, u] = first


def settled(rows, share):
    shape = (TP, ROWS, FEATS)
    vmem = pl.BlockSpec(memory_space=pltpu.VMEM)
    return pl.pallas_call(
        settle_kernel,
        out_shape=[pltpu.VMEM(shape, jnp.bfloat16), pltpu.VMEM((TP, *shape), jnp.bfloat16)],
        in_specs=[vmem, vmem],
        out_specs=[vmem, vmem],
        compiler_params=pltpu.CompilerParams(vmem_limit_bytes=24 << 20),
        name="settle",
    )(in_vmem(rows), in_vmem(share))


def mix_kernel(first_ref, tiles_ref, copies_ref):
    mixed = jnp.sum(tiles_ref[...].astype(jnp.float32), axis=0)
    for u in range(TP):
        cols = slice(u * FEATS, (u + 1) * FEATS)
        rows = (first_ref[u].astype(jnp.float32) + mixed[:, cols]).astype(jnp.bfloat16)
        for z in range(Z):
            copies_ref[z, :, cols] = rows


def mixed_copies(first, tiles):
    vmem = pl.BlockSpec(memory_space=pltpu.VMEM)
    return pl.pallas_call(
        mix_kernel,
        out_shape=pltpu.VMEM((Z, ROWS, D), jnp.bfloat16),
        in_specs=[vmem, vmem],
        out_specs=vmem,
        compiler_params=pltpu.CompilerParams(vmem_limit_bytes=8 << 20),
        name="mix",
    )(in_vmem(first), in_vmem(tiles))


def second_kernel(
    place_ref, rows_ref, weights_hbm, out_ref, normed_ref, weights_ref, arrived
):
    rows = Z * ROWS
    copies = [
        pltpu.make_async_copy(
            weights_hbm.at[pl.ds(n * 4, 4)], weights_ref.at[pl.ds(n * 4, 4)], arrived.at[n]
        )
        for n in range(Y * TP // 4)
    ]
    for copy in copies:
        copy.start()
    values = rows_ref[...].astype(jnp.float32).reshape(rows, D)
    factor = lax.rsqrt(jnp.sum(values * values, axis=-1, keepdims=True) * (1.0 / D) + norm_eps)
    row = lax.broadcasted_iota(jnp.int32, (rows, 1), 0)
    own = jnp.where(row // ROWS == place_ref[1], 2.0, 0.0)
    for u in range(TP):
        normed_ref[u] = (values[:, u * FEATS : (u + 1) * FEATS] * factor).astype(jnp.bfloat16)
    hidden = []
    for y in range(Y):
        both = jnp.zeros((rows, 2 * HIDDEN), jnp.float32)
        for n in range(TP // 4):
            copies[y * TP // 4 + n].wait()
        for u in range(TP):
            both += lax.dot_general(
                normed_ref[u],
                weights_ref[y * TP + u, : 2 * HIDDEN],
                by_rows,
                preferred_element_type=jnp.float32,
            )
        gate, lift = both[:, :HIDDEN], both[:, HIDDEN:]
        hidden.append((gate * jax.nn.sigmoid(gate) * lift).astype(jnp.bfloat16))
    for u in range(TP):
        down = values[:, u * FEATS : (u + 1) * FEATS] * own
        for y in range(Y):
            down += jnp.dot(
                hidden[y],
                weights_ref[y * TP + u, 2 * HIDDEN :],
                preferred_element_type=jnp.float32,
            )
        out_ref[u] = down.reshape(Z, ROWS, FEATS).astype(jnp.bfloat16)


def second_partial(place, rows, weights):
    vmem = pl.BlockSpec(memory_space=pltpu.VMEM)
    return pl.pallas_call(
        second_kernel,
        out_shape=pltpu.VMEM((TP, Z, ROWS, FEATS), jnp.bfloat16),
        in_specs=[
            pl.BlockSpec(memory_space=pltpu.SMEM),
            vmem,
            pl.BlockSpec(memory_space=pltpu.HBM),
        ],
        out_specs=vmem,
        scratch_shapes=[
            pltpu.VMEM((TP, Z * ROWS, FEATS), jnp.bfloat16),
            pltpu.VMEM(weights.shape, jnp.bfloat16),
            pltpu.SemaphoreType.DMA((Y * TP // 4,)),
        ],
        compiler_params=pltpu.CompilerParams(vmem_limit_bytes=24 << 20),
        name="second_ffn",
    )(place, in_vmem(rows), in_hbm(weights))


def last_kernel(share_ref, out_ref):
    branch = jnp.sum(share_ref[...].astype(jnp.float32), axis=1)
    out_ref[...] = (0.5 * branch).reshape(TP * ROWS, FEATS).astype(jnp.bfloat16)


def last_sum(share):
    return pl.pallas_call(
        last_kernel,
        out_shape=jax.ShapeDtypeStruct((TP * ROWS, FEATS), jnp.bfloat16),
        in_specs=[pl.BlockSpec(memory_space=pltpu.VMEM)],
        compiler_params=pltpu.CompilerParams(vmem_limit_bytes=8 << 20),
        name="last",
    )(in_vmem(share))


def conv_silu(newest, buffer_ref, taps_ref):
    taps = taps_ref[...].astype(jnp.float32)
    summed = newest.astype(jnp.float32) * taps[3:4]
    for k in range(3):
        summed += buffer_ref[k].astype(jnp.float32) * taps[k : k + 1]
    return summed * jax.nn.sigmoid(summed)


SEQS = TP * ROWS
BLOCK = 8
CHANNELS = 256
PER_DEVICE = 4


def mixer_kernel(
    rows_ref,
    gain_ref,
    gate_ref,
    input_ref,
    write_ref,
    read_hbm,
    step_ref,
    bias_ref,
    rate_ref,
    skip_ref,
    taps_input_ref,
    taps_write_ref,
    taps_read_ref,
    buffer_input_ref,
    buffer_write_ref,
    buffer_read_ref,
    state_ref,
    group_ref,
    output_hbm,
    mixed_ref,
    new_state_ref,
    normed_ref,
    gate_z_ref,
    xc_ref,
    added_ref,
    retain_ref,
    bc_ref,
    rc_ref,
    out_cols_ref,
    read_ref,
    output_ref,
    arrived,
):
    i = pl.program_id(0)
    read_copy = pltpu.make_async_copy(read_hbm, read_ref, arrived.at[0])
    output_copy = pltpu.make_async_copy(output_hbm, output_ref, arrived.at[1])

    @pl.when(i == 0)
    def _():
        read_copy.start()
        output_copy.start()
        total = jnp.zeros((TP, ROWS, 1), jnp.float32)
        for u in range(TP):
            values = rows_ref[:, u].astype(jnp.float32)
            total += jnp.sum(values * values, axis=-1, keepdims=True)
        factor = lax.rsqrt(total * (1.0 / D) + norm_eps)
        for u in range(TP):
            values = (rows_ref[:, u].astype(jnp.float32) * factor).reshape(SEQS, FEATS)
            cols = slice(u * FEATS, (u + 1) * FEATS)
            gain = gain_ref[cols].astype(jnp.float32).reshape(1, FEATS)
            normed_ref[:, cols] = (values * gain).astype(jnp.bfloat16)
        normed = normed_ref[...]

        def project(weight_ref):
            return jnp.dot(normed, weight_ref[...], preferred_element_type=jnp.float32).astype(
                jnp.bfloat16
            )

        gate_z_ref[...] = project(gate_ref)
        step_raw = lax.dot_general(
            normed, step_ref[...], by_rows, preferred_element_type=jnp.float32
        ).astype(jnp.bfloat16)
        xc = conv_silu(project(input_ref), buffer_input_ref, taps_input_ref)
        bc_ref[...] = conv_silu(project(write_ref), buffer_write_ref, taps_write_ref)
        read_copy.wait()
        rc_ref[...] = conv_silu(project(read_ref), buffer_read_ref, taps_read_ref)
        xc_ref[...] = xc
        step = jax.nn.softplus(step_raw.astype(jnp.float32) + bias_ref[...].reshape(1, PER_DEVICE))
        retain = jnp.exp(-step * jnp.exp(rate_ref[...].reshape(1, PER_DEVICE)))
        head = lax.broadcasted_iota(jnp.int32, (SEQS, CHANNELS), 1) // HEAD_DIM
        step_wide = jnp.zeros((SEQS, CHANNELS), jnp.float32)
        retain_wide = jnp.zeros((SEQS, CHANNELS), jnp.float32)
        for h in range(PER_DEVICE):
            step_wide = jnp.where(head == h, step[:, h : h + 1], step_wide)
            retain_wide = jnp.where(head == h, retain[:, h : h + 1], retain_wide)
        added = (step_wide * xc).T
        retain_cols = retain_wide.T
        for s in range(SEQS // BLOCK):
            added_ref[s] = added[:, s * BLOCK : (s + 1) * BLOCK]
            retain_ref[s] = retain_cols[:, s * BLOCK : (s + 1) * BLOCK]

    added = added_ref[i]
    retain = retain_ref[i]
    writes = bc_ref[pl.ds(pl.multiple_of(i * BLOCK, BLOCK), BLOCK)]
    reads = rc_ref[pl.ds(pl.multiple_of(i * BLOCK, BLOCK), BLOCK)].astype(jnp.bfloat16)
    column = lax.broadcasted_iota(jnp.int32, (CHANNELS, BLOCK), 1)
    cols = jnp.zeros((CHANNELS, BLOCK), jnp.float32)
    for b in range(BLOCK):
        new = []
        for h in range(PER_DEVICE):
            top = h * HEAD_DIM
            kept = jnp.broadcast_to(retain[top : top + 8, b : b + 1], (8, STATE))
            old = state_ref[i * BLOCK + b, h].reshape(HEAD_DIM // 8, 8, STATE) * kept[None]
            new.append(
                old.reshape(HEAD_DIM, STATE)
                + added[top : top + HEAD_DIM, b : b + 1] * writes[b : b + 1]
            )
            new_state_ref[b, h] = new[h]
        new = jnp.concatenate(new, axis=0).astype(jnp.bfloat16)
        read = lax.dot_general(new, reads, by_rows, preferred_element_type=jnp.float32)
        cols = jnp.where(column == b, read, cols)
    out_cols_ref[i] = cols

    @pl.when(i == pl.num_programs(0) - 1)
    def _():
        cols = jnp.concatenate([out_cols_ref[s] for s in range(SEQS // BLOCK)], axis=1)
        head = lax.broadcasted_iota(jnp.int32, (1, CHANNELS), 1) // HEAD_DIM
        skip_own = skip_ref[...].reshape(1, PER_DEVICE)
        skip = jnp.zeros((1, CHANNELS), jnp.float32)
        for h in range(PER_DEVICE):
            skip = jnp.where(head == h, skip_own[:, h : h + 1], skip)
        head_out = (cols.T + skip * xc_ref[...]).astype(jnp.bfloat16).astype(jnp.float32)
        gate_z = gate_z_ref[...].astype(jnp.float32)
        gated = head_out * (gate_z * jax.nn.sigmoid(gate_z))
        gated = gated * inverse_rms(gated) * group_ref[...].astype(jnp.float32).reshape(1, CHANNELS)
        output_copy.wait()
        part = jnp.dot(
            gated.astype(jnp.bfloat16), output_ref[...], preferred_element_type=jnp.float32
        )
        mixed_ref[...] = part.reshape(TP, ROWS, D).astype(jnp.bfloat16)


def state_mixer(first, rows, small, buffers, scan_state, group_gain, proj_output):
    operands = [rows, *small, *[b.transpose(1, 0, 2) for b in buffers]]
    operands += [scan_state, group_gain, proj_output]
    from_hbm = (5, len(operands) - 1)
    operands = [in_hbm(o) if n in from_hbm else in_vmem(o) for n, o in enumerate(operands)]
    specs = [pl.BlockSpec(memory_space=pltpu.VMEM) for _ in operands]
    for n in from_hbm:
        specs[n] = pl.BlockSpec(memory_space=pltpu.HBM)
    state_spec = pl.BlockSpec((BLOCK, PER_DEVICE, HEAD_DIM, STATE), lambda i: (i, 0, 0, 0))
    blocks = SEQS // BLOCK
    partial_out, state_out = pl.pallas_call(
        mixer_kernel,
        grid=(blocks,),
        out_shape=[
            pltpu.VMEM((TP, ROWS, D), jnp.bfloat16),
            jax.ShapeDtypeStruct(scan_state.shape, jnp.float32),
        ],
        in_specs=specs,
        out_specs=[pl.BlockSpec(memory_space=pltpu.VMEM), state_spec],
        scratch_shapes=[
            pltpu.VMEM((SEQS, D), jnp.bfloat16),
            pltpu.VMEM((SEQS, CHANNELS), jnp.bfloat16),
            pltpu.VMEM((SEQS, CHANNELS), jnp.float32),
            pltpu.VMEM((blocks, CHANNELS, BLOCK), jnp.float32),
            pltpu.VMEM((blocks, CHANNELS, BLOCK), jnp.float32),
            pltpu.VMEM((SEQS, STATE), jnp.float32),
            pltpu.VMEM((SEQS, STATE), jnp.float32),
            pltpu.VMEM((blocks, CHANNELS, BLOCK), jnp.float32),
            pltpu.VMEM((D, STATE), jnp.bfloat16),
            pltpu.VMEM((CHANNELS, D), jnp.bfloat16),
            pltpu.SemaphoreType.DMA((2,)),
        ],
        compiler_params=pltpu.CompilerParams(vmem_limit_bytes=24 << 20),
        name="mixer",
    )(*operands)
    tiles = lax.all_to_all(partial_out, TP_AXES, 0, 0, tiled=True)
    return (mixed_copies(first, tiles), state_out)


def per_device(
    residual,
    first_gain,
    first_gate,
    first_lift,
    first_down,
    mixer_gain,
    proj_gate,
    proj_input,
    proj_write,
    proj_read,
    proj_step,
    step_bias,
    rate_log,
    skip_gain,
    taps_input,
    taps_write,
    taps_read,
    buffer_input,
    buffer_write,
    buffer_read,
    scan_state,
    group_gain,
    proj_output,
    second_gain,
    second_gate,
    second_lift,
    second_down,
):
    place = jnp.stack([lax.axis_index(BLOCK_AXES), lax.axis_index("z")]).astype(jnp.int32)
    share_one, share_two, pieces = weight_shares(
        place,
        residual,
        (first_gain, first_gate, first_lift, first_down),
        (second_gain, second_gate, second_lift, second_down),
    )
    weights_one = lax.all_gather(share_one, TP_AXES)

    mine = lax.all_to_all(pieces, TP_AXES, 0, 0, tiled=True)
    share_two, mine = lax.optimization_barrier((share_two, mine))
    weights_two = lax.all_gather(share_two, ("y", *TP_AXES))
    tiles = sent_to_all(mine, BLOCK_AXES).reshape(Z * Y, TP, ROWS, FEATS)
    share, own = first_partial(place, tiles, weights_one)
    share = lax.all_to_all(share, BLOCK_AXES, 0, 0, tiled=True)
    first, copies = settled(own, share)

    mixed, state_out = state_mixer(
        first,
        lax.all_to_all(copies, TP_AXES, 0, 0, tiled=True),
        (
            mixer_gain,
            proj_gate,
            proj_input,
            proj_write,
            proj_read,
            proj_step.T,
            step_bias,
            rate_log,
            skip_gain,
            taps_input,
            taps_write,
            taps_read,
        ),
        (buffer_input, buffer_write, buffer_read),
        scan_state,
        group_gain,
        proj_output,
    )

    rows = lax.all_to_all(mixed, "z", 0, 0, tiled=True)
    share = second_partial(place, rows, weights_two)
    share = lax.all_to_all(share.reshape(-1, ROWS, FEATS), (*TP_AXES, "z"), 0, 0, tiled=True)
    residual_out = last_sum(share.reshape(TP, Z, ROWS, FEATS))
    return (residual_out, state_out)


def solution(mesh):
    mesh = Mesh(mesh.devices.reshape(Z, Y, TP // 2, 2), (*KV_AXES, *TP_AXES))
    placed = (
        P(KV_AXES, TP_AXES),
        P(TP_AXES),
        P(TP_AXES, KV_AXES),
        P(TP_AXES, KV_AXES),
        P(KV_AXES, TP_AXES),
        P(),
        P(None, TP_AXES),
        P(None, TP_AXES),
        P(None, TP_AXES),
        P(None, TP_AXES),
        P(None, TP_AXES),
        P(TP_AXES),
        P(TP_AXES),
        P(TP_AXES),
        P(None, TP_AXES),
        P(None, TP_AXES),
        P(None, TP_AXES),
        P(KV_AXES, None, TP_AXES),
        P(KV_AXES, None, TP_AXES),
        P(KV_AXES, None, TP_AXES),
        P(KV_AXES, TP_AXES, None, None),
        P(TP_AXES),
        P(TP_AXES, None),
        P(TP_AXES),
        P(TP_AXES, KV_AXES),
        P(TP_AXES, KV_AXES),
        P(KV_AXES, TP_AXES),
    )
    return jax.shard_map(
        per_device,
        mesh=mesh,
        in_specs=placed,
        out_specs=(P(KV_AXES, TP_AXES), P(KV_AXES, TP_AXES, None, None)),
        check_vma=False,
    )
```
